32 devices in a mesh: ep: 32 (over z, y, x, core).
Axes of the slice: x: 2, y: 2, z: 4, core: 2. Of those that a mesh axis runs over, the one named last changes fastest.
Arguments:
- tokens: bfloat16 [576, 2048], P('ep'), may hold values from -6 to 6
- attn_norm_gain: float32 [2048], replicated, may hold values from 0.1 to 1.9
- w_query: bfloat16 [2048, 512], replicated, may hold values from -0.125 to 0.125
- w_key: bfloat16 [2048, 128], replicated, may hold values from -0.125 to 0.125
- w_value: bfloat16 [2048, 128], replicated, may hold values from -0.125 to 0.125
- w_forget: bfloat16 [2048, 8], replicated, may hold values from -0.125 to 0.125
- forget_bias: float32 [8], replicated, may hold values from 0.5 to 4
- w_attn_out: bfloat16 [512, 2048], replicated, may hold values from -0.25 to 0.25
- cache_keys: bfloat16 [576, 1024, 128], P('ep'), may hold values from -72 to 72
- cache_values: bfloat16 [576, 1024, 128], P('ep'), may hold values from -6 to 6
- cache_logcum: float32 [576, 8, 1024], P('ep'), as said below
- cache_lengths: int32 [576], P('ep'), may hold values from 128 to 1024
- expert_norm_gain: float32 [2048], replicated, may hold values from 0.4 to 40
- expert_ids: int32 [576, 6], P('ep'), may hold values from 0 to 31, all different within a row; in each aligned block of 18 rows (0 to 17, 18 to 35, ...) at most 6 rows name the same one
- expert_weights: float32 [576, 6], P('ep'), may hold values from 0.1 to 1
- w_expert_gate: bfloat16 [32, 2048, 512], P('ep'), may hold values from -0.125 to 0.125
- w_expert_up: bfloat16 [32, 2048, 512], P('ep'), may hold values from -0.125 to 0.125
- w_expert_down: bfloat16 [32, 512, 2048], P('ep'), may hold values from -0.25 to 0.25
- w_dense_gate: bfloat16 [2048, 4096], P(None, 'ep'), may hold values from -0.125 to 0.125
- w_dense_up: bfloat16 [2048, 4096], P(None, 'ep'), may hold values from -2 to 2
- w_dense_down: bfloat16 [4096, 2048], P('ep'), may hold values from -0.09375 to 0.09375
- dense_norm_gain: float32 [4096], replicated, may hold values from 0.1 to 1.9
- branch_gate: float32 [2048], replicated, may hold values from -0.125 to 0.125
Outputs:
- result: bfloat16 [576, 2048], P('ep')
The draws below stay inside these ranges and needn't reach their ends.
Inputs may be any that keep to these rules, and one draw needn't show every extreme that they name: `cache_logcum`: along the positions of each sequence and head the values never rise. `expert_ids`: each row names 6 different experts; among the rows of one device no expert is named by more than 6 rows, and in every draw some device names some expert exactly 6 times.
All inputs are finite; a program needn't handle non-finite values.
Results may differ from the reference program's by a relative error of at most 0.012.
The reference program's roundings to bfloat16 on the way count: a program that leaves them out, or rounds other values in their place, can miss the bound.
Values may be sent and summed in bfloat16 or wider, within the bound.
A program may use at most 128 MiB of HBM per device.

```python
import math
import jax
import jax.numpy as jnp
import numpy as np
from jax import lax

D = 2048
HEADS = 8
KV_HEADS = 2
HEAD_DIM = 64
EXPERT_FF = 512
DENSE_FF = 4096
TOPK = 6
SEQ_DEV = 18
CACHE_POSITIONS = 1024
SEQS = 576
EXPERTS = 32
CAP = 6
N_EP = 32


def draw_cache_keys(key, part):
    tensor_extent = (SEQS, CACHE_POSITIONS, KV_HEADS * HEAD_DIM)
    base = jnp.clip(jax.random.normal(jax.random.fold_in(key, 11), tensor_extent, jnp.float32), -6.0, 6.0)
    values = base
    return jnp.clip(values, -72.0, 72.0).astype(jnp.bfloat16)


def draw_cache_logcum(key, part):
    tensor_extent = (SEQS, HEADS, CACHE_POSITIONS)
    order = jax.random.permutation(jax.random.fold_in(key, 21), HEADS)
    gradual_decay = (order < HEADS // 2)[None, :, None]
    chain_total = jax.random.uniform(jax.random.fold_in(key, 22), (SEQS, HEADS, 1), jnp.float32, 0.3, 1.5)
    fast_span = jax.random.uniform(jax.random.fold_in(key, 23), (SEQS, HEADS, 1), jnp.float32, 30.0, 100.0)
    decay_speed = jnp.where(gradual_decay, chain_total / CACHE_POSITIONS, 1.0 / fast_span)
    sequence_multiplier = jnp.exp(jax.random.uniform(jax.random.fold_in(key, 24), (SEQS, 1, 1), jnp.float32, -0.7, 0.7))
    coarse_estimate = jnp.exp(jax.random.uniform(jax.random.fold_in(key, 25), tensor_extent, jnp.float32, -0.7, 0.7))
    spike_position = jax.random.uniform(jax.random.fold_in(key, 26), tensor_extent, jnp.float32) < 3.0 / CACHE_POSITIONS
    spike_amount = -jnp.log(jax.random.uniform(jax.random.fold_in(key, 27), tensor_extent, jnp.float32, 0.5, 0.8))
    step_numbers = decay_speed * sequence_multiplier * coarse_estimate + jnp.where(spike_position & gradual_decay, spike_amount, 0.0)
    return -jnp.cumsum(step_numbers, axis=2)


def draw_expert_norm_gain(key, part):
    base = 1.0 + 0.18 * jnp.clip(jax.random.normal(jax.random.fold_in(key, 31), (D,), jnp.float32), -3.0, 3.0)
    return base


def draw_w_dense_up(key, part):
    normal_part = jnp.clip(jax.random.normal(jax.random.fold_in(key, 41), (D, DENSE_FF), jnp.float32), -6.0, 6.0)
    column = jnp.arange(DENSE_FF, dtype=jnp.float32)[None, :] / DENSE_FF
    scale = 3.0 ** column * jnp.exp(jax.random.uniform(jax.random.fold_in(key, 43), (1, DENSE_FF), jnp.float32, -0.3, 0.3))
    return jnp.clip(normal_part * D ** (-0.5) * scale, -2.0, 2.0).astype(jnp.bfloat16)


def with_ends(drawn, key, smallest, largest):
    shape = drawn.shape
    spot = [jax.random.randint(jax.random.fold_in(key, axis), (), 0, shape[axis]) for axis in range(len(shape))]
    drawn = drawn.at[tuple(spot)].set(smallest)
    longest = shape.index(max(shape))
    spot[longest] = (spot[longest] + 1) % shape[longest]
    return drawn.at[tuple(spot)].set(largest)


def steps_of(key, extent, cuts, least, top_value):
    factor_of = 1.0
    for axis_at, parts in cuts:
        steps = jax.random.uniform(jax.random.fold_in(jax.random.fold_in(key, 6), axis_at), (parts,), jnp.float32, least / len(cuts), top_value / len(cuts))
        factor_of = factor_of * jnp.repeat(jnp.exp(steps), extent[axis_at] // parts).reshape((-1,) + (1,) * (len(extent) - 1 - axis_at))
    return factor_of


def deal_out(rng, own, number, rows, number_of, top, most, lean):
    sequence = jax.random.permutation(rng, number_of)
    crowded, usual = shares(number_of, rows * top, most, lean, True), shares(number_of, rows * top, most, lean, False)
    places = jnp.arange(number_of)

    def named(tallies, rotation):
        used = int((tallies > 0).sum())
        fixed = max(1, used // 4)
        shifted = fixed + (places - fixed + rotation * (used - fixed)) % max(1, number_of - fixed)
        return jnp.zeros((number_of,), jnp.int32).at[sequence[jnp.where(places < fixed, places, shifted)]].set(jnp.asarray(tallies, jnp.int32))

    tallies = jnp.where(number % 4 == 0, named(crowded, number // 4), named(usual, number - number // 4 - 1))
    mixed = jax.random.permutation(jax.random.fold_in(own, 3), number_of)
    giver, receiver = mixed[0:number_of // 2 * 2:2], mixed[1:number_of // 2 * 2:2]
    margin = jnp.minimum(tallies[giver] - 1, most - tallies[receiver]) // 2
    margin = jnp.where((giver == sequence[0]) | (receiver == sequence[0]) | (tallies[receiver] == 0), 0, jnp.maximum(margin, 0))
    shifted = jax.random.randint(jax.random.fold_in(own, 4), (number_of // 2,), 0, 1 << 20) % (margin + 1)
    tallies = tallies.at[giver].add(-shifted).at[receiver].add(shifted)
    labels = jnp.searchsorted(jnp.cumsum(tallies), jnp.arange(rows * top), side="right").astype(jnp.int32)
    listing = labels.reshape(top, rows).T
    listing = listing[jax.random.permutation(jax.random.fold_in(own, 1), rows)]
    rotation = jax.random.randint(jax.random.fold_in(own, 2), (rows, 1), 0, top)
    return jnp.take_along_axis(listing, (jnp.arange(top)[None, :] + rotation) % top, axis=1)


def shares(number_of, total, limit, skew, full):
    loads = [(1 << 20) // math.isqrt(standing ** skew) + 1 for standing in range(1, number_of + 1)]
    largest = limit if full else min(limit, max(-(-total // number_of), total * loads[0] // sum(loads)))
    least = 1 if total - largest >= number_of - 1 else 0
    given, spare = [largest] + [least] * (number_of - 1), total - largest - least * (number_of - 1)
    while spare > 0:
        candidates = [i for i in range(1, number_of) if given[i] < largest] or [i for i in range(1, number_of) if given[i] < limit]
        whole, budget = sum([loads[i] for i in candidates]), spare
        for i in candidates:
            extra = min(limit - given[i], max(1, budget * loads[i] // whole), spare)
            given[i] = given[i] + extra
            spare = spare - extra
    return np.array(given)


def centred(rng, extent, deviation, bound, shards=(), held_as=jnp.bfloat16):
    values = deviation * jax.random.normal(rng, extent, jnp.float32)
    if shards:
        values = values * steps_of(rng, extent, shards, -0.22, 0.18)
    return jnp.clip(values, -bound, bound).astype(held_as)


def setup_inputs(seed: int = 0) -> dict:
    splits = jax.random.split(jax.random.key(seed), 24)
    tokens = centred(splits[0], (SEQS, D), 1.0, 6.0, ((0, 32),))
    attn_norm_gain = jnp.clip(1.0 + 0.18 * jax.random.normal(splits[1], (D,), jnp.float32), 0.1, 1.9)
    w_query = centred(splits[2], (D, HEADS * HEAD_DIM), D ** -0.5, 0.125)
    w_key = centred(splits[3], (D, KV_HEADS * HEAD_DIM), D ** -0.5, 0.125)
    w_value = centred(splits[4], (D, KV_HEADS * HEAD_DIM), D ** -0.5, 0.125)
    w_forget = centred(splits[5], (D, HEADS), D ** -0.5, 0.125)
    forget_bias = jnp.clip(jax.random.uniform(splits[6], (HEADS,), jnp.float32, 0.5, 4.0), 0.5, 4.0)
    w_attn_out = centred(splits[7], (HEADS * HEAD_DIM, D), (HEADS * HEAD_DIM) ** -0.5, 0.25)
    cache_keys = draw_cache_keys(jax.random.fold_in(splits[23], 71), 0)
    cache_values = centred(splits[9], (SEQS, CACHE_POSITIONS, KV_HEADS * HEAD_DIM), 1.0, 6.0, ((0, 32),))
    cache_logcum = draw_cache_logcum(jax.random.fold_in(splits[23], 71), 0)
    cache_lengths = with_ends(jax.random.randint(splits[11], (SEQS,), CACHE_POSITIONS // 8, CACHE_POSITIONS + 1), jax.random.fold_in(splits[11], 1), CACHE_POSITIONS // 8, CACHE_POSITIONS).astype(jnp.int32)
    expert_norm_gain = draw_expert_norm_gain(jax.random.fold_in(splits[23], 71), 0)
    expert_ids_keys = jax.random.split(jax.random.fold_in(splits[13], 1), SEQS // SEQ_DEV)
    expert_ids_turns = jax.random.permutation(jax.random.fold_in(splits[13], 3), SEQS // SEQ_DEV)
    expert_ids = jax.vmap(lambda own, number: deal_out(jax.random.fold_in(splits[13], 2), own, number, SEQ_DEV, EXPERTS, TOPK, CAP, 2))(expert_ids_keys, expert_ids_turns).reshape((SEQS, TOPK))
    expert_weights = jnp.clip(jnp.exp(math.log(1.0) - 2.3025851 * jax.random.uniform(splits[14], (SEQS, TOPK), jnp.float32) ** steps_of(splits[14], (SEQS, TOPK), ((0, 32),), -0.2, 0.2)), 0.1, 1.0)
    w_expert_gate = centred(splits[15], (EXPERTS, D, EXPERT_FF), D ** -0.5, 0.125, ((0, 32),))
    w_expert_up = centred(splits[16], (EXPERTS, D, EXPERT_FF), D ** -0.5, 0.125, ((0, 32),))
    w_expert_down = centred(splits[17], (EXPERTS, EXPERT_FF, D), EXPERT_FF ** -0.5, 0.25, ((0, 32),))
    w_dense_gate = centred(splits[18], (D, DENSE_FF), D ** -0.5, 0.125, ((1, 32),))
    w_dense_up = draw_w_dense_up(jax.random.fold_in(splits[23], 71), 0)
    w_dense_down = centred(splits[20], (DENSE_FF, D), DENSE_FF ** -0.5, 0.09375, ((0, 32),))
    dense_norm_gain = jnp.clip(1.0 + 0.18 * jax.random.normal(splits[21], (DENSE_FF,), jnp.float32), 0.1, 1.9)
    branch_gate = centred(splits[22], (D,), D ** -0.5, 0.125, (), jnp.float32)
    return dict(tokens=tokens, attn_norm_gain=attn_norm_gain, w_query=w_query, w_key=w_key, w_value=w_value, w_forget=w_forget, forget_bias=forget_bias, w_attn_out=w_attn_out, cache_keys=cache_keys, cache_values=cache_values, cache_logcum=cache_logcum, cache_lengths=cache_lengths, expert_norm_gain=expert_norm_gain, expert_ids=expert_ids, expert_weights=expert_weights, w_expert_gate=w_expert_gate, w_expert_up=w_expert_up, w_expert_down=w_expert_down, w_dense_gate=w_dense_gate, w_dense_up=w_dense_up, w_dense_down=w_dense_down, dense_norm_gain=dense_norm_gain, branch_gate=branch_gate)


EPS = 1e-06
LIMIT = 7.0
ALPHA = 1.702

def normalize(values, gain):
    return values * lax.rsqrt(lax.optimization_barrier(jnp.mean(values * values, axis=-1, keepdims=True)) + EPS) * gain

def stored(values):
    return lax.optimization_barrier(values.astype(jnp.bfloat16))

def attend(query, key_new, value_new, log_forget, cache_keys, cache_values, cache_logcum, cache_lengths):
    seqs, length = (cache_keys.shape[0], cache_keys.shape[1])
    group = HEADS // KV_HEADS
    scale = HEAD_DIM ** (-0.5)
    heads_q = query.astype(jnp.float32).reshape(seqs, KV_HEADS, group, HEAD_DIM)
    keys = cache_keys.astype(jnp.float32).reshape(seqs, length, KV_HEADS, HEAD_DIM)
    values = cache_values.astype(jnp.float32).reshape(seqs, length, KV_HEADS, HEAD_DIM)
    own_key = key_new.astype(jnp.float32).reshape(seqs, KV_HEADS, HEAD_DIM)
    own_value = value_new.astype(jnp.float32).reshape(seqs, KV_HEADS, 1, HEAD_DIM)
    last_index = jnp.broadcast_to((cache_lengths - 1)[:, None, None], (seqs, HEADS, 1)).astype(jnp.int32)
    carried = jnp.take_along_axis(cache_logcum, last_index, axis=2)[:, :, 0] + log_forget
    offset = (carried[:, :, None] - cache_logcum).reshape(seqs, KV_HEADS, group, length)
    scores = jnp.einsum('skgd,slkd->skgl', heads_q, keys) * scale + offset
    live = jnp.arange(length, dtype=jnp.int32)[None, :] < cache_lengths[:, None]
    scores = jnp.where(live[:, None, None, :], scores, -jnp.inf)
    own = jnp.einsum('skgd,skd->skg', heads_q, own_key) * scale
    top = jnp.maximum(lax.optimization_barrier(jnp.max(scores, axis=-1)), own)
    expo = jnp.exp(scores - top[..., None])
    own_expo = jnp.exp(own - top)
    total = lax.optimization_barrier(jnp.sum(expo, axis=-1)) + own_expo
    weights = stored(expo / total[..., None]).astype(jnp.float32)
    own_weight = stored(own_expo / total).astype(jnp.float32)
    out = jnp.einsum('skgl,slkd->skgd', weights, values) + own_weight[..., None] * own_value
    return out.reshape(seqs, HEADS * HEAD_DIM).astype(jnp.bfloat16)

def expert_unit(rows, gate_w, up_w, down_w):
    gate = jnp.minimum(jnp.dot(rows, gate_w, preferred_element_type=jnp.float32), LIMIT)
    up = jnp.clip(jnp.dot(rows, up_w, preferred_element_type=jnp.float32), -LIMIT, LIMIT)
    act = ((up + 1.0) * gate * jax.nn.sigmoid(gate * ALPHA)).astype(jnp.bfloat16)
    return jnp.dot(act, down_w, preferred_element_type=jnp.float32).astype(jnp.bfloat16)

def reference(tokens, attn_norm_gain, w_query, w_key, w_value, w_forget, forget_bias, w_attn_out, cache_keys, cache_values, cache_logcum, cache_lengths, expert_norm_gain, expert_ids, expert_weights, w_expert_gate, w_expert_up, w_expert_down, w_dense_gate, w_dense_up, w_dense_down, dense_norm_gain, branch_gate):
    seqs = tokens.shape[0]
    normed = normalize(tokens.astype(jnp.float32), attn_norm_gain).astype(jnp.bfloat16)
    query = jnp.dot(normed, w_query, preferred_element_type=jnp.float32).astype(jnp.bfloat16)
    key_new = jnp.dot(normed, w_key, preferred_element_type=jnp.float32).astype(jnp.bfloat16)
    value_new = jnp.dot(normed, w_value, preferred_element_type=jnp.float32).astype(jnp.bfloat16)
    log_forget = jax.nn.log_sigmoid(jnp.dot(normed, w_forget, preferred_element_type=jnp.float32) + forget_bias)

    def one_block(index):
        start = index * SEQ_DEV

        def pick(array):
            return lax.dynamic_slice_in_dim(array, start, SEQ_DEV, 0)
        return attend(pick(query), pick(key_new), pick(value_new), pick(log_forget), pick(cache_keys), pick(cache_values), pick(cache_logcum), pick(cache_lengths))
    attended = lax.map(one_block, jnp.arange(N_EP, dtype=jnp.int32)).reshape(seqs, HEADS * HEAD_DIM)
    mixed = stored(tokens.astype(jnp.float32) + jnp.dot(attended, w_attn_out, preferred_element_type=jnp.float32))
    routed_in = normalize(mixed.astype(jnp.float32), expert_norm_gain).astype(jnp.bfloat16)
    flat_ids = expert_ids.reshape(-1)
    rows_all = flat_ids.shape[0]
    room = N_EP * CAP

    def run_expert(outputs, expert):
        chosen = flat_ids == expert
        order = jnp.cumsum(chosen.astype(jnp.int32)) - 1
        where_to = jnp.where(chosen, order, room).astype(jnp.int32)
        source = jnp.zeros((room,), jnp.int32).at[where_to].set(jnp.arange(rows_all, dtype=jnp.int32), mode='drop')
        picked = jnp.take(routed_in, source // TOPK, axis=0)
        answer = expert_unit(picked, w_expert_gate[expert], w_expert_up[expert], w_expert_down[expert])
        filled = jnp.arange(room, dtype=jnp.int32) < jnp.sum(chosen.astype(jnp.int32))
        target = jnp.where(filled, source, rows_all).astype(jnp.int32)
        return (outputs.at[target].set(answer, mode='drop'), None)
    outputs = lax.scan(run_expert, jnp.zeros((rows_all, D), jnp.bfloat16), jnp.arange(EXPERTS, dtype=jnp.int32))[0]
    routed = lax.optimization_barrier(jnp.sum(expert_weights[:, :, None] * outputs.astype(jnp.float32).reshape(seqs, TOPK, D), axis=1))
    gate_dense = jnp.dot(routed_in, w_dense_gate, preferred_element_type=jnp.float32)
    up_dense = jnp.dot(routed_in, w_dense_up, preferred_element_type=jnp.float32)
    units = stored(jax.nn.silu(gate_dense) * up_dense).astype(jnp.float32)
    unit_scale = lax.rsqrt(lax.optimization_barrier(jnp.mean(units * units, axis=1, keepdims=True)) + EPS)
    hidden = (units * unit_scale * dense_norm_gain).astype(jnp.bfloat16)
    dense = jnp.dot(hidden, w_dense_down, preferred_element_type=jnp.float32)
    branch_scale = jax.nn.sigmoid(lax.optimization_barrier(jnp.sum(routed_in.astype(jnp.float32) * branch_gate, axis=1, keepdims=True)))
    return (mixed.astype(jnp.float32) + routed + branch_scale * dense).astype(jnp.bfloat16)
```

```python
import functools

import jax
import jax.numpy as jnp
from jax import lax
from jax.experimental import pallas as pl
from jax.experimental.pallas import tpu as pltpu
from jax.sharding import PartitionSpec as P

HEADS = 8
KV_HEADS = 2
HEAD_DIM = 64
TOPK = 6


EPS = 1e-06
LIMIT = 7.0
ALPHA = 1.702


def normalize(values, gain):
    return values * lax.rsqrt(jnp.mean(values * values, axis=-1, keepdims=True) + EPS) * gain


def stored(values):
    return lax.optimization_barrier(values.astype(jnp.bfloat16))


def front_body(
    lengths,
    tokens,
    gain_ref,
    w_query,
    w_key,
    w_value,
    w_forget,
    bias,
    w_out,
    gain_next,
    keys,
    values,
    logcum,
    mixed_ref,
    routed_ref,
    query_s,
    key_s,
    value_s,
    forget_s,
    attended_s,
):
    step = pl.program_id(0)
    batch, length, pair = keys.shape
    rows = jnp.float32
    group = HEADS // KV_HEADS
    tiles = HEADS * HEAD_DIM // pair

    @pl.when(step == 0)
    def _():
        normed = normalize(tokens[...].astype(rows), gain_ref[...]).astype(jnp.bfloat16)
        for weight, kept in ((w_key, key_s), (w_value, value_s)):
            product = jnp.dot(normed, weight[...], preferred_element_type=rows)
            kept[...] = product.astype(jnp.bfloat16).astype(rows)
        product = jnp.dot(normed, w_query[...], preferred_element_type=rows)
        product = product.astype(jnp.bfloat16).astype(rows)
        for tile in range(tiles):
            query_s[tile] = product[:, tile * pair : (tile + 1) * pair]
        forget = lax.dot_general(
            w_forget[...], normed, (((1,), (1,)), ((), ())), preferred_element_type=rows
        )
        forget = forget + bias[...]
        forget_s[...] = jnp.minimum(forget, 0.0) - jnp.log1p(jnp.exp(-jnp.abs(forget)))

    lane = lax.broadcasted_iota(jnp.int32, (HEADS, pair), 1)
    head = lax.broadcasted_iota(jnp.int32, (HEADS, pair), 0)
    odd = lane // HEAD_DIM
    place = head // group
    seq_lane = lax.broadcasted_iota(jnp.int32, forget_s.shape, 1)
    position = lax.broadcasted_iota(jnp.int32, (HEADS, length), 1)
    scale = HEAD_DIM ** (-0.5)
    for item in range(batch):
        seq = step * batch + item
        stay = jnp.zeros((HEADS, pair), rows)
        move = jnp.zeros((HEADS, pair), rows)
        for tile in range(tiles):
            piece = jnp.broadcast_to(
                query_s[tile, pl.ds(seq, 1), :], (HEADS, pair)
            )
            own_lanes = head == 2 * tile + odd
            stay = jnp.where(own_lanes & (odd == place), piece, stay)
            move = jnp.where(own_lanes & (odd != place), piece, move)
        query = stay + pltpu.roll(move, HEAD_DIM, 1)
        own = jnp.sum(query * key_s[pl.ds(seq, 1), :], axis=1, keepdims=True) * scale
        forget = jnp.sum(jnp.where(seq_lane == seq, forget_s[...], 0.0), axis=1, keepdims=True)
        cum = logcum[item]
        live_count = lengths[seq]
        last = jnp.sum(jnp.where(position == live_count - 1, cum, 0.0), axis=1, keepdims=True)
        scores = lax.dot_general(
            query.astype(jnp.bfloat16),
            keys[item],
            (((1,), (1,)), ((), ())),
            preferred_element_type=rows,
        )
        scores = scores * scale + ((last + forget) - cum)
        scores = jnp.where(position < live_count, scores, -jnp.inf)
        top = jnp.maximum(jnp.max(scores, axis=1, keepdims=True), own)
        expo = jnp.exp(scores - top)
        own_expo = jnp.exp(own - top)
        total = jnp.sum(expo, axis=1, keepdims=True) + own_expo
        weights = (expo / total).astype(jnp.bfloat16)
        own_weight = (own_expo / total).astype(jnp.bfloat16).astype(rows)
        out = jnp.dot(weights, values[item], preferred_element_type=rows)
        out = out + own_weight * value_s[pl.ds(seq, 1), :]
        turned = pltpu.roll(out, HEAD_DIM, 1)
        for tile in range(tiles):
            own_lanes = head == 2 * tile + odd
            part = jnp.where(own_lanes, jnp.where(odd == place, out, turned), 0.0)
            attended_s[tile, pl.ds(seq, 1), :] = jnp.sum(part, axis=0, keepdims=True)

    @pl.when(step == pl.num_programs(0) - 1)
    def _():
        attended = jnp.concatenate([attended_s[tile] for tile in range(tiles)], axis=1)
        attended = attended.astype(jnp.bfloat16)
        mixed = tokens[...].astype(rows) + jnp.dot(
            attended, w_out[...], preferred_element_type=rows
        )
        mixed = mixed.astype(jnp.bfloat16)
        mixed_ref[...] = mixed
        routed_ref[...] = normalize(mixed.astype(rows), gain_next[...]).astype(jnp.bfloat16)


def front(
    tokens, gain, w_query, w_key, w_value, w_forget, bias, w_out, keys, values, logcum, lengths, gain_next
):
    seqs, width = tokens.shape
    batch = max(size for size in (1, 2, 3) if seqs % size == 0)
    pair = keys.shape[2]

    def whole(*shape):
        return pl.BlockSpec(shape, lambda i, *_: (0,) * len(shape))

    def each(*shape):
        return pl.BlockSpec((batch, *shape), lambda i, *_: (i, 0, 0))

    small = (
        tokens,
        gain[None, :],
        w_query,
        w_key,
        w_value,
        w_forget.T,
        bias[:, None],
        w_out,
        gain_next[None, :],
    )
    kept = jax.ShapeDtypeStruct((seqs, width), jnp.bfloat16)
    return pl.pallas_call(
        front_body,
        out_shape=(kept, kept),
        grid_spec=pltpu.PrefetchScalarGridSpec(
            num_scalar_prefetch=1,
            grid=(seqs // batch,),
            in_specs=[whole(*array.shape) for array in small]
            + [each(*keys.shape[1:]), each(*values.shape[1:]), each(*logcum.shape[1:])],
            out_specs=[whole(seqs, width)] * 2,
            scratch_shapes=[
                pltpu.VMEM((HEADS * HEAD_DIM // pair, seqs, pair), jnp.float32),
                pltpu.VMEM((seqs, pair), jnp.float32),
                pltpu.VMEM((seqs, pair), jnp.float32),
                pltpu.VMEM((HEADS, seqs), jnp.float32),
                pltpu.VMEM((HEADS * HEAD_DIM // pair, seqs, pair), jnp.float32),
            ],
        ),
        compiler_params=pltpu.CompilerParams(
            dimension_semantics=("arbitrary",), vmem_limit_bytes=40 * 1024 * 1024
        ),
        cost_estimate=pl.CostEstimate(
            flops=10**9, bytes_accessed=16 * 10**6, transcendentals=2 * 10**5
        ),
        name="front",
    )(lengths, *small, keys, values, logcum)


def split3(values):
    parts = []
    for _ in range(3):
        part = stored(values)
        parts.append(part)
        values = values - part.astype(jnp.float32)
    return parts


def expert_unit(rows, gate_w, up_w, down_w):
    gate = jnp.minimum(jnp.dot(rows, gate_w, preferred_element_type=jnp.float32), LIMIT)
    up = jnp.clip(jnp.dot(rows, up_w, preferred_element_type=jnp.float32), -LIMIT, LIMIT)
    act = ((up + 1.0) * gate * jax.nn.sigmoid(gate * ALPHA)).astype(jnp.bfloat16)
    return jnp.dot(act, down_w, preferred_element_type=jnp.float32).astype(jnp.bfloat16)


def reach(source, target, sent, landed, device):
    return pltpu.make_async_remote_copy(
        src_ref=source,
        dst_ref=target,
        send_sem=sent,
        recv_sem=landed,
        device_id=(device,),
        device_id_type=pl.DeviceIdType.MESH,
    )


def to_row(column, same):
    return jnp.sum(jnp.where(same, column, 0.0), axis=0, keepdims=True)


def to_column(row, same):
    return jnp.sum(jnp.where(same, row, 0.0), axis=1, keepdims=True)


def rest_body(
    units_total,
    plane,
    packed,
    mixed,
    w_gate,
    w_up,
    w_down,
    d_gate,
    d_up,
    d_down,
    gain,
    branch,
    out,
    rows_s,
    units_s,
    answer_s,
    coef_s,
    square_s,
    squares_s,
    theirs_s,
    joint_s,
    final_s,
    own_sem,
    ag_send,
    ag_recv,
    fw_send,
    fw_recv,
    sq_send,
    sq_recv,
    d2d_send,
    d2d_recv,
    rs_send,
    rs_recv,
):
    kind = jnp.float32
    n = squares_s.shape[0]
    chips = n // 2
    pad = packed.shape[0]
    width = out.shape[1]
    chunk = units_s.shape[1] // pad
    halves = chips // chunk
    size = chunk * pad
    me = lax.axis_index("ep")
    core = lax.rem(me, 2)
    chip = me // 2
    other = chip * 2 + 1 - core
    mine = core * chips
    peer = (1 - core) * chips

    barrier = pltpu.get_barrier_semaphore()

    @pl.loop(1, n)
    def _(k):
        pl.semaphore_signal(
            barrier,
            inc=1,
            device_id=(lax.rem(me + k, n),),
            device_id_type=pl.DeviceIdType.MESH,
        )

    pl.semaphore_wait(barrier, n - 1)

    deep = chips // plane
    level = chip // plane
    spot = lax.rem(chip, plane)

    def before(dz, dp):
        return lax.rem(level - dz + deep, deep) * plane + lax.rem(spot - dp + plane, plane)

    def along(dz):
        to = lax.rem(level + dz, deep) * plane + spot
        k = dz * plane
        return reach(packed, rows_s.at[mine + chip], ag_send.at[k], ag_recv.at[k], to * 2 + core)

    def across(dz, dp):
        to = level * plane + lax.rem(spot + dp, plane)
        k = dz * plane + dp
        slot = rows_s.at[mine + before(dz, 0)]
        return reach(slot, slot, ag_send.at[k], ag_recv.at[k], to * 2 + core)

    def landed(dz, dp):
        slot = rows_s.at[mine + before(dz, dp)]
        k = dz * plane + dp
        return reach(slot, slot, ag_send.at[k], ag_recv.at[k], before(0, dp) * 2 + core)

    def forward(dz, dp):
        slot = rows_s.at[mine + before(dz, dp)]
        k = dz * plane + dp
        return reach(slot, slot, fw_send.at[k], fw_recv.at[k], other)

    def forwarded(dz, dp):
        slot = rows_s.at[peer + before(dz, dp)]
        k = dz * plane + dp
        return reach(slot, slot, fw_send.at[k], fw_recv.at[k], other)

    keep = pltpu.make_async_copy(packed, rows_s.at[mine + chip], own_sem)
    keep.start()

    @pl.loop(1, deep)
    def _(dz):
        along(dz).start()

    keep.wait()

    @pl.loop(1, plane)
    def _(dp):
        across(0, dp).start()

    forward(0, 0).start()

    @pl.loop(1, deep)
    def _(dz):
        landed(dz, 0).wait_recv()

        @pl.loop(1, plane)
        def _(dp):
            across(dz, dp).start()

        forward(dz, 0).start()

    @pl.loop(0, deep)
    def _(dz):
        @pl.loop(1, plane)
        def _(dp):
            landed(dz, dp).wait_recv()
            forward(dz, dp).start()

    @pl.loop(0, deep)
    def _(dz):
        @pl.loop(0, plane)
        def _(dp):
            forwarded(dz, dp).wait_recv()

    first = lax.broadcasted_iota(jnp.int32, (size, size), 0)
    second = lax.broadcasted_iota(jnp.int32, (size, size), 1)
    same = first == second

    def load(at):
        block = rows_s[pl.ds(at * chunk, chunk)]
        return block.astype(kind).reshape(size, block.shape[2])

    @pl.loop(0, 2 * halves)
    def _(at):
        wide = load(at)
        block = wide[:, :width].astype(jnp.bfloat16)
        gate = jnp.dot(block, d_gate[...], preferred_element_type=kind)
        up = jnp.dot(block, d_up[...], preferred_element_type=kind)
        units = (gate * jax.nn.sigmoid(gate) * up).astype(jnp.bfloat16).astype(kind)
        units_s[at] = units
        square_s[at] = to_row(jnp.sum(units * units, axis=1, keepdims=True), same)
        side = wide[:, width:]
        lane = lax.broadcasted_iota(jnp.int32, side.shape, 1)
        picked = jnp.where((side == me.astype(kind)) & (lane < TOPK), 1.0, 0.0)
        weight = jnp.zeros((size, 1), kind)
        for part in (3, 2, 1):
            moved = pltpu.roll(side, side.shape[1] - part * TOPK, 1)
            weight = weight + jnp.sum(picked * moved, axis=1, keepdims=True)
        branch_scale = jax.nn.sigmoid(
            jnp.sum(wide[:, :width] * branch[...], axis=1, keepdims=True)
        )
        coef_s[at] = jnp.where(lane == 0, weight, branch_scale)

    def share(k):
        return reach(
            square_s, squares_s.at[k], sq_send.at[k], sq_recv.at[k], lax.rem(me + k, n)
        )

    @pl.loop(1, n)
    def _(k):
        share(k).start()

    @pl.loop(0, 2 * halves)
    def _(at):
        block = load(at)[:, :width].astype(jnp.bfloat16)
        answer_s[at] = expert_unit(block, w_gate[...], w_up[...], w_down[...])

    @pl.loop(1, n)
    def _(k):
        share(k).wait_recv()

    squares_s[0] = square_s[...]
    totals = jnp.sum(squares_s[...], axis=0)
    square_rows = lax.rsqrt(totals / units_total + EPS)
    squares_s[0] = square_rows

    def partial(at):
        scale = to_column(squares_s[0, at], same)
        hidden = (units_s[at] * scale * gain[...]).astype(jnp.bfloat16)
        dense = jnp.dot(hidden, d_down[...], preferred_element_type=kind)
        coef = coef_s[at]
        routed = coef[:, 0:1] * answer_s[at].astype(kind)
        return (routed + coef[:, 1:2] * dense).reshape(chunk, pad, width)

    def cross(half):
        part = pl.ds(half * chunk, chunk)
        return reach(theirs_s.at[part], joint_s.at[part], d2d_send.at[half], d2d_recv.at[half], other)

    def back(dz, dp):
        k = dz * plane + dp
        slot = joint_s.at[before(dz, dp)]
        return reach(slot, final_s.at[k], rs_send.at[k], rs_recv.at[k], before(0, dp) * 2 + core)

    def down(dz):
        k = dz * plane
        to = before(dz, 0)
        return reach(joint_s.at[to], final_s.at[k], rs_send.at[k], rs_recv.at[k], to * 2 + core)

    def collected(dz):
        total = joint_s[before(dz, 0)].astype(kind)
        for dp in range(1, plane):
            back(dz, dp).wait_recv()
            total = total + final_s[dz * plane + dp].astype(kind)
        return total

    @pl.loop(0, halves)
    def _(half):
        theirs_s[pl.ds(half * chunk, chunk)] = partial((1 - core) * halves + half).astype(
            jnp.bfloat16
        )
        cross(half).start()

    @pl.loop(0, halves)
    def _(half):
        part = pl.ds(half * chunk, chunk)
        own = partial(core * halves + half)
        cross(half).wait_recv()
        joint_s[part] = (own + joint_s[part].astype(kind)).astype(jnp.bfloat16)

    @pl.loop(1, deep + 1)
    def _(step):
        @pl.loop(1, plane)
        def _(dp):
            back(lax.rem(step, deep), dp).start()

    @pl.loop(1, deep)
    def _(dz):
        joint_s[before(dz, 0)] = collected(dz).astype(jnp.bfloat16)
        down(dz).start()

    total = collected(0)
    for dz in range(1, deep):
        down(dz).wait_recv()
        total = total + final_s[dz * plane].astype(kind)
    result = mixed[...].astype(kind) + total[: mixed.shape[0]]
    out[...] = result.astype(jnp.bfloat16)

    @pl.loop(1, deep)
    def _(dz):
        along(dz).wait_send()
        down(dz).wait_send()

    @pl.loop(0, deep)
    def _(dz):
        forward(dz, 0).wait_send()

        @pl.loop(1, plane)
        def _(dp):
            across(dz, dp).wait_send()
            back(dz, dp).wait_send()
            forward(dz, dp).wait_send()

    @pl.loop(1, n)
    def _(k):
        share(k).wait_send()

    @pl.loop(0, halves)
    def _(half):
        cross(half).wait_send()


def rest(n, packed, mixed, w_gate, w_up, w_down, d_gate, d_up, d_down, gain, branch, units_total):
    pad = packed.shape[0]
    width = mixed.shape[1]
    local = d_gate.shape[1]
    chips = n // 2
    chunk = max(size for size in (1, 2, 4, 8) if chips % size == 0)
    halves = chips // chunk
    plane = chips // 4 if chips % 4 == 0 else chips
    size = chunk * pad
    half_type = jnp.bfloat16
    vmem = pl.BlockSpec(memory_space=pltpu.VMEM)
    dma = pltpu.SemaphoreType.DMA
    return pl.pallas_call(
        functools.partial(rest_body, units_total, plane),
        out_shape=jax.ShapeDtypeStruct(mixed.shape, half_type),
        in_specs=[vmem] * 10,
        out_specs=vmem,
        scratch_shapes=[
            pltpu.VMEM((n, *packed.shape), half_type),
            pltpu.VMEM((2 * halves, size, local), jnp.float32),
            pltpu.VMEM((2 * halves, size, width), half_type),
            pltpu.VMEM((2 * halves, size, 128), jnp.float32),
            pltpu.VMEM((2 * halves, 1, size), jnp.float32),
            pltpu.VMEM((n, 2 * halves, 1, size), jnp.float32),
            pltpu.VMEM((chips, pad, width), half_type),
            pltpu.VMEM((chips, pad, width), half_type),
            pltpu.VMEM((chips, pad, width), half_type),
            dma,
            dma((chips,)),
            dma((chips,)),
            dma((chips,)),
            dma((chips,)),
            dma((n,)),
            dma((n,)),
            dma((halves,)),
            dma((halves,)),
            dma((chips,)),
            dma((chips,)),
        ],
        compiler_params=pltpu.CompilerParams(
            collective_id=0, has_side_effects=True, vmem_limit_bytes=62 * 1024 * 1024
        ),
        name="rest",
    )(packed, mixed, w_gate, w_up, w_down, d_gate, d_up, d_down, gain, branch)


def fast_body(
    units_total,
    tokens_h,
    gain_h,
    w_query_h,
    w_key_h,
    w_value_h,
    w_forget_h,
    bias_h,
    w_out_h,
    keys_h,
    values_h,
    logcum_h,
    lengths_h,
    gain_next_h,
    ids_h,
    weights_h,
    e_gate_h,
    e_up_h,
    e_down_h,
    d_gate_h,
    d_up_h,
    d_down_h,
    d_gain_h,
    branch_h,
    out,
    tokens_s,
    gain_s,
    w_qkv_s,
    w_forget_s,
    bias_s,
    w_out_s,
    keys_s,
    values_s,
    logcum_s,
    lengths_s,
    gain_next_s,
    ids_s,
    weights_s,
    e_gate_s,
    e_up_s,
    e_down_s,
    d_in_s,
    d_down_s,
    d_gain_s,
    branch_s,
    query_s,
    key_s,
    value_s,
    forget_s,
    own_s,
    heads_s,
    mixed_s,
    fold_s,
    rows_s,
    x_s,
    spread_s,
    hidden_s,
    branch_col_s,
    square_s,
    squares_s,
    info_s,
    infos_s,
    scale_s,
    coef_s,
    answer_s,
    part_s,
    joint_s,
    pair_s,
    first_a,
    first_b,
    turn_a,
    turn_b,
    second_a,
    second_b,
    level_s,
    levels_s,
    ld,
    kv_sem,
    z_send,
    z_recv,
    x_send,
    x_recv,
    y_send,
    y_recv,
    da_send,
    da_recv,
    db_send,
    db_recv,
    f_send,
    f_recv,
    i_send,
    i_recv,
    q_send,
    q_recv,
    c_send,
    c_recv,
    s1a_send,
    s1a_recv,
    s1b_send,
    s1b_recv,
    s2a_send,
    s2a_recv,
    s2b_send,
    s2b_recv,
    zz_send,
    zz_recv,
):
    kind = jnp.float32
    half_type = jnp.bfloat16
    n = squares_s.shape[0]
    chips = n // 2
    deep = x_s.shape[0]
    plane = chips // deep
    side = 2
    seqs, width = tokens_s.shape
    block, wide = rows_s.shape[1:]
    cut = wide // 2
    fold = wide - width
    folds = width // fold
    spare = seqs - block
    members = 2 * plane
    bulk = members * block
    tail = members * spare
    length, pair = keys_s.shape[1:]
    group = HEADS // KV_HEADS
    tiles = HEADS * HEAD_DIM // pair
    me = lax.axis_index("ep")
    core = lax.rem(me, 2)
    chip = me // 2
    other = chip * 2 + 1 - core
    level = chip // plane
    spot = lax.rem(chip, plane)
    row = spot // side
    col = lax.rem(spot, side)

    barrier = pltpu.get_barrier_semaphore()

    @pl.loop(1, n)
    def _(k):
        pl.semaphore_signal(
            barrier,
            inc=1,
            device_id=(lax.rem(me + k, n),),
            device_id_type=pl.DeviceIdType.MESH,
        )

    heads_wide = HEADS * HEAD_DIM
    loads = [
        (tokens_h, tokens_s),
        (gain_h, gain_s),
        (w_query_h, w_qkv_s.at[:, 0:heads_wide]),
        (w_key_h, w_qkv_s.at[:, heads_wide : heads_wide + pair]),
        (w_value_h, w_qkv_s.at[:, heads_wide + pair : heads_wide + 2 * pair]),
        (w_forget_h, w_forget_s),
        (bias_h, bias_s),
        (lengths_h, lengths_s),
        (logcum_h, logcum_s),
        (ids_h, ids_s),
        (weights_h, weights_s),
    ]
    later = [
        (w_out_h, w_out_s),
        (gain_next_h, gain_next_s),
        (d_gate_h, d_in_s.at[:, 0:pair]),
        (d_up_h, d_in_s.at[:, pair : 2 * pair]),
        (d_gain_h, d_gain_s),
        (branch_h, branch_s),
        (e_gate_h.at[0], e_gate_s),
        (e_up_h.at[0], e_up_s),
        (e_down_h.at[0], e_down_s),
        (d_down_h, d_down_s),
    ]
    copies = [
        pltpu.make_async_copy(source, target, ld.at[at])
        for at, (source, target) in enumerate(loads + later)
    ]
    batch = seqs // kv_sem.shape[1]
    groups = kv_sem.shape[1]

    def cached(at):
        part = pl.ds(at * batch, batch)
        return (
            pltpu.make_async_copy(keys_h.at[part], keys_s.at[part], kv_sem.at[0, at]),
            pltpu.make_async_copy(values_h.at[part], values_s.at[part], kv_sem.at[1, at]),
        )

    for copy in copies[: len(loads)]:
        copy.start()

    @pl.loop(0, groups)
    def _(at):
        for copy in cached(at):
            copy.start()

    for copy in copies[len(loads) :]:
        copy.start()

    for at in range(9):
        copies[at].wait()

    normed = normalize(tokens_s[...].astype(kind), gain_s[...]).astype(half_type)
    product = jnp.dot(normed, w_qkv_s[...], preferred_element_type=kind)
    product = product.astype(half_type).astype(kind)
    key_s[...] = product[:, heads_wide : heads_wide + pair]
    value_s[...] = product[:, heads_wide + pair : heads_wide + 2 * pair]
    lane = lax.broadcasted_iota(jnp.int32, (seqs, pair), 1)
    for head in range(HEADS):
        piece = product[:, head // 2 * pair : (head // 2 + 1) * pair]
        if head % 2 != head // group:
            piece = pltpu.roll(piece, HEAD_DIM, 1)
        piece = jnp.where(lane // HEAD_DIM == head // group, piece, 0.0)
        query_s[pl.ds(head, seqs, stride=HEADS), :] = piece
    forget = lax.dot_general(
        w_forget_s[...], normed, (((1,), (1,)), ((), ())), preferred_element_type=kind
    )
    eye = lax.broadcasted_iota(jnp.int32, (HEADS, HEADS), 0)
    eye = eye == lax.broadcasted_iota(jnp.int32, (HEADS, HEADS), 1)
    forget = forget + to_column(bias_s[...], eye)
    forget_s[...] = jnp.minimum(forget, 0.0) - jnp.log1p(jnp.exp(-jnp.abs(forget)))

    seq_lane = lax.broadcasted_iota(jnp.int32, forget_s.shape, 1)
    position = lax.broadcasted_iota(jnp.int32, (HEADS, length), 1)
    unit = HEAD_DIM ** (-0.5)

    @pl.loop(0, groups)
    def _(at):
        for copy in cached(at):
            copy.wait()
        scores_all = []
        own_all = []
        for item in range(batch):
            seq = at * batch + item
            query = query_s[pl.ds(pl.multiple_of(seq * HEADS, HEADS), HEADS), :]
            own = jnp.sum(query * key_s[pl.ds(seq, 1), :], axis=1, keepdims=True) * unit
            forget = jnp.sum(jnp.where(seq_lane == seq, forget_s[...], 0.0), axis=1, keepdims=True)
            cum = logcum_s[seq]
            live = lengths_s[seq]
            last = jnp.sum(jnp.where(position == live - 1, cum, 0.0), axis=1, keepdims=True)
            scores = lax.dot_general(
                query.astype(half_type),
                keys_s[seq],
                (((1,), (1,)), ((), ())),
                preferred_element_type=kind,
            )
            scores = scores * unit + ((last + forget) - cum)
            scores_all.append(jnp.where(position < live, scores, -jnp.inf))
            own_all.append(own)
        scores = jnp.concatenate(scores_all, axis=0)
        own = jnp.concatenate(own_all, axis=0)
        top = jnp.maximum(jnp.max(scores, axis=1, keepdims=True), own)
        expo = jnp.exp(scores - top)
        own_expo = jnp.exp(own - top)
        total = jnp.sum(expo, axis=1, keepdims=True) + own_expo
        share = (expo / total).astype(half_type)
        own_share = (own_expo / total).astype(half_type).astype(kind)
        for item in range(batch):
            seq = at * batch + item
            part = slice(item * HEADS, (item + 1) * HEADS)
            result = jnp.dot(share[part], values_s[seq], preferred_element_type=kind)
            result = result + own_share[part] * value_s[pl.ds(seq, 1), :]
            heads_s[pl.ds(pl.multiple_of(seq * HEADS, HEADS), HEADS), :] = result

    for at in range(9, len(loads) + 6):
        copies[at].wait()

    found = [heads_s[pl.ds(head, seqs, stride=HEADS), :] for head in range(HEADS)]
    pieces = []
    for tile in range(tiles):
        left, right = found[2 * tile], found[2 * tile + 1]
        if 2 * tile // group:
            left = pltpu.roll(left, HEAD_DIM, 1)
        else:
            right = pltpu.roll(right, HEAD_DIM, 1)
        pieces.append(jnp.where(lane < HEAD_DIM, left, right))
    attended = jnp.concatenate(pieces, axis=1).astype(half_type)
    mixed = tokens_s[...].astype(kind) + jnp.dot(
        attended, w_out_s[...], preferred_element_type=kind
    )
    mixed = mixed.astype(half_type).astype(kind)
    mixed_s[...] = mixed
    routed = normalize(mixed, gain_next_s[...])

    def slot(at, which, place):
        return (at * 2 + which) * plane + place

    home = slot(level, core, spot)
    for part in range(folds):
        fold_s[pl.ds(part * spare, spare), :] = routed[block:, part * fold : (part + 1) * fold]
    rows_s[home, :, 0:width] = routed[:block].astype(half_type)
    rows_s[home, :, width:wide] = fold_s[...].astype(half_type)

    experts = lax.broadcasted_iota(jnp.int32, (n, seqs), 0)
    matched = jnp.zeros((n, seqs), kind)
    for at in range(TOPK):
        chosen = ids_s[at : at + 1, :] == experts
        matched = matched + jnp.where(chosen, weights_s[at : at + 1, :], 0.0)
    token = lax.broadcasted_iota(jnp.int32, (seqs, bulk), 0)
    spread = lax.broadcasted_iota(jnp.int32, (seqs, bulk), 1)
    member = core * plane + spot
    exact = lax.Precision.HIGHEST

    def placed(place):
        return jnp.dot(
            matched, jnp.where(place, 1.0, 0.0), preferred_element_type=kind, precision=exact
        )

    main_row = placed((token < block) & (spread == member * block + token))
    tail_row = placed(
        (token >= block) & (spread == level * tail + (token - block) * members + member)
    )
    line = lax.broadcasted_iota(jnp.int32, square_s.shape, 0)
    for at in range(n):
        info_s[at] = jnp.where(
            line == level,
            main_row[at : at + 1, :],
            jnp.where(line == deep, tail_row[at : at + 1, :], 0.0),
        )

    def device(z, y, x, which):
        return ((z * side + y) * side + x) * 2 + which

    spot_x = row * side + 1 - col
    spot_y = (1 - row) * side + col
    spot_d = (1 - row) * side + 1 - col
    near_x = device(level, row, 1 - col, core)
    near_y = device(level, 1 - row, col, core)

    def along(at, way):
        place = rows_s.at[slot(at, core, spot)]
        to = device(level + (1 if way else -1), row, col, core)
        return reach(place, place, z_send.at[way, at], z_recv.at[at], to)

    def beside(at, place):
        here = rows_s.at[slot(at, core, place)]
        return reach(here, here, x_send.at[at], x_recv.at[at], near_x)

    def above(at, place):
        here = rows_s.at[slot(at, core, place)]
        return reach(here, here, y_send.at[at], y_recv.at[at], near_y)

    def relay_a(at, place):
        here = rows_s.at[slot(at, core, place), :, 0:cut]
        return reach(here, here, da_send.at[at], da_recv.at[at], near_y)

    def relay_b(at, place):
        here = rows_s.at[slot(at, core, place), :, cut:wide]
        return reach(here, here, db_send.at[at], db_recv.at[at], near_x)

    def across(at, which, place):
        here = rows_s.at[slot(at, which, place)]
        return reach(here, here, f_send.at[at, place], f_recv.at[at, place], other)

    balance = jnp.minimum(level, deep - 1 - level)
    lean = jnp.where(2 * level < deep - 1, 1, -1)

    def ordered(j):
        paired = jnp.where(lax.rem(j, 2) == 1, -1, 1) * ((j + 1) // 2)
        single = lean * (j - balance)
        return level + jnp.where(j <= 2 * balance, paired, single)

    def inform(k):
        to = lax.rem(me + k, n)
        return reach(info_s.at[to], infos_s.at[k], i_send.at[k], i_recv.at[k], to)

    def informed(k):
        return reach(info_s.at[0], infos_s.at[k], i_send.at[k], i_recv.at[k], lax.rem(me + k, n))

    def share(k):
        return reach(square_s, squares_s.at[k], q_send.at[k], q_recv.at[k], lax.rem(me + k, n))

    pl.semaphore_wait(barrier, n - 1)

    def spread_native(at):
        beside(at, spot).start()
        above(at, spot).start()
        across(at, core, spot).start()

    @pl.when(level + 1 < deep)
    def _():
        along(level, 1).start()

    @pl.when(level > 0)
    def _():
        along(level, 0).start()

    spread_native(level)

    @pl.loop(1, n)
    def _(k):
        inform(k).start()

    infos_s[0] = info_s[me]

    for at in range(len(loads) + 6, len(loads) + len(later)):
        copies[at].wait()

    ones = jnp.ones((8, pair), kind)
    same_bulk = lax.broadcasted_iota(jnp.int32, (bulk, bulk), 0)
    same_bulk = same_bulk == lax.broadcasted_iota(jnp.int32, (bulk, bulk), 1)
    tail_at = lax.broadcasted_iota(jnp.int32, (tail, bulk), 1)
    tail_of = lax.broadcasted_iota(jnp.int32, (tail, bulk), 0)

    square_s[...] = jnp.zeros_like(square_s)

    @pl.loop(0, deep)
    def _(j):
        at = ordered(j)
        beside(at, spot_x).wait_recv()
        relay_a(at, spot_x).start()
        across(at, core, spot_x).start()
        above(at, spot_y).wait_recv()
        relay_b(at, spot_y).start()
        across(at, core, spot_y).start()

        @pl.when(j + 1 < deep)
        def _():
            following = ordered(j + 1)
            along(following, 0).wait_recv()

            @pl.when((following < level) & (level + 1 < deep))
            def _():
                along(following, 1).start()

            @pl.when((following > level) & (level > 0))
            def _():
                along(following, 0).start()

            spread_native(following)

        relay_a(at, spot_d).wait_recv()
        relay_b(at, spot_d).wait_recv()
        across(at, core, spot_d).start()
        for place in range(plane):
            across(at, 1 - core, place).wait_recv()

        part = pl.ds(at * members, members)
        x_s[at, 0:bulk, :] = rows_s[part, :, 0:width].reshape(bulk, width)
        folded = rows_s[part, :, width:wide].astype(kind).reshape(bulk, fold)
        for tile in range(fold // pair):
            spread_s[tile] = folded[:, tile * pair : (tile + 1) * pair]
        for piece in range(folds):
            for tile in range(fold // pair):
                lanes = slice(piece * fold + tile * pair, piece * fold + (tile + 1) * pair)
                taken = [
                    spread_s[tile, pl.ds(piece * spare + extra, members, stride=block), :]
                    for extra in range(spare)
                ]
                x_s[at, bulk : bulk + tail, lanes] = jnp.concatenate(taken, axis=0).astype(
                    half_type
                )
        values = x_s[at]
        inner = jnp.sum(values.astype(kind) * branch_s[...], axis=1, keepdims=True)
        branch_col_s[at] = jnp.broadcast_to(jax.nn.sigmoid(inner), (bulk + tail, pair))
        both = jnp.dot(values, d_in_s[...], preferred_element_type=kind)
        gate, up = both[:, 0:pair], both[:, pair : 2 * pair]
        units = (gate * jax.nn.sigmoid(gate) * up).astype(half_type).astype(kind)
        hidden_s[at] = (units * d_gain_s[pl.ds(me, 1), :]).astype(half_type)
        squares = lax.dot_general(
            ones,
            units * units,
            (((1,), (1,)), ((), ())),
            preferred_element_type=kind,
            precision=exact,
        )
        square_s[pl.ds(at, 1), :] = squares[0:1, 0:bulk]
        ends = jnp.sum(units[bulk:] * units[bulk:], axis=1, keepdims=True)
        ends = jnp.sum(jnp.where(tail_at == at * tail + tail_of, ends, 0.0), axis=0, keepdims=True)
        square_s[deep : deep + 1, :] = square_s[deep : deep + 1, :] + ends

        @pl.when(j + 1 == deep)
        def _():
            @pl.loop(1, n)
            def _(k):
                share(k).start()

        gate = jnp.minimum(jnp.dot(values, e_gate_s[...], preferred_element_type=kind), LIMIT)
        up = jnp.clip(jnp.dot(values, e_up_s[...], preferred_element_type=kind), -LIMIT, LIMIT)
        act = ((up + 1.0) * gate * jax.nn.sigmoid(gate * ALPHA)).astype(half_type)
        answer_s[at] = jnp.dot(act, e_down_s[...], preferred_element_type=kind).astype(half_type)

    @pl.loop(1, n)
    def _(k):
        informed(k).wait_recv()
        share(k).wait_recv()

    coef_s[...] = jnp.sum(infos_s[...], axis=0)
    squares_s[0] = square_s[...]
    scale_s[...] = lax.rsqrt(jnp.sum(squares_s[...], axis=0) / units_total + EPS)

    def columns(ref, at):
        main = to_column(ref[pl.ds(at, 1), :], same_bulk)
        ends = jnp.where(tail_at == at * tail + tail_of, ref[deep : deep + 1, :], 0.0)
        return main, jnp.sum(ends, axis=1, keepdims=True)

    def cross(at):
        return reach(
            part_s.at[at, pl.ds((1 - core) * plane, plane)],
            joint_s.at[at],
            c_send.at[at],
            c_recv.at[at],
            other,
        )

    def first(at, k):
        return (
            reach(
                pair_s.at[at, k * side + 1 - col, :, 0:cut],
                first_a.at[at, k],
                s1a_send.at[at, k],
                s1a_recv.at[at, k],
                near_x,
            ),
            reach(
                pair_s.at[at, (1 - row) * side + k, :, cut:wide],
                first_b.at[at, k],
                s1b_send.at[at, k],
                s1b_recv.at[at, k],
                near_y,
            ),
        )

    def second(at):
        return (
            reach(turn_a.at[at], second_a.at[at], s2a_send.at[at], s2a_recv.at[at], near_y),
            reach(turn_b.at[at], second_b.at[at], s2b_send.at[at], s2b_recv.at[at], near_x),
        )

    def home_to(at):
        return reach(
            level_s.at[at],
            levels_s.at[level],
            zz_send.at[at],
            zz_recv.at[level],
            device(at, row, col, core),
        )

    def home_from(at):
        return reach(
            level_s.at[at],
            levels_s.at[at],
            zz_send.at[at],
            zz_recv.at[at],
            device(at, row, col, core),
        )

    @pl.loop(0, deep + 3)
    def _(step):
        @pl.when(step < deep)
        def _():
            at = ordered(deep - 1 - step)
            dense = jnp.dot(hidden_s[at], d_down_s[...], preferred_element_type=kind)
            weight, weight_end = columns(coef_s, at)
            scale, scale_end = columns(scale_s, at)
            twice = branch_col_s[at, :, 0:1]
            main = weight * answer_s[at, 0:bulk, :].astype(kind)
            main = main + (scale * twice[0:bulk]) * dense[0:bulk]
            ends = weight_end * answer_s[at, bulk : bulk + tail, :].astype(kind)
            ends = ends + (scale_end * twice[bulk:]) * dense[bulk:]
            part_s[at, :, :, 0:width] = main.astype(half_type).reshape(members, block, width)
            for piece in range(folds):
                for tile in range(fold // pair):
                    first_lane = piece * fold + tile * pair
                    for extra in range(spare):
                        spread_s[tile, pl.ds(piece * spare + extra, members, stride=block), :] = (
                            ends[
                                extra * members : (extra + 1) * members,
                                first_lane : first_lane + pair,
                            ]
                        )
            for tile in range(fold // pair):
                part_s[at, :, :, width + tile * pair : width + (tile + 1) * pair] = (
                    spread_s[tile].astype(half_type).reshape(members, block, pair)
                )
            cross(at).start()

        @pl.when((step >= 1) & (step < deep + 1))
        def _():
            at = ordered(deep - step)
            cross(at).wait_recv()
            mine = part_s[at, pl.ds(core * plane, plane)].astype(kind)
            pair_s[at] = (mine + joint_s[at].astype(kind)).astype(half_type)
            for k in range(side):
                for copy in first(at, k):
                    copy.start()

        @pl.when((step >= 2) & (step < deep + 2))
        def _():
            at = ordered(deep + 1 - step)
            for k in range(side):
                for copy in first(at, k):
                    copy.wait_recv()
            turned = pair_s[at, spot_y, :, 0:cut].astype(kind) + first_a[at, 1 - row].astype(kind)
            turn_a[at] = turned.astype(half_type)
            turned = pair_s[at, spot_x, :, cut:wide].astype(kind) + first_b[at, 1 - col].astype(kind)
            turn_b[at] = turned.astype(half_type)
            for copy in second(at):
                copy.start()

        @pl.when(step >= 3)
        def _():
            at = ordered(deep + 2 - step)
            for copy in second(at):
                copy.wait_recv()
            total = pair_s[at, spot, :, 0:cut].astype(kind) + first_a[at, row].astype(kind)
            total = total + second_a[at].astype(kind)
            level_s[at, :, 0:cut] = total.astype(half_type)
            total = pair_s[at, spot, :, cut:wide].astype(kind) + first_b[at, col].astype(kind)
            total = total + second_b[at].astype(kind)
            level_s[at, :, cut:wide] = total.astype(half_type)

            @pl.when(step < deep + 2)
            def _():
                home_to(at).start()

    total = level_s[level].astype(kind)
    for j in range(1, deep):
        at = ordered(j)
        home_from(at).wait_recv()
        total = total + levels_s[at].astype(kind)
    out[0:block, :] = (mixed_s[0:block, :] + total[:, 0:width]).astype(half_type)
    fold_s[...] = total[:, width:wide]
    for part in range(folds):
        lanes = slice(part * fold, (part + 1) * fold)
        ends = mixed_s[block:seqs, lanes] + fold_s[pl.ds(part * spare, spare), :]
        out[block:seqs, lanes] = ends.astype(half_type)

    @pl.loop(0, deep)
    def _(at):
        @pl.when((at <= level) & (level + 1 < deep))
        def _():
            along(at, 1).wait_send()

        @pl.when((at >= level) & (level > 0))
        def _():
            along(at, 0).wait_send()

        beside(at, spot).wait_send()
        above(at, spot).wait_send()
        relay_a(at, spot_x).wait_send()
        relay_b(at, spot_y).wait_send()
        for place in range(plane):
            across(at, core, place).wait_send()
        cross(at).wait_send()
        for k in range(side):
            for copy in first(at, k):
                copy.wait_send()
        for copy in second(at):
            copy.wait_send()

        @pl.when(at != level)
        def _():
            home_to(at).wait_send()

    @pl.loop(1, n)
    def _(k):
        informed(k).wait_send()
        share(k).wait_send()


def fast(n, deep, arrays, units_total):
    (tokens, keys, logcum, e_gate, e_down, d_gate, d_gain) = (
        arrays[0],
        arrays[8],
        arrays[10],
        arrays[15],
        arrays[17],
        arrays[18],
        arrays[21],
    )
    seqs, width = tokens.shape
    length, pair = keys.shape[1:]
    hidden = e_gate.shape[2]
    local = d_gate.shape[1]
    chips = n // 2
    plane = chips // deep
    block = seqs // 16 * 16
    spare = seqs - block
    wide = width + spare * width // block
    fold = wide - width
    cut = wide // 2
    members = 2 * plane
    bulk = members * block
    tail = members * spare
    heads_wide = HEADS * HEAD_DIM
    half_type = jnp.bfloat16
    kind = jnp.float32
    dma = pltpu.SemaphoreType.DMA
    groups = 6
    vmem = pltpu.VMEM
    scratch = [
        vmem((seqs, width), half_type),
        vmem((1, width), kind),
        vmem((width, heads_wide + 2 * pair), half_type),
        vmem((HEADS, width), half_type),
        vmem((1, HEADS), kind),
        vmem((heads_wide, width), half_type),
        vmem((seqs, length, pair), half_type),
        vmem((seqs, length, pair), half_type),
        vmem((seqs, HEADS, length), kind),
        pltpu.SMEM((seqs,), jnp.int32),
        vmem((1, width), kind),
        vmem((TOPK, seqs), jnp.int32),
        vmem((TOPK, seqs), kind),
        vmem((width, hidden), half_type),
        vmem((width, hidden), half_type),
        vmem((hidden, width), half_type),
        vmem((width, 2 * local), half_type),
        vmem((local, width), half_type),
        vmem(d_gain.shape, kind),
        vmem((1, width), kind),
        vmem((seqs * HEADS, pair), kind),
        vmem((seqs, pair), kind),
        vmem((seqs, pair), kind),
        vmem((HEADS, seqs), kind),
        vmem((8, pair), kind),
        vmem((seqs * HEADS, pair), kind),
        vmem((seqs, width), kind),
        vmem((block, fold), kind),
        vmem((n, block, wide), half_type),
        vmem((deep, bulk + tail, width), half_type),
        vmem((fold // pair, bulk, pair), kind),
        vmem((deep, bulk + tail, local), half_type),
        vmem((deep, bulk + tail, pair), kind),
        vmem((8, bulk), kind),
        vmem((n, 8, bulk), kind),
        vmem((n, 8, bulk), kind),
        vmem((n, 8, bulk), kind),
        vmem((8, bulk), kind),
        vmem((8, bulk), kind),
        vmem((deep, bulk + tail, width), half_type),
        vmem((deep, members, block, wide), half_type),
        vmem((deep, plane, block, wide), half_type),
        vmem((deep, plane, block, wide), half_type),
        vmem((deep, 2, block, cut), half_type),
        vmem((deep, 2, block, cut), half_type),
        vmem((deep, block, cut), half_type),
        vmem((deep, block, cut), half_type),
        vmem((deep, block, cut), half_type),
        vmem((deep, block, cut), half_type),
        vmem((deep, block, wide), half_type),
        vmem((deep, block, wide), half_type),
        dma((21,)),
        dma((2, groups)),
        dma((2, deep)),
        dma((deep,)),
        dma((deep,)),
        dma((deep,)),
        dma((deep,)),
        dma((deep,)),
        dma((deep,)),
        dma((deep,)),
        dma((deep,)),
        dma((deep,)),
        dma((deep, plane)),
        dma((deep, plane)),
        dma((n,)),
        dma((n,)),
        dma((n,)),
        dma((n,)),
        dma((deep,)),
        dma((deep,)),
        dma((deep, 2)),
        dma((deep, 2)),
        dma((deep, 2)),
        dma((deep, 2)),
        dma((deep,)),
        dma((deep,)),
        dma((deep,)),
        dma((deep,)),
        dma((deep,)),
        dma((deep,)),
    ]
    return pl.pallas_call(
        functools.partial(fast_body, units_total),
        out_shape=jax.ShapeDtypeStruct(tokens.shape, half_type),
        in_specs=[pl.BlockSpec(memory_space=pl.ANY)] * len(arrays),
        out_specs=pl.BlockSpec(memory_space=pltpu.VMEM),
        scratch_shapes=scratch,
        compiler_params=pltpu.CompilerParams(
            collective_id=0, has_side_effects=True, vmem_limit_bytes=62 * 1024 * 1024
        ),
        name="layer",
    )(*arrays)


def shards(
    tokens,
    attn_norm_gain,
    w_query,
    w_key,
    w_value,
    w_forget,
    forget_bias,
    w_attn_out,
    cache_keys,
    cache_values,
    cache_logcum,
    cache_lengths,
    expert_norm_gain,
    expert_ids,
    expert_weights,
    w_expert_gate,
    w_expert_up,
    w_expert_down,
    w_dense_gate,
    w_dense_up,
    w_dense_down,
    dense_norm_gain,
    branch_gate,
):
    n = lax.axis_size("ep")
    deep = 4
    seqs, width = tokens.shape
    local = w_dense_gate.shape[1]
    spare = seqs % 16
    fits = n == 8 * deep and local == cache_keys.shape[2] and 0 < spare and spare * width % 2048 == 0
    if fits and seqs // 16 == 1:
        return fast(
            n,
            deep,
            (
                tokens,
                attn_norm_gain[None, :],
                w_query,
                w_key,
                w_value,
                w_forget.T,
                forget_bias[None, :],
                w_attn_out,
                cache_keys,
                cache_values,
                cache_logcum,
                cache_lengths,
                expert_norm_gain[None, :],
                expert_ids.T,
                expert_weights.T,
                w_expert_gate,
                w_expert_up,
                w_expert_down,
                w_dense_gate,
                w_dense_up,
                w_dense_down,
                dense_norm_gain.reshape(n, local),
                branch_gate[None, :],
            ),
            dense_norm_gain.shape[0],
        )
    mixed, routed_in = front(
        tokens,
        attn_norm_gain,
        w_query,
        w_key,
        w_value,
        w_forget,
        forget_bias,
        w_attn_out,
        cache_keys,
        cache_values,
        cache_logcum,
        cache_lengths,
        expert_norm_gain,
    )
    n = lax.axis_size("ep")
    me = lax.axis_index("ep")
    seqs = tokens.shape[0]
    extra = jnp.concatenate([expert_ids.astype(jnp.bfloat16), *split3(expert_weights)], axis=1)
    packed = jnp.concatenate([routed_in, jnp.pad(extra, ((0, 0), (0, 128 - 4 * TOPK)))], axis=1)
    packed = jnp.pad(packed, ((0, -seqs % 8), (0, 0)))
    local = w_dense_gate.shape[1]
    gain = lax.dynamic_slice_in_dim(dense_norm_gain, me * local, local, 0)
    return rest(
        n,
        packed,
        mixed,
        w_expert_gate[0],
        w_expert_up[0],
        w_expert_down[0],
        w_dense_gate,
        w_dense_up,
        w_dense_down,
        gain[None, :],
        branch_gate[None, :],
        dense_norm_gain.shape[0],
    )


def solution(mesh):
    in_specs = (
        P("ep", None),
        P(),
        P(),
        P(),
        P(),
        P(),
        P(),
        P(),
        P("ep", None, None),
        P("ep", None, None),
        P("ep", None, None),
        P("ep"),
        P(),
        P("ep", None),
        P("ep", None),
        P("ep", None, None),
        P("ep", None, None),
        P("ep", None, None),
        P(None, "ep"),
        P(None, "ep"),
        P("ep", None),
        P(),
        P(),
    )
    out_specs = P("ep", None)
    return jax.shard_map(shards, mesh=mesh, in_specs=in_specs, out_specs=out_specs, check_vma=False)
```

```python
import functools

import jax
import jax.numpy as jnp
from jax import lax
from jax.experimental import pallas as pl
from jax.experimental.pallas import tpu as pltpu
from jax.sharding import PartitionSpec as P

HEADS = 8
KV_HEADS = 2
HEAD_DIM = 64
TOPK = 6


EPS = 1e-06
LIMIT = 7.0
ALPHA = 1.702


def normalize(values, gain):
    return values * lax.rsqrt(jnp.mean(values * values, axis=-1, keepdims=True) + EPS) * gain


def stored(values):
    return lax.optimization_barrier(values.astype(jnp.bfloat16))


def front_body(
    lengths,
    tokens,
    gain_ref,
    w_query,
    w_key,
    w_value,
    w_forget,
    bias,
    w_out,
    gain_next,
    keys,
    values,
    logcum,
    mixed_ref,
    routed_ref,
    query_s,
    key_s,
    value_s,
    forget_s,
    attended_s,
):
    step = pl.program_id(0)
    batch, length, pair = keys.shape
    rows = jnp.float32
    group = HEADS // KV_HEADS
    tiles = HEADS * HEAD_DIM // pair

    @pl.when(step == 0)
    def _():
        normed = normalize(tokens[...].astype(rows), gain_ref[...]).astype(jnp.bfloat16)
        for weight, kept in ((w_key, key_s), (w_value, value_s)):
            product = jnp.dot(normed, weight[...], preferred_element_type=rows)
            kept[...] = product.astype(jnp.bfloat16).astype(rows)
        product = jnp.dot(normed, w_query[...], preferred_element_type=rows)
        product = product.astype(jnp.bfloat16).astype(rows)
        for tile in range(tiles):
            query_s[tile] = product[:, tile * pair : (tile + 1) * pair]
        forget = lax.dot_general(
            w_forget[...], normed, (((1,), (1,)), ((), ())), preferred_element_type=rows
        )
        forget = forget + bias[...]
        forget_s[...] = jnp.minimum(forget, 0.0) - jnp.log1p(jnp.exp(-jnp.abs(forget)))

    lane = lax.broadcasted_iota(jnp.int32, (HEADS, pair), 1)
    head = lax.broadcasted_iota(jnp.int32, (HEADS, pair), 0)
    odd = lane // HEAD_DIM
    place = head // group
    seq_lane = lax.broadcasted_iota(jnp.int32, forget_s.shape, 1)
    position = lax.broadcasted_iota(jnp.int32, (HEADS, length), 1)
    scale = HEAD_DIM ** (-0.5)
    for item in range(batch):
        seq = step * batch + item
        stay = jnp.zeros((HEADS, pair), rows)
        move = jnp.zeros((HEADS, pair), rows)
        for tile in range(tiles):
            piece = jnp.broadcast_to(
                query_s[tile, pl.ds(seq, 1), :], (HEADS, pair)
            )
            own_lanes = head == 2 * tile + odd
            stay = jnp.where(own_lanes & (odd == place), piece, stay)
            move = jnp.where(own_lanes & (odd != place), piece, move)
        query = stay + pltpu.roll(move, HEAD_DIM, 1)
        own = jnp.sum(query * key_s[pl.ds(seq, 1), :], axis=1, keepdims=True) * scale
        forget = jnp.sum(jnp.where(seq_lane == seq, forget_s[...], 0.0), axis=1, keepdims=True)
        cum = logcum[item]
        live_count = lengths[seq]
        last = jnp.sum(jnp.where(position == live_count - 1, cum, 0.0), axis=1, keepdims=True)
        scores = lax.dot_general(
            query.astype(jnp.bfloat16),
            keys[item],
            (((1,), (1,)), ((), ())),
            preferred_element_type=rows,
        )
        scores = scores * scale + ((last + forget) - cum)
        scores = jnp.where(position < live_count, scores, -jnp.inf)
        top = jnp.maximum(jnp.max(scores, axis=1, keepdims=True), own)
        expo = jnp.exp(scores - top)
        own_expo = jnp.exp(own - top)
        total = jnp.sum(expo, axis=1, keepdims=True) + own_expo
        weights = (expo / total).astype(jnp.bfloat16)
        own_weight = (own_expo / total).astype(jnp.bfloat16).astype(rows)
        out = jnp.dot(weights, values[item], preferred_element_type=rows)
        out = out + own_weight * value_s[pl.ds(seq, 1), :]
        turned = pltpu.roll(out, HEAD_DIM, 1)
        for tile in range(tiles):
            own_lanes = head == 2 * tile + odd
            part = jnp.where(own_lanes, jnp.where(odd == place, out, turned), 0.0)
            attended_s[tile, pl.ds(seq, 1), :] = jnp.sum(part, axis=0, keepdims=True)

    @pl.when(step == pl.num_programs(0) - 1)
    def _():
        attended = jnp.concatenate([attended_s[tile] for tile in range(tiles)], axis=1)
        attended = attended.astype(jnp.bfloat16)
        mixed = tokens[...].astype(rows) + jnp.dot(
            attended, w_out[...], preferred_element_type=rows
        )
        mixed = mixed.astype(jnp.bfloat16)
        mixed_ref[...] = mixed
        routed_ref[...] = normalize(mixed.astype(rows), gain_next[...]).astype(jnp.bfloat16)


def front(
    tokens, gain, w_query, w_key, w_value, w_forget, bias, w_out, keys, values, logcum, lengths, gain_next
):
    seqs, width = tokens.shape
    batch = max(size for size in (1, 2, 3) if seqs % size == 0)
    pair = keys.shape[2]

    def whole(*shape):
        return pl.BlockSpec(shape, lambda i, *_: (0,) * len(shape))

    def each(*shape):
        return pl.BlockSpec((batch, *shape), lambda i, *_: (i, 0, 0))

    small = (
        tokens,
        gain[None, :],
        w_query,
        w_key,
        w_value,
        w_forget.T,
        bias[:, None],
        w_out,
        gain_next[None, :],
    )
    kept = jax.ShapeDtypeStruct((seqs, width), jnp.bfloat16)
    return pl.pallas_call(
        front_body,
        out_shape=(kept, kept),
        grid_spec=pltpu.PrefetchScalarGridSpec(
            num_scalar_prefetch=1,
            grid=(seqs // batch,),
            in_specs=[whole(*array.shape) for array in small]
            + [each(*keys.shape[1:]), each(*values.shape[1:]), each(*logcum.shape[1:])],
            out_specs=[whole(seqs, width)] * 2,
            scratch_shapes=[
                pltpu.VMEM((HEADS * HEAD_DIM // pair, seqs, pair), jnp.float32),
                pltpu.VMEM((seqs, pair), jnp.float32),
                pltpu.VMEM((seqs, pair), jnp.float32),
                pltpu.VMEM((HEADS, seqs), jnp.float32),
                pltpu.VMEM((HEADS * HEAD_DIM // pair, seqs, pair), jnp.float32),
            ],
        ),
        compiler_params=pltpu.CompilerParams(
            dimension_semantics=("arbitrary",), vmem_limit_bytes=40 * 1024 * 1024
        ),
        cost_estimate=pl.CostEstimate(
            flops=10**9, bytes_accessed=16 * 10**6, transcendentals=2 * 10**5
        ),
        name="front",
    )(lengths, *small, keys, values, logcum)


def split3(values):
    parts = []
    for _ in range(3):
        part = stored(values)
        parts.append(part)
        values = values - part.astype(jnp.float32)
    return parts


def expert_unit(rows, gate_w, up_w, down_w):
    gate = jnp.minimum(jnp.dot(rows, gate_w, preferred_element_type=jnp.float32), LIMIT)
    up = jnp.clip(jnp.dot(rows, up_w, preferred_element_type=jnp.float32), -LIMIT, LIMIT)
    act = ((up + 1.0) * gate * jax.nn.sigmoid(gate * ALPHA)).astype(jnp.bfloat16)
    return jnp.dot(act, down_w, preferred_element_type=jnp.float32).astype(jnp.bfloat16)


def reach(source, target, sent, landed, device):
    return pltpu.make_async_remote_copy(
        src_ref=source,
        dst_ref=target,
        send_sem=sent,
        recv_sem=landed,
        device_id=(device,),
        device_id_type=pl.DeviceIdType.MESH,
    )


def to_row(column, same):
    return jnp.sum(jnp.where(same, column, 0.0), axis=0, keepdims=True)


def to_column(row, same):
    return jnp.sum(jnp.where(same, row, 0.0), axis=1, keepdims=True)


def rest_body(
    units_total,
    plane,
    packed,
    mixed,
    w_gate,
    w_up,
    w_down,
    d_gate,
    d_up,
    d_down,
    gain,
    branch,
    out,
    rows_s,
    units_s,
    answer_s,
    coef_s,
    square_s,
    squares_s,
    theirs_s,
    joint_s,
    final_s,
    own_sem,
    ag_send,
    ag_recv,
    fw_send,
    fw_recv,
    sq_send,
    sq_recv,
    d2d_send,
    d2d_recv,
    rs_send,
    rs_recv,
):
    kind = jnp.float32
    n = squares_s.shape[0]
    chips = n // 2
    pad = packed.shape[0]
    width = out.shape[1]
    chunk = units_s.shape[1] // pad
    halves = chips // chunk
    size = chunk * pad
    me = lax.axis_index("ep")
    core = lax.rem(me, 2)
    chip = me // 2
    other = chip * 2 + 1 - core
    mine = core * chips
    peer = (1 - core) * chips

    barrier = pltpu.get_barrier_semaphore()

    @pl.loop(1, n)
    def _(k):
        pl.semaphore_signal(
            barrier,
            inc=1,
            device_id=(lax.rem(me + k, n),),
            device_id_type=pl.DeviceIdType.MESH,
        )

    pl.semaphore_wait(barrier, n - 1)

    deep = chips // plane
    level = chip // plane
    spot = lax.rem(chip, plane)

    def before(dz, dp):
        return lax.rem(level - dz + deep, deep) * plane + lax.rem(spot - dp + plane, plane)

    def along(dz):
        to = lax.rem(level + dz, deep) * plane + spot
        k = dz * plane
        return reach(packed, rows_s.at[mine + chip], ag_send.at[k], ag_recv.at[k], to * 2 + core)

    def across(dz, dp):
        to = level * plane + lax.rem(spot + dp, plane)
        k = dz * plane + dp
        slot = rows_s.at[mine + before(dz, 0)]
        return reach(slot, slot, ag_send.at[k], ag_recv.at[k], to * 2 + core)

    def landed(dz, dp):
        slot = rows_s.at[mine + before(dz, dp)]
        k = dz * plane + dp
        return reach(slot, slot, ag_send.at[k], ag_recv.at[k], before(0, dp) * 2 + core)

    def forward(dz, dp):
        slot = rows_s.at[mine + before(dz, dp)]
        k = dz * plane + dp
        return reach(slot, slot, fw_send.at[k], fw_recv.at[k], other)

    def forwarded(dz, dp):
        slot = rows_s.at[peer + before(dz, dp)]
        k = dz * plane + dp
        return reach(slot, slot, fw_send.at[k], fw_recv.at[k], other)

    keep = pltpu.make_async_copy(packed, rows_s.at[mine + chip], own_sem)
    keep.start()

    @pl.loop(1, deep)
    def _(dz):
        along(dz).start()

    keep.wait()

    @pl.loop(1, plane)
    def _(dp):
        across(0, dp).start()

    forward(0, 0).start()

    @pl.loop(1, deep)
    def _(dz):
        landed(dz, 0).wait_recv()

        @pl.loop(1, plane)
        def _(dp):
            across(dz, dp).start()

        forward(dz, 0).start()

    @pl.loop(0, deep)
    def _(dz):
        @pl.loop(1, plane)
        def _(dp):
            landed(dz, dp).wait_recv()
            forward(dz, dp).start()

    @pl.loop(0, deep)
    def _(dz):
        @pl.loop(0, plane)
        def _(dp):
            forwarded(dz, dp).wait_recv()

    first = lax.broadcasted_iota(jnp.int32, (size, size), 0)
    second = lax.broadcasted_iota(jnp.int32, (size, size), 1)
    same = first == second

    def load(at):
        block = rows_s[pl.ds(at * chunk, chunk)]
        return block.astype(kind).reshape(size, block.shape[2])

    @pl.loop(0, 2 * halves)
    def _(at):
        wide = load(at)
        block = wide[:, :width].astype(jnp.bfloat16)
        gate = jnp.dot(block, d_gate[...], preferred_element_type=kind)
        up = jnp.dot(block, d_up[...], preferred_element_type=kind)
        units = (gate * jax.nn.sigmoid(gate) * up).astype(jnp.bfloat16).astype(kind)
        units_s[at] = units
        square_s[at] = to_row(jnp.sum(units * units, axis=1, keepdims=True), same)
        side = wide[:, width:]
        lane = lax.broadcasted_iota(jnp.int32, side.shape, 1)
        picked = jnp.where((side == me.astype(kind)) & (lane < TOPK), 1.0, 0.0)
        weight = jnp.zeros((size, 1), kind)
        for part in (3, 2, 1):
            moved = pltpu.roll(side, side.shape[1] - part * TOPK, 1)
            weight = weight + jnp.sum(picked * moved, axis=1, keepdims=True)
        branch_scale = jax.nn.sigmoid(
            jnp.sum(wide[:, :width] * branch[...], axis=1, keepdims=True)
        )
        coef_s[at] = jnp.where(lane == 0, weight, branch_scale)

    def share(k):
        return reach(
            square_s, squares_s.at[k], sq_send.at[k], sq_recv.at[k], lax.rem(me + k, n)
        )

    @pl.loop(1, n)
    def _(k):
        share(k).start()

    @pl.loop(0, 2 * halves)
    def _(at):
        block = load(at)[:, :width].astype(jnp.bfloat16)
        answer_s[at] = expert_unit(block, w_gate[...], w_up[...], w_down[...])

    @pl.loop(1, n)
    def _(k):
        share(k).wait_recv()

    squares_s[0] = square_s[...]
    totals = jnp.sum(squares_s[...], axis=0)
    square_rows = lax.rsqrt(totals / units_total + EPS)
    squares_s[0] = square_rows

    def partial(at):
        scale = to_column(squares_s[0, at], same)
        hidden = (units_s[at] * scale * gain[...]).astype(jnp.bfloat16)
        dense = jnp.dot(hidden, d_down[...], preferred_element_type=kind)
        coef = coef_s[at]
        routed = coef[:, 0:1] * answer_s[at].astype(kind)
        return (routed + coef[:, 1:2] * dense).reshape(chunk, pad, width)

    def cross(half):
        part = pl.ds(half * chunk, chunk)
        return reach(theirs_s.at[part], joint_s.at[part], d2d_send.at[half], d2d_recv.at[half], other)

    def back(dz, dp):
        k = dz * plane + dp
        slot = joint_s.at[before(dz, dp)]
        return reach(slot, final_s.at[k], rs_send.at[k], rs_recv.at[k], before(0, dp) * 2 + core)

    def down(dz):
        k = dz * plane
        to = before(dz, 0)
        return reach(joint_s.at[to], final_s.at[k], rs_send.at[k], rs_recv.at[k], to * 2 + core)

    def collected(dz):
        total = joint_s[before(dz, 0)].astype(kind)
        for dp in range(1, plane):
            back(dz, dp).wait_recv()
            total = total + final_s[dz * plane + dp].astype(kind)
        return total

    @pl.loop(0, halves)
    def _(half):
        theirs_s[pl.ds(half * chunk, chunk)] = partial((1 - core) * halves + half).astype(
            jnp.bfloat16
        )
        cross(half).start()

    @pl.loop(0, halves)
    def _(half):
        part = pl.ds(half * chunk, chunk)
        own = partial(core * halves + half)
        cross(half).wait_recv()
        joint_s[part] = (own + joint_s[part].astype(kind)).astype(jnp.bfloat16)

    @pl.loop(1, deep + 1)
    def _(step):
        @pl.loop(1, plane)
        def _(dp):
            back(lax.rem(step, deep), dp).start()

    @pl.loop(1, deep)
    def _(dz):
        joint_s[before(dz, 0)] = collected(dz).astype(jnp.bfloat16)
        down(dz).start()

    total = collected(0)
    for dz in range(1, deep):
        down(dz).wait_recv()
        total = total + final_s[dz * plane].astype(kind)
    result = mixed[...].astype(kind) + total[: mixed.shape[0]]
    out[...] = result.astype(jnp.bfloat16)

    @pl.loop(1, deep)
    def _(dz):
        along(dz).wait_send()
        down(dz).wait_send()

    @pl.loop(0, deep)
    def _(dz):
        forward(dz, 0).wait_send()

        @pl.loop(1, plane)
        def _(dp):
            across(dz, dp).wait_send()
            back(dz, dp).wait_send()
            forward(dz, dp).wait_send()

    @pl.loop(1, n)
    def _(k):
        share(k).wait_send()

    @pl.loop(0, halves)
    def _(half):
        cross(half).wait_send()


def rest(n, packed, mixed, w_gate, w_up, w_down, d_gate, d_up, d_down, gain, branch, units_total):
    pad = packed.shape[0]
    width = mixed.shape[1]
    local = d_gate.shape[1]
    chips = n // 2
    chunk = max(size for size in (1, 2, 4, 8) if chips % size == 0)
    halves = chips // chunk
    plane = chips // 4 if chips % 4 == 0 else chips
    size = chunk * pad
    half_type = jnp.bfloat16
    vmem = pl.BlockSpec(memory_space=pltpu.VMEM)
    dma = pltpu.SemaphoreType.DMA
    return pl.pallas_call(
        functools.partial(rest_body, units_total, plane),
        out_shape=jax.ShapeDtypeStruct(mixed.shape, half_type),
        in_specs=[vmem] * 10,
        out_specs=vmem,
        scratch_shapes=[
            pltpu.VMEM((n, *packed.shape), half_type),
            pltpu.VMEM((2 * halves, size, local), jnp.float32),
            pltpu.VMEM((2 * halves, size, width), half_type),
            pltpu.VMEM((2 * halves, size, 128), jnp.float32),
            pltpu.VMEM((2 * halves, 1, size), jnp.float32),
            pltpu.VMEM((n, 2 * halves, 1, size), jnp.float32),
            pltpu.VMEM((chips, pad, width), half_type),
            pltpu.VMEM((chips, pad, width), half_type),
            pltpu.VMEM((chips, pad, width), half_type),
            dma,
            dma((chips,)),
            dma((chips,)),
            dma((chips,)),
            dma((chips,)),
            dma((n,)),
            dma((n,)),
            dma((halves,)),
            dma((halves,)),
            dma((chips,)),
            dma((chips,)),
        ],
        compiler_params=pltpu.CompilerParams(
            collective_id=0, has_side_effects=True, vmem_limit_bytes=62 * 1024 * 1024
        ),
        name="rest",
    )(packed, mixed, w_gate, w_up, w_down, d_gate, d_up, d_down, gain, branch)


def fast_body(
    units_total,
    tokens_h,
    gain_h,
    w_query_h,
    w_key_h,
    w_value_h,
    w_forget_h,
    bias_h,
    w_out_h,
    keys_h,
    values_h,
    logcum_h,
    lengths_h,
    gain_next_h,
    ids_h,
    weights_h,
    e_gate_h,
    e_up_h,
    e_down_h,
    d_gate_h,
    d_up_h,
    d_down_h,
    d_gain_h,
    branch_h,
    out,
    tokens_s,
    gain_s,
    w_qkv_s,
    w_forget_s,
    bias_s,
    w_out_s,
    keys_s,
    values_s,
    logcum_s,
    lengths_s,
    gain_next_s,
    ids_s,
    weights_s,
    e_gate_s,
    e_up_s,
    e_down_s,
    d_in_s,
    d_down_s,
    d_gain_s,
    branch_s,
    query_s,
    key_s,
    value_s,
    forget_s,
    heads_s,
    mixed_s,
    fold_s,
    rows_s,
    x_s,
    spread_s,
    hidden_s,
    branch_col_s,
    square_s,
    squares_s,
    info_s,
    infos_s,
    scale_s,
    answer_s,
    part_s,
    joint_s,
    pair_s,
    first_a,
    first_b,
    turn_a,
    turn_b,
    second_a,
    second_b,
    level_s,
    levels_s,
    ld,
    kv_sem,
    z_send,
    z_recv,
    rows_send,
    x_recv,
    y_recv,
    da_recv,
    db_recv,
    f_recv,
    i_send,
    i_recv,
    q_send,
    q_recv,
    back_send,
    c_recv,
    s1a_recv,
    s1b_recv,
    s2a_recv,
    s2b_recv,
    zz_recv,
):
    kind = jnp.float32
    half_type = jnp.bfloat16
    n = squares_s.shape[0]
    chips = n // 2
    deep = x_s.shape[0]
    plane = chips // deep
    side = 2
    seqs, width = tokens_s.shape
    block, wide = rows_s.shape[1:]
    cut = wide // 2
    fold = wide - width
    folds = width // fold
    spare = seqs - block
    members = 2 * plane
    bulk = members * block
    tail = members * spare
    length, pair = keys_s.shape[1:]
    group = HEADS // KV_HEADS
    tiles = HEADS * HEAD_DIM // pair
    me = lax.axis_index("ep")
    core = lax.rem(me, 2)
    chip = me // 2
    other = chip * 2 + 1 - core
    level = chip // plane
    spot = lax.rem(chip, plane)
    row = spot // side
    col = lax.rem(spot, side)

    barrier = pltpu.get_barrier_semaphore()

    @pl.loop(1, n)
    def _(k):
        pl.semaphore_signal(
            barrier,
            inc=1,
            device_id=(lax.rem(me + k, n),),
            device_id_type=pl.DeviceIdType.MESH,
        )

    heads_wide = HEADS * HEAD_DIM
    loads = [
        (tokens_h, tokens_s),
        (gain_h, gain_s),
        (w_query_h, w_qkv_s.at[:, 0:heads_wide]),
        (w_key_h, w_qkv_s.at[:, heads_wide : heads_wide + pair]),
        (w_value_h, w_qkv_s.at[:, heads_wide + pair : heads_wide + 2 * pair]),
        (w_forget_h, w_forget_s),
        (bias_h, bias_s),
        (lengths_h, lengths_s),
        (logcum_h, logcum_s),
        (ids_h, ids_s),
        (weights_h, weights_s),
    ]
    later = [
        (w_out_h, w_out_s),
        (gain_next_h, gain_next_s),
        (d_gate_h, d_in_s.at[:, 0:pair]),
        (d_up_h, d_in_s.at[:, pair : 2 * pair]),
        (d_gain_h, d_gain_s),
        (branch_h, branch_s),
        (e_gate_h.at[0], e_gate_s),
        (e_up_h.at[0], e_up_s),
        (e_down_h.at[0], e_down_s),
        (d_down_h, d_down_s),
    ]
    copies = [
        pltpu.make_async_copy(source, target, ld.at[at])
        for at, (source, target) in enumerate(loads + later)
    ]
    batch = seqs // kv_sem.shape[1]
    groups = kv_sem.shape[1]

    def cached(at):
        part = pl.ds(at * batch, batch)
        return (
            pltpu.make_async_copy(keys_h.at[part], keys_s.at[part], kv_sem.at[0, at]),
            pltpu.make_async_copy(values_h.at[part], values_s.at[part], kv_sem.at[1, at]),
        )

    for copy in copies[: len(loads)]:
        copy.start()

    @pl.loop(0, groups)
    def _(at):
        for copy in cached(at):
            copy.start()

    for copy in copies[len(loads) :]:
        copy.start()

    for at in (1, 2):
        copies[len(loads) - at].wait()

    experts = lax.broadcasted_iota(jnp.int32, (n, seqs), 0)
    matched = jnp.zeros((n, seqs), kind)
    for at in range(TOPK):
        chosen = ids_s[at : at + 1, :] == experts
        matched = matched + jnp.where(chosen, weights_s[at : at + 1, :], 0.0)
    token = lax.broadcasted_iota(jnp.int32, (seqs, 2 * bulk), 0)
    spread = lax.broadcasted_iota(jnp.int32, (seqs, 2 * bulk), 1)
    member = core * plane + spot
    exact = lax.Precision.HIGHEST
    in_block = (token < block) & (spread == member * block + token)
    in_tail = (token >= block) & (spread == bulk + (token - block) * members + member)
    spread = jnp.where(in_block | in_tail, 1.0, 0.0)
    spread = jnp.dot(matched, spread, preferred_element_type=kind, precision=exact)
    for at in range(n):
        info_s[at] = spread[at : at + 1, :]
    infos_s[pl.ds(me, 1)] = info_s[pl.ds(me, 1)]
    square_s[...] = jnp.zeros_like(square_s)

    for at in range(9):
        copies[at].wait()

    normed = normalize(tokens_s[...].astype(kind), gain_s[...]).astype(half_type)
    product = jnp.dot(normed, w_qkv_s[...], preferred_element_type=kind)
    product = product.astype(half_type).astype(kind)
    key_s[...] = product[:, heads_wide : heads_wide + pair]
    value_s[...] = product[:, heads_wide + pair : heads_wide + 2 * pair]
    lane = lax.broadcasted_iota(jnp.int32, (seqs, pair), 1)
    for head in range(HEADS):
        piece = product[:, head // 2 * pair : (head // 2 + 1) * pair]
        if head % 2 != head // group:
            piece = pltpu.roll(piece, HEAD_DIM, 1)
        piece = jnp.where(lane // HEAD_DIM == head // group, piece, 0.0)
        query_s[pl.ds(head, seqs, stride=HEADS), :] = piece
    forget = lax.dot_general(
        w_forget_s[...], normed, (((1,), (1,)), ((), ())), preferred_element_type=kind
    )
    eye = lax.broadcasted_iota(jnp.int32, (HEADS, HEADS), 0)
    eye = eye == lax.broadcasted_iota(jnp.int32, (HEADS, HEADS), 1)
    forget = forget + to_column(bias_s[...], eye)
    forget_s[...] = jnp.minimum(forget, 0.0) - jnp.log1p(jnp.exp(-jnp.abs(forget)))

    seq_lane = lax.broadcasted_iota(jnp.int32, forget_s.shape, 1)
    position = lax.broadcasted_iota(jnp.int32, (HEADS, length), 1)
    unit = HEAD_DIM ** (-0.5)

    def attend(at):
        for copy in cached(at):
            copy.wait()
        scores_all = []
        own_all = []
        for item in range(batch):
            seq = at * batch + item
            query = query_s[pl.ds(pl.multiple_of(seq * HEADS, HEADS), HEADS), :]
            own = jnp.sum(query * key_s[pl.ds(seq, 1), :], axis=1, keepdims=True) * unit
            forget = jnp.sum(jnp.where(seq_lane == seq, forget_s[...], 0.0), axis=1, keepdims=True)
            cum = logcum_s[seq]
            live = lengths_s[seq]
            last = jnp.sum(jnp.where(position == live - 1, cum, 0.0), axis=1, keepdims=True)
            scores = lax.dot_general(
                query.astype(half_type),
                keys_s[seq],
                (((1,), (1,)), ((), ())),
                preferred_element_type=kind,
            )
            scores = scores * unit + ((last + forget) - cum)
            scores_all.append(jnp.where(position < live, scores, -jnp.inf))
            own_all.append(own)
        scores = jnp.concatenate(scores_all, axis=0)
        own = jnp.concatenate(own_all, axis=0)
        top = jnp.maximum(jnp.max(scores, axis=1, keepdims=True), own)
        expo = jnp.exp(scores - top)
        own_expo = jnp.exp(own - top)
        total = jnp.sum(expo, axis=1, keepdims=True) + own_expo
        share = (expo / total).astype(half_type)
        own_share = (own_expo / total).astype(half_type).astype(kind)
        for item in range(batch):
            seq = at * batch + item
            part = slice(item * HEADS, (item + 1) * HEADS)
            result = jnp.dot(share[part], values_s[seq], preferred_element_type=kind)
            result = result + own_share[part] * value_s[pl.ds(seq, 1), :]
            heads_s[pl.ds(pl.multiple_of(seq * HEADS, HEADS), HEADS), :] = result

    def inform(k):
        to = lax.rem(me + k, n)
        return reach(info_s.at[to], infos_s.at[me], i_send.at[0], i_recv.at[0], to)

    def informed():
        every = infos_s.at[pl.ds(0, n - 1)]
        return reach(every, every, i_send.at[0], i_recv.at[0], other)

    pl.loop(0, groups // 2)(attend)
    pl.semaphore_wait(barrier, n - 1)

    @pl.loop(1, n)
    def _(k):
        inform(k).start()

    pl.loop(groups // 2, groups)(attend)

    for at in range(len(loads), len(loads) + 6):
        copies[at].wait()

    found = [heads_s[pl.ds(head, seqs, stride=HEADS), :] for head in range(HEADS)]
    pieces = []
    for tile in range(tiles):
        left, right = found[2 * tile], found[2 * tile + 1]
        if 2 * tile // group:
            left = pltpu.roll(left, HEAD_DIM, 1)
        else:
            right = pltpu.roll(right, HEAD_DIM, 1)
        pieces.append(jnp.where(lane < HEAD_DIM, left, right))
    attended = jnp.concatenate(pieces, axis=1).astype(half_type)
    mixed = tokens_s[...].astype(kind) + jnp.dot(
        attended, w_out_s[...], preferred_element_type=kind
    )
    mixed = mixed.astype(half_type).astype(kind)
    mixed_s[...] = mixed
    routed = normalize(mixed, gain_next_s[...])

    def slot(at, which, place):
        return (at * 2 + which) * plane + place

    home = slot(level, core, spot)
    for part in range(folds):
        fold_s[pl.ds(part * spare, spare), :] = routed[block:, part * fold : (part + 1) * fold]
    rows_s[home, :, 0:width] = routed[:block].astype(half_type)
    rows_s[home, :, width:wide] = fold_s[...].astype(half_type)

    def device(z, y, x, which):
        return ((z * side + y) * side + x) * 2 + which

    spot_x = row * side + 1 - col
    spot_y = (1 - row) * side + col
    spot_d = (1 - row) * side + 1 - col
    near_x = device(level, row, 1 - col, core)
    near_y = device(level, 1 - row, col, core)

    def part_of(at, place, piece):
        return rows_s.at[slot(at, core, place), :, piece * cut : (piece + 1) * cut]

    def along(at, way, piece):
        here = part_of(at, spot, piece)
        to = device(level + (1 if way else -1), row, col, core)
        return reach(here, here, z_send.at[way, at], z_recv.at[piece, at], to)

    def beside(at, place, piece):
        here = part_of(at, place, piece)
        return reach(here, here, rows_send.at[0], x_recv.at[piece, at], near_x)

    def above(at, place, piece):
        here = part_of(at, place, piece)
        return reach(here, here, rows_send.at[0], y_recv.at[piece, at], near_y)

    def relay_a(at, place):
        here = rows_s.at[slot(at, core, place), :, 0:cut]
        return reach(here, here, rows_send.at[0], da_recv.at[at], near_y)

    def relay_b(at, place):
        here = rows_s.at[slot(at, core, place), :, cut:wide]
        return reach(here, here, rows_send.at[0], db_recv.at[at], near_x)

    def across(at, which, place):
        here = rows_s.at[slot(at, which, place)]
        return reach(here, here, rows_send.at[0], f_recv.at[at], other)

    def crossed(at):
        here = rows_s.at[pl.ds(slot(at, 1 - core, 0), plane)]
        return reach(here, here, rows_send.at[0], f_recv.at[at], other)

    balance = jnp.minimum(level, deep - 1 - level)
    lean = jnp.where(2 * level < deep - 1, 1, -1)

    def ordered(j):
        paired = jnp.where(lax.rem(j, 2) == 1, -1, 1) * ((j + 1) // 2)
        single = lean * (j - balance)
        return level + jnp.where(j <= 2 * balance, paired, single)

    def share(k, at):
        return reach(
            square_s.at[at],
            squares_s.at[k, at],
            q_send.at[0],
            q_recv.at[0],
            lax.rem(me + k, n),
        )

    def shared():
        every = squares_s.at[pl.ds(1, n - 1)]
        return reach(every, every, q_send.at[0], q_recv.at[0], other)

    def sent(blocks, sem):
        every = rows_s.at[pl.ds(0, blocks)]
        return reach(every, every, sem, sem, other)

    def spread_piece(at, piece):
        if piece:
            above(at, spot, piece).start()
            beside(at, spot, piece).start()
        else:
            beside(at, spot, piece).start()
            above(at, spot, piece).start()

    for piece in range(2):

        @pl.when(level + 1 < deep)
        def _():
            along(level, 1, piece).start()

        @pl.when(level > 0)
        def _():
            along(level, 0, piece).start()

        spread_piece(level, piece)

    across(level, core, spot).start()

    for at in range(len(loads) + 6, len(loads) + len(later)):
        copies[at].wait()

    ones = jnp.ones((8, pair), kind)
    same_bulk = lax.broadcasted_iota(jnp.int32, (bulk, bulk), 0)
    same_bulk = same_bulk == lax.broadcasted_iota(jnp.int32, (bulk, bulk), 1)
    tail_at = lax.broadcasted_iota(jnp.int32, (tail, bulk), 1)
    tail_of = lax.broadcasted_iota(jnp.int32, (tail, bulk), 0)

    def dense_units(at):
        crossed(at).wait_recv()

        part = pl.ds(at * members, members)
        x_s[at, 0:bulk, :] = rows_s[part, :, 0:width].reshape(bulk, width)
        folded = rows_s[part, :, width:wide].astype(kind).reshape(bulk, fold)
        for tile in range(fold // pair):
            spread_s[tile] = folded[:, tile * pair : (tile + 1) * pair]
        for piece in range(folds):
            for tile in range(fold // pair):
                lanes = slice(piece * fold + tile * pair, piece * fold + (tile + 1) * pair)
                taken = [
                    spread_s[tile, pl.ds(piece * spare + extra, members, stride=block), :]
                    for extra in range(spare)
                ]
                x_s[at, bulk : bulk + tail, lanes] = jnp.concatenate(taken, axis=0).astype(
                    half_type
                )
        values = x_s[at]
        inner = jnp.sum(values.astype(kind) * branch_s[...], axis=1, keepdims=True)
        branch_col_s[at] = jnp.broadcast_to(jax.nn.sigmoid(inner), (bulk + tail, pair))
        both = jnp.dot(values, d_in_s[...], preferred_element_type=kind)
        gate, up = both[:, 0:pair], both[:, pair : 2 * pair]
        units = (gate * jax.nn.sigmoid(gate) * up).astype(half_type).astype(kind)
        hidden_s[at] = (units * d_gain_s[pl.ds(me, 1), :]).astype(half_type)
        squares = lax.dot_general(
            ones,
            units * units,
            (((1,), (1,)), ((), ())),
            preferred_element_type=kind,
            precision=exact,
        )
        square_s[at, :, 0:bulk] = squares[0:1, 0:bulk]
        square_s[at, :, bulk : bulk + tail] = squares[0:1, bulk : bulk + tail]

        @pl.loop(1, n)
        def _(k):
            share(k, at).start()

    def run_expert(at):
        values = x_s[at]
        gate = jnp.minimum(jnp.dot(values, e_gate_s[...], preferred_element_type=kind), LIMIT)
        up = jnp.clip(jnp.dot(values, e_up_s[...], preferred_element_type=kind), -LIMIT, LIMIT)
        act = ((up + 1.0) * gate * jax.nn.sigmoid(gate * ALPHA)).astype(half_type)
        answer_s[at] = jnp.dot(act, e_down_s[...], preferred_element_type=kind).astype(half_type)

    @pl.loop(0, deep + 1)
    def _(step):
        @pl.when(step + 1 < deep)
        def _():
            at = ordered(step + 1)
            for piece in range(2):
                along(at, 0, piece).wait_recv()

                @pl.when((at < level) & (level + 1 < deep))
                def _():
                    along(at, 1, piece).start()

                @pl.when((at > level) & (level > 0))
                def _():
                    along(at, 0, piece).start()

                spread_piece(at, piece)
            across(at, core, spot).start()

        @pl.when(step < deep)
        def _():
            at = ordered(step)
            beside(at, spot_x, 0).wait_recv()
            relay_a(at, spot_x).start()
            above(at, spot_y, 1).wait_recv()
            relay_b(at, spot_y).start()
            beside(at, spot_x, 1).wait_recv()
            across(at, core, spot_x).start()
            above(at, spot_y, 0).wait_recv()
            across(at, core, spot_y).start()

        @pl.when(step >= 1)
        def _():
            at = ordered(step - 1)
            relay_a(at, spot_d).wait_recv()
            relay_b(at, spot_d).wait_recv()
            across(at, core, spot_d).start()

        @pl.when((step >= 2) & (step < deep))
        def _():
            run_expert(ordered(step - 2))

        @pl.when(step >= 1)
        def _():
            dense_units(ordered(step - 1))

    @pl.loop(deep - 2, deep)
    def _(step):
        run_expert(ordered(step))

    informed().wait_recv()
    shared().wait_recv()

    squares_s[0] = square_s[...]
    scale_s[...] = lax.rsqrt(jnp.sum(squares_s[...], axis=0) / units_total + EPS)

    def columns(line):
        main = to_column(line[:, 0:bulk], same_bulk)
        ends = jnp.where(tail_at == tail_of, line[:, bulk : 2 * bulk], 0.0)
        return main, jnp.sum(ends, axis=1, keepdims=True)

    def cross(at):
        return reach(
            part_s.at[at, pl.ds((1 - core) * plane, plane)],
            joint_s.at[at],
            back_send.at[0],
            c_recv.at[at],
            other,
        )

    def first(at, k):
        return (
            reach(
                pair_s.at[at, k * side + 1 - col, :, 0:cut],
                first_a.at[at, k],
                back_send.at[0],
                s1a_recv.at[at],
                near_x,
            ),
            reach(
                pair_s.at[at, (1 - row) * side + k, :, cut:wide],
                first_b.at[at, k],
                back_send.at[0],
                s1b_recv.at[at],
                near_y,
            ),
        )

    def second(at):
        return (
            reach(turn_a.at[at], second_a.at[at], back_send.at[0], s2a_recv.at[at], near_y),
            reach(turn_b.at[at], second_b.at[at], back_send.at[0], s2b_recv.at[at], near_x),
        )

    def home_to(at):
        return reach(
            level_s.at[at],
            levels_s.at[level],
            back_send.at[0],
            zz_recv.at[level],
            device(at, row, col, core),
        )

    def home_from(at):
        return reach(
            level_s.at[at],
            levels_s.at[at],
            back_send.at[0],
            zz_recv.at[at],
            device(at, row, col, core),
        )

    @pl.loop(0, deep + 3)
    def _(step):
        @pl.when(step < deep)
        def _():
            at = ordered(deep - 1 - step)
            dense = jnp.dot(hidden_s[at], d_down_s[...], preferred_element_type=kind)
            coef = jnp.sum(infos_s[pl.ds(at * members, members)], axis=0)
            weight, weight_end = columns(coef)
            scale, scale_end = columns(scale_s[at])
            twice = branch_col_s[at, :, 0:1]
            main = weight * answer_s[at, 0:bulk, :].astype(kind)
            main = main + (scale * twice[0:bulk]) * dense[0:bulk]
            ends = weight_end * answer_s[at, bulk : bulk + tail, :].astype(kind)
            ends = ends + (scale_end * twice[bulk:]) * dense[bulk:]
            part_s[at, :, :, 0:width] = main.astype(half_type).reshape(members, block, width)
            for piece in range(folds):
                for tile in range(fold // pair):
                    first_lane = piece * fold + tile * pair
                    for extra in range(spare):
                        spread_s[tile, pl.ds(piece * spare + extra, members, stride=block), :] = (
                            ends[
                                extra * members : (extra + 1) * members,
                                first_lane : first_lane + pair,
                            ]
                        )
            for tile in range(fold // pair):
                part_s[at, :, :, width + tile * pair : width + (tile + 1) * pair] = (
                    spread_s[tile].astype(half_type).reshape(members, block, pair)
                )
            cross(at).start()

        @pl.when((step >= 1) & (step < deep + 1))
        def _():
            at = ordered(deep - step)
            cross(at).wait_recv()
            mine = part_s[at, pl.ds(core * plane, plane)].astype(kind)
            pair_s[at] = (mine + joint_s[at].astype(kind)).astype(half_type)
            for k in range(side):
                for copy in first(at, k):
                    copy.start()

        @pl.when((step >= 2) & (step < deep + 2))
        def _():
            at = ordered(deep + 1 - step)
            for here, sem in ((first_a.at[at], s1a_recv.at[at]), (first_b.at[at], s1b_recv.at[at])):
                reach(here, here, back_send.at[0], sem, other).wait_recv()
            turned = pair_s[at, spot_y, :, 0:cut].astype(kind) + first_a[at, 1 - row].astype(kind)
            turn_a[at] = turned.astype(half_type)
            turned = pair_s[at, spot_x, :, cut:wide].astype(kind) + first_b[at, 1 - col].astype(kind)
            turn_b[at] = turned.astype(half_type)
            for copy in second(at):
                copy.start()

        @pl.when(step >= 3)
        def _():
            at = ordered(deep + 2 - step)
            for copy in second(at):
                copy.wait_recv()
            total = pair_s[at, spot, :, 0:cut].astype(kind) + first_a[at, row].astype(kind)
            total = total + second_a[at].astype(kind)
            level_s[at, :, 0:cut] = total.astype(half_type)
            total = pair_s[at, spot, :, cut:wide].astype(kind) + first_b[at, col].astype(kind)
            total = total + second_b[at].astype(kind)
            level_s[at, :, cut:wide] = total.astype(half_type)

            @pl.when(step < deep + 2)
            def _():
                home_to(at).start()

    total = level_s[level].astype(kind)
    for j in range(1, deep):
        at = ordered(j)
        home_from(at).wait_recv()
        total = total + levels_s[at].astype(kind)
    out[0:block, :] = (mixed_s[0:block, :] + total[:, 0:width]).astype(half_type)
    fold_s[...] = total[:, width:wide]
    for part in range(folds):
        lanes = slice(part * fold, (part + 1) * fold)
        ends = mixed_s[block:seqs, lanes] + fold_s[pl.ds(part * spare, spare), :]
        out[block:seqs, lanes] = ends.astype(half_type)

    @pl.loop(0, deep)
    def _(at):
        whole = rows_s.at[slot(at, core, spot)]

        @pl.when((at <= level) & (level + 1 < deep))
        def _():
            reach(whole, whole, z_send.at[1, at], z_send.at[1, at], other).wait_send()

        @pl.when((at >= level) & (level > 0))
        def _():
            reach(whole, whole, z_send.at[0, at], z_send.at[0, at], other).wait_send()

    sent(chips + 3 * deep, rows_send.at[0]).wait_send()
    sent(chips + 4 * deep - 1, back_send.at[0]).wait_send()
    informed().wait_send()
    shared().wait_send()


def fast(n, deep, arrays, units_total):
    (tokens, keys, logcum, e_gate, e_down, d_gate, d_gain) = (
        arrays[0],
        arrays[8],
        arrays[10],
        arrays[15],
        arrays[17],
        arrays[18],
        arrays[21],
    )
    seqs, width = tokens.shape
    length, pair = keys.shape[1:]
    hidden = e_gate.shape[2]
    local = d_gate.shape[1]
    chips = n // 2
    plane = chips // deep
    block = seqs // 16 * 16
    spare = seqs - block
    wide = width + spare * width // block
    fold = wide - width
    cut = wide // 2
    members = 2 * plane
    bulk = members * block
    tail = members * spare
    heads_wide = HEADS * HEAD_DIM
    half_type = jnp.bfloat16
    kind = jnp.float32
    dma = pltpu.SemaphoreType.DMA
    groups = 3
    vmem = pltpu.VMEM
    scratch = [
        vmem((seqs, width), half_type),
        vmem((1, width), kind),
        vmem((width, heads_wide + 2 * pair), half_type),
        vmem((HEADS, width), half_type),
        vmem((1, HEADS), kind),
        vmem((heads_wide, width), half_type),
        vmem((seqs, length, pair), half_type),
        vmem((seqs, length, pair), half_type),
        vmem((seqs, HEADS, length), kind),
        pltpu.SMEM((seqs,), jnp.int32),
        vmem((1, width), kind),
        vmem((TOPK, seqs), jnp.int32),
        vmem((TOPK, seqs), kind),
        vmem((width, hidden), half_type),
        vmem((width, hidden), half_type),
        vmem((hidden, width), half_type),
        vmem((width, 2 * local), half_type),
        vmem((local, width), half_type),
        vmem(d_gain.shape, kind),
        vmem((1, width), kind),
        vmem((seqs * HEADS, pair), kind),
        vmem((seqs, pair), kind),
        vmem((seqs, pair), kind),
        vmem((HEADS, seqs), kind),
        vmem((seqs * HEADS, pair), kind),
        vmem((seqs, width), kind),
        vmem((block, fold), kind),
        vmem((n, block, wide), half_type),
        vmem((deep, bulk + tail, width), half_type),
        vmem((fold // pair, bulk, pair), kind),
        vmem((deep, bulk + tail, local), half_type),
        vmem((deep, bulk + tail, pair), kind),
        vmem((deep, 1, 2 * bulk), kind),
        vmem((n, deep, 1, 2 * bulk), kind),
        vmem((n, 1, 2 * bulk), kind),
        vmem((n, 1, 2 * bulk), kind),
        vmem((deep, 1, 2 * bulk), kind),
        vmem((deep, bulk + tail, width), half_type),
        vmem((deep, members, block, wide), half_type),
        vmem((deep, plane, block, wide), half_type),
        vmem((deep, plane, block, wide), half_type),
        vmem((deep, 2, block, cut), half_type),
        vmem((deep, 2, block, cut), half_type),
        vmem((deep, block, cut), half_type),
        vmem((deep, block, cut), half_type),
        vmem((deep, block, cut), half_type),
        vmem((deep, block, cut), half_type),
        vmem((deep, block, wide), half_type),
        vmem((deep, block, wide), half_type),
        dma((21,)),
        dma((2, groups)),
        dma((2, deep)),
        dma((2, deep)),
        dma((1,)),
        dma((2, deep)),
        dma((2, deep)),
        dma((deep,)),
        dma((deep,)),
        dma((deep,)),
        dma((1,)),
        dma((1,)),
        dma((1,)),
        dma((1,)),
        dma((1,)),
        dma((deep,)),
        dma((deep,)),
        dma((deep,)),
        dma((deep,)),
        dma((deep,)),
        dma((deep,)),
    ]
    return pl.pallas_call(
        functools.partial(fast_body, units_total),
        out_shape=jax.ShapeDtypeStruct(tokens.shape, half_type),
        in_specs=[pl.BlockSpec(memory_space=pl.ANY)] * len(arrays),
        out_specs=pl.BlockSpec(memory_space=pltpu.VMEM),
        scratch_shapes=scratch,
        compiler_params=pltpu.CompilerParams(
            collective_id=0, has_side_effects=True, vmem_limit_bytes=62 * 1024 * 1024
        ),
        name="layer",
    )(*arrays)


def shards(
    tokens,
    attn_norm_gain,
    w_query,
    w_key,
    w_value,
    w_forget,
    forget_bias,
    w_attn_out,
    cache_keys,
    cache_values,
    cache_logcum,
    cache_lengths,
    expert_norm_gain,
    expert_ids,
    expert_weights,
    w_expert_gate,
    w_expert_up,
    w_expert_down,
    w_dense_gate,
    w_dense_up,
    w_dense_down,
    dense_norm_gain,
    branch_gate,
):
    n = lax.axis_size("ep")
    deep = 4
    seqs, width = tokens.shape
    local = w_dense_gate.shape[1]
    spare = seqs % 16
    fits = n == 8 * deep and local == cache_keys.shape[2] and 0 < spare and spare * width % 2048 == 0
    if fits and seqs // 16 == 1:
        return fast(
            n,
            deep,
            (
                tokens,
                attn_norm_gain[None, :],
                w_query,
                w_key,
                w_value,
                w_forget.T,
                forget_bias[None, :],
                w_attn_out,
                cache_keys,
                cache_values,
                cache_logcum,
                cache_lengths,
                expert_norm_gain[None, :],
                expert_ids.T,
                expert_weights.T,
                w_expert_gate,
                w_expert_up,
                w_expert_down,
                w_dense_gate,
                w_dense_up,
                w_dense_down,
                dense_norm_gain.reshape(n, local),
                branch_gate[None, :],
            ),
            dense_norm_gain.shape[0],
        )
    mixed, routed_in = front(
        tokens,
        attn_norm_gain,
        w_query,
        w_key,
        w_value,
        w_forget,
        forget_bias,
        w_attn_out,
        cache_keys,
        cache_values,
        cache_logcum,
        cache_lengths,
        expert_norm_gain,
    )
    n = lax.axis_size("ep")
    me = lax.axis_index("ep")
    seqs = tokens.shape[0]
    extra = jnp.concatenate([expert_ids.astype(jnp.bfloat16), *split3(expert_weights)], axis=1)
    packed = jnp.concatenate([routed_in, jnp.pad(extra, ((0, 0), (0, 128 - 4 * TOPK)))], axis=1)
    packed = jnp.pad(packed, ((0, -seqs % 8), (0, 0)))
    local = w_dense_gate.shape[1]
    gain = lax.dynamic_slice_in_dim(dense_norm_gain, me * local, local, 0)
    return rest(
        n,
        packed,
        mixed,
        w_expert_gate[0],
        w_expert_up[0],
        w_expert_down[0],
        w_dense_gate,
        w_dense_up,
        w_dense_down,
        gain[None, :],
        branch_gate[None, :],
        dense_norm_gain.shape[0],
    )


def solution(mesh):
    in_specs = (
        P("ep", None),
        P(),
        P(),
        P(),
        P(),
        P(),
        P(),
        P(),
        P("ep", None, None),
        P("ep", None, None),
        P("ep", None, None),
        P("ep"),
        P(),
        P("ep", None),
        P("ep", None),
        P("ep", None, None),
        P("ep", None, None),
        P("ep", None, None),
        P(None, "ep"),
        P(None, "ep"),
        P("ep", None),
        P(),
        P(),
    )
    out_specs = P("ep", None)
    return jax.shard_map(shards, mesh=mesh, in_specs=in_specs, out_specs=out_specs, check_vma=False)
```

```python
import functools

import jax
import jax.numpy as jnp
from jax import lax
from jax.experimental import pallas as pl
from jax.experimental.pallas import tpu as pltpu
from jax.sharding import PartitionSpec as P

HEADS = 8
KV_HEADS = 2
HEAD_DIM = 64
TOPK = 6


EPS = 1e-06
LIMIT = 7.0
ALPHA = 1.702


def normalize(values, gain):
    return values * lax.rsqrt(jnp.mean(values * values, axis=-1, keepdims=True) + EPS) * gain


def stored(values):
    return lax.optimization_barrier(values.astype(jnp.bfloat16))


def front_body(
    lengths,
    tokens,
    gain_ref,
    w_query,
    w_key,
    w_value,
    w_forget,
    bias,
    w_out,
    gain_next,
    keys,
    values,
    logcum,
    mixed_ref,
    routed_ref,
    query_s,
    key_s,
    value_s,
    forget_s,
    attended_s,
):
    step = pl.program_id(0)
    batch, length, pair = keys.shape
    rows = jnp.float32
    group = HEADS // KV_HEADS
    tiles = HEADS * HEAD_DIM // pair

    @pl.when(step == 0)
    def _():
        normed = normalize(tokens[...].astype(rows), gain_ref[...]).astype(jnp.bfloat16)
        for weight, kept in ((w_key, key_s), (w_value, value_s)):
            product = jnp.dot(normed, weight[...], preferred_element_type=rows)
            kept[...] = product.astype(jnp.bfloat16).astype(rows)
        product = jnp.dot(normed, w_query[...], preferred_element_type=rows)
        product = product.astype(jnp.bfloat16).astype(rows)
        for tile in range(tiles):
            query_s[tile] = product[:, tile * pair : (tile + 1) * pair]
        forget = lax.dot_general(
            w_forget[...], normed, (((1,), (1,)), ((), ())), preferred_element_type=rows
        )
        forget = forget + bias[...]
        forget_s[...] = jnp.minimum(forget, 0.0) - jnp.log1p(jnp.exp(-jnp.abs(forget)))

    lane = lax.broadcasted_iota(jnp.int32, (HEADS, pair), 1)
    head = lax.broadcasted_iota(jnp.int32, (HEADS, pair), 0)
    odd = lane // HEAD_DIM
    place = head // group
    seq_lane = lax.broadcasted_iota(jnp.int32, forget_s.shape, 1)
    position = lax.broadcasted_iota(jnp.int32, (HEADS, length), 1)
    scale = HEAD_DIM ** (-0.5)
    for item in range(batch):
        seq = step * batch + item
        stay = jnp.zeros((HEADS, pair), rows)
        move = jnp.zeros((HEADS, pair), rows)
        for tile in range(tiles):
            piece = jnp.broadcast_to(
                query_s[tile, pl.ds(seq, 1), :], (HEADS, pair)
            )
            own_lanes = head == 2 * tile + odd
            stay = jnp.where(own_lanes & (odd == place), piece, stay)
            move = jnp.where(own_lanes & (odd != place), piece, move)
        query = stay + pltpu.roll(move, HEAD_DIM, 1)
        own = jnp.sum(query * key_s[pl.ds(seq, 1), :], axis=1, keepdims=True) * scale
        forget = jnp.sum(jnp.where(seq_lane == seq, forget_s[...], 0.0), axis=1, keepdims=True)
        cum = logcum[item]
        live_count = lengths[seq]
        last = jnp.sum(jnp.where(position == live_count - 1, cum, 0.0), axis=1, keepdims=True)
        scores = lax.dot_general(
            query.astype(jnp.bfloat16),
            keys[item],
            (((1,), (1,)), ((), ())),
            preferred_element_type=rows,
        )
        scores = scores * scale + ((last + forget) - cum)
        scores = jnp.where(position < live_count, scores, -jnp.inf)
        top = jnp.maximum(jnp.max(scores, axis=1, keepdims=True), own)
        expo = jnp.exp(scores - top)
        own_expo = jnp.exp(own - top)
        total = jnp.sum(expo, axis=1, keepdims=True) + own_expo
        weights = (expo / total).astype(jnp.bfloat16)
        own_weight = (own_expo / total).astype(jnp.bfloat16).astype(rows)
        out = jnp.dot(weights, values[item], preferred_element_type=rows)
        out = out + own_weight * value_s[pl.ds(seq, 1), :]
        turned = pltpu.roll(out, HEAD_DIM, 1)
        for tile in range(tiles):
            own_lanes = head == 2 * tile + odd
            part = jnp.where(own_lanes, jnp.where(odd == place, out, turned), 0.0)
            attended_s[tile, pl.ds(seq, 1), :] = jnp.sum(part, axis=0, keepdims=True)

    @pl.when(step == pl.num_programs(0) - 1)
    def _():
        attended = jnp.concatenate([attended_s[tile] for tile in range(tiles)], axis=1)
        attended = attended.astype(jnp.bfloat16)
        mixed = tokens[...].astype(rows) + jnp.dot(
            attended, w_out[...], preferred_element_type=rows
        )
        mixed = mixed.astype(jnp.bfloat16)
        mixed_ref[...] = mixed
        routed_ref[...] = normalize(mixed.astype(rows), gain_next[...]).astype(jnp.bfloat16)


def front(
    tokens, gain, w_query, w_key, w_value, w_forget, bias, w_out, keys, values, logcum, lengths, gain_next
):
    seqs, width = tokens.shape
    batch = max(size for size in (1, 2, 3) if seqs % size == 0)
    pair = keys.shape[2]

    def whole(*shape):
        return pl.BlockSpec(shape, lambda i, *_: (0,) * len(shape))

    def each(*shape):
        return pl.BlockSpec((batch, *shape), lambda i, *_: (i, 0, 0))

    small = (
        tokens,
        gain[None, :],
        w_query,
        w_key,
        w_value,
        w_forget.T,
        bias[:, None],
        w_out,
        gain_next[None, :],
    )
    kept = jax.ShapeDtypeStruct((seqs, width), jnp.bfloat16)
    return pl.pallas_call(
        front_body,
        out_shape=(kept, kept),
        grid_spec=pltpu.PrefetchScalarGridSpec(
            num_scalar_prefetch=1,
            grid=(seqs // batch,),
            in_specs=[whole(*array.shape) for array in small]
            + [each(*keys.shape[1:]), each(*values.shape[1:]), each(*logcum.shape[1:])],
            out_specs=[whole(seqs, width)] * 2,
            scratch_shapes=[
                pltpu.VMEM((HEADS * HEAD_DIM // pair, seqs, pair), jnp.float32),
                pltpu.VMEM((seqs, pair), jnp.float32),
                pltpu.VMEM((seqs, pair), jnp.float32),
                pltpu.VMEM((HEADS, seqs), jnp.float32),
                pltpu.VMEM((HEADS * HEAD_DIM // pair, seqs, pair), jnp.float32),
            ],
        ),
        compiler_params=pltpu.CompilerParams(
            dimension_semantics=("arbitrary",), vmem_limit_bytes=40 * 1024 * 1024
        ),
        cost_estimate=pl.CostEstimate(
            flops=10**9, bytes_accessed=16 * 10**6, transcendentals=2 * 10**5
        ),
        name="front",
    )(lengths, *small, keys, values, logcum)


def split3(values):
    parts = []
    for _ in range(3):
        part = stored(values)
        parts.append(part)
        values = values - part.astype(jnp.float32)
    return parts


def expert_unit(rows, gate_w, up_w, down_w):
    gate = jnp.minimum(jnp.dot(rows, gate_w, preferred_element_type=jnp.float32), LIMIT)
    up = jnp.clip(jnp.dot(rows, up_w, preferred_element_type=jnp.float32), -LIMIT, LIMIT)
    act = ((up + 1.0) * gate * jax.nn.sigmoid(gate * ALPHA)).astype(jnp.bfloat16)
    return jnp.dot(act, down_w, preferred_element_type=jnp.float32).astype(jnp.bfloat16)


def reach(source, target, sent, landed, device):
    return pltpu.make_async_remote_copy(
        src_ref=source,
        dst_ref=target,
        send_sem=sent,
        recv_sem=landed,
        device_id=(device,),
        device_id_type=pl.DeviceIdType.MESH,
    )


def to_row(column, same):
    return jnp.sum(jnp.where(same, column, 0.0), axis=0, keepdims=True)


def to_column(row, same):
    return jnp.sum(jnp.where(same, row, 0.0), axis=1, keepdims=True)


def rest_body(
    units_total,
    plane,
    packed,
    mixed,
    w_gate,
    w_up,
    w_down,
    d_gate,
    d_up,
    d_down,
    gain,
    branch,
    out,
    rows_s,
    units_s,
    answer_s,
    coef_s,
    square_s,
    squares_s,
    theirs_s,
    joint_s,
    final_s,
    own_sem,
    ag_send,
    ag_recv,
    fw_send,
    fw_recv,
    sq_send,
    sq_recv,
    d2d_send,
    d2d_recv,
    rs_send,
    rs_recv,
):
    kind = jnp.float32
    n = squares_s.shape[0]
    chips = n // 2
    pad = packed.shape[0]
    width = out.shape[1]
    chunk = units_s.shape[1] // pad
    halves = chips // chunk
    size = chunk * pad
    me = lax.axis_index("ep")
    core = lax.rem(me, 2)
    chip = me // 2
    other = chip * 2 + 1 - core
    mine = core * chips
    peer = (1 - core) * chips

    barrier = pltpu.get_barrier_semaphore()

    @pl.loop(1, n)
    def _(k):
        pl.semaphore_signal(
            barrier,
            inc=1,
            device_id=(lax.rem(me + k, n),),
            device_id_type=pl.DeviceIdType.MESH,
        )

    pl.semaphore_wait(barrier, n - 1)

    deep = chips // plane
    level = chip // plane
    spot = lax.rem(chip, plane)

    def before(dz, dp):
        return lax.rem(level - dz + deep, deep) * plane + lax.rem(spot - dp + plane, plane)

    def along(dz):
        to = lax.rem(level + dz, deep) * plane + spot
        k = dz * plane
        return reach(packed, rows_s.at[mine + chip], ag_send.at[k], ag_recv.at[k], to * 2 + core)

    def across(dz, dp):
        to = level * plane + lax.rem(spot + dp, plane)
        k = dz * plane + dp
        slot = rows_s.at[mine + before(dz, 0)]
        return reach(slot, slot, ag_send.at[k], ag_recv.at[k], to * 2 + core)

    def landed(dz, dp):
        slot = rows_s.at[mine + before(dz, dp)]
        k = dz * plane + dp
        return reach(slot, slot, ag_send.at[k], ag_recv.at[k], before(0, dp) * 2 + core)

    def forward(dz, dp):
        slot = rows_s.at[mine + before(dz, dp)]
        k = dz * plane + dp
        return reach(slot, slot, fw_send.at[k], fw_recv.at[k], other)

    def forwarded(dz, dp):
        slot = rows_s.at[peer + before(dz, dp)]
        k = dz * plane + dp
        return reach(slot, slot, fw_send.at[k], fw_recv.at[k], other)

    keep = pltpu.make_async_copy(packed, rows_s.at[mine + chip], own_sem)
    keep.start()

    @pl.loop(1, deep)
    def _(dz):
        along(dz).start()

    keep.wait()

    @pl.loop(1, plane)
    def _(dp):
        across(0, dp).start()

    forward(0, 0).start()

    @pl.loop(1, deep)
    def _(dz):
        landed(dz, 0).wait_recv()

        @pl.loop(1, plane)
        def _(dp):
            across(dz, dp).start()

        forward(dz, 0).start()

    @pl.loop(0, deep)
    def _(dz):
        @pl.loop(1, plane)
        def _(dp):
            landed(dz, dp).wait_recv()
            forward(dz, dp).start()

    @pl.loop(0, deep)
    def _(dz):
        @pl.loop(0, plane)
        def _(dp):
            forwarded(dz, dp).wait_recv()

    first = lax.broadcasted_iota(jnp.int32, (size, size), 0)
    second = lax.broadcasted_iota(jnp.int32, (size, size), 1)
    same = first == second

    def load(at):
        block = rows_s[pl.ds(at * chunk, chunk)]
        return block.astype(kind).reshape(size, block.shape[2])

    @pl.loop(0, 2 * halves)
    def _(at):
        wide = load(at)
        block = wide[:, :width].astype(jnp.bfloat16)
        gate = jnp.dot(block, d_gate[...], preferred_element_type=kind)
        up = jnp.dot(block, d_up[...], preferred_element_type=kind)
        units = (gate * jax.nn.sigmoid(gate) * up).astype(jnp.bfloat16).astype(kind)
        units_s[at] = units
        square_s[at] = to_row(jnp.sum(units * units, axis=1, keepdims=True), same)
        side = wide[:, width:]
        lane = lax.broadcasted_iota(jnp.int32, side.shape, 1)
        picked = jnp.where((side == me.astype(kind)) & (lane < TOPK), 1.0, 0.0)
        weight = jnp.zeros((size, 1), kind)
        for part in (3, 2, 1):
            moved = pltpu.roll(side, side.shape[1] - part * TOPK, 1)
            weight = weight + jnp.sum(picked * moved, axis=1, keepdims=True)
        branch_scale = jax.nn.sigmoid(
            jnp.sum(wide[:, :width] * branch[...], axis=1, keepdims=True)
        )
        coef_s[at] = jnp.where(lane == 0, weight, branch_scale)

    def share(k):
        return reach(
            square_s, squares_s.at[k], sq_send.at[k], sq_recv.at[k], lax.rem(me + k, n)
        )

    @pl.loop(1, n)
    def _(k):
        share(k).start()

    @pl.loop(0, 2 * halves)
    def _(at):
        block = load(at)[:, :width].astype(jnp.bfloat16)
        answer_s[at] = expert_unit(block, w_gate[...], w_up[...], w_down[...])

    @pl.loop(1, n)
    def _(k):
        share(k).wait_recv()

    squares_s[0] = square_s[...]
    totals = jnp.sum(squares_s[...], axis=0)
    square_rows = lax.rsqrt(totals / units_total + EPS)
    squares_s[0] = square_rows

    def partial(at):
        scale = to_column(squares_s[0, at], same)
        hidden = (units_s[at] * scale * gain[...]).astype(jnp.bfloat16)
        dense = jnp.dot(hidden, d_down[...], preferred_element_type=kind)
        coef = coef_s[at]
        routed = coef[:, 0:1] * answer_s[at].astype(kind)
        return (routed + coef[:, 1:2] * dense).reshape(chunk, pad, width)

    def cross(half):
        part = pl.ds(half * chunk, chunk)
        return reach(theirs_s.at[part], joint_s.at[part], d2d_send.at[half], d2d_recv.at[half], other)

    def back(dz, dp):
        k = dz * plane + dp
        slot = joint_s.at[before(dz, dp)]
        return reach(slot, final_s.at[k], rs_send.at[k], rs_recv.at[k], before(0, dp) * 2 + core)

    def down(dz):
        k = dz * plane
        to = before(dz, 0)
        return reach(joint_s.at[to], final_s.at[k], rs_send.at[k], rs_recv.at[k], to * 2 + core)

    def collected(dz):
        total = joint_s[before(dz, 0)].astype(kind)
        for dp in range(1, plane):
            back(dz, dp).wait_recv()
            total = total + final_s[dz * plane + dp].astype(kind)
        return total

    @pl.loop(0, halves)
    def _(half):
        theirs_s[pl.ds(half * chunk, chunk)] = partial((1 - core) * halves + half).astype(
            jnp.bfloat16
        )
        cross(half).start()

    @pl.loop(0, halves)
    def _(half):
        part = pl.ds(half * chunk, chunk)
        own = partial(core * halves + half)
        cross(half).wait_recv()
        joint_s[part] = (own + joint_s[part].astype(kind)).astype(jnp.bfloat16)

    @pl.loop(1, deep + 1)
    def _(step):
        @pl.loop(1, plane)
        def _(dp):
            back(lax.rem(step, deep), dp).start()

    @pl.loop(1, deep)
    def _(dz):
        joint_s[before(dz, 0)] = collected(dz).astype(jnp.bfloat16)
        down(dz).start()

    total = collected(0)
    for dz in range(1, deep):
        down(dz).wait_recv()
        total = total + final_s[dz * plane].astype(kind)
    result = mixed[...].astype(kind) + total[: mixed.shape[0]]
    out[...] = result.astype(jnp.bfloat16)

    @pl.loop(1, deep)
    def _(dz):
        along(dz).wait_send()
        down(dz).wait_send()

    @pl.loop(0, deep)
    def _(dz):
        forward(dz, 0).wait_send()

        @pl.loop(1, plane)
        def _(dp):
            across(dz, dp).wait_send()
            back(dz, dp).wait_send()
            forward(dz, dp).wait_send()

    @pl.loop(1, n)
    def _(k):
        share(k).wait_send()

    @pl.loop(0, halves)
    def _(half):
        cross(half).wait_send()


def rest(n, packed, mixed, w_gate, w_up, w_down, d_gate, d_up, d_down, gain, branch, units_total):
    pad = packed.shape[0]
    width = mixed.shape[1]
    local = d_gate.shape[1]
    chips = n // 2
    chunk = max(size for size in (1, 2, 4, 8) if chips % size == 0)
    halves = chips // chunk
    plane = chips // 4 if chips % 4 == 0 else chips
    size = chunk * pad
    half_type = jnp.bfloat16
    vmem = pl.BlockSpec(memory_space=pltpu.VMEM)
    dma = pltpu.SemaphoreType.DMA
    return pl.pallas_call(
        functools.partial(rest_body, units_total, plane),
        out_shape=jax.ShapeDtypeStruct(mixed.shape, half_type),
        in_specs=[vmem] * 10,
        out_specs=vmem,
        scratch_shapes=[
            pltpu.VMEM((n, *packed.shape), half_type),
            pltpu.VMEM((2 * halves, size, local), jnp.float32),
            pltpu.VMEM((2 * halves, size, width), half_type),
            pltpu.VMEM((2 * halves, size, 128), jnp.float32),
            pltpu.VMEM((2 * halves, 1, size), jnp.float32),
            pltpu.VMEM((n, 2 * halves, 1, size), jnp.float32),
            pltpu.VMEM((chips, pad, width), half_type),
            pltpu.VMEM((chips, pad, width), half_type),
            pltpu.VMEM((chips, pad, width), half_type),
            dma,
            dma((chips,)),
            dma((chips,)),
            dma((chips,)),
            dma((chips,)),
            dma((n,)),
            dma((n,)),
            dma((halves,)),
            dma((halves,)),
            dma((chips,)),
            dma((chips,)),
        ],
        compiler_params=pltpu.CompilerParams(
            collective_id=0, has_side_effects=True, vmem_limit_bytes=62 * 1024 * 1024
        ),
        name="rest",
    )(packed, mixed, w_gate, w_up, w_down, d_gate, d_up, d_down, gain, branch)


def fast_body(
    units_total,
    tokens_h,
    gain_h,
    w_query_h,
    w_key_h,
    w_value_h,
    w_forget_h,
    bias_h,
    w_out_h,
    keys_h,
    values_h,
    logcum_h,
    lengths_h,
    gain_next_h,
    ids_h,
    weights_h,
    e_gate_h,
    e_up_h,
    e_down_h,
    d_gate_h,
    d_up_h,
    d_down_h,
    d_gain_h,
    branch_h,
    out,
    tokens_s,
    gain_s,
    w_qkv_s,
    w_forget_s,
    bias_s,
    w_out_s,
    keys_s,
    values_s,
    logcum_s,
    lengths_s,
    gain_next_s,
    ids_s,
    weights_s,
    e_gate_s,
    e_up_s,
    e_down_s,
    d_in_s,
    d_down_s,
    d_gain_s,
    branch_s,
    query_s,
    key_s,
    value_s,
    forget_s,
    heads_s,
    mixed_s,
    fold_s,
    rows_s,
    x_s,
    spread_s,
    hidden_s,
    branch_col_s,
    square_s,
    squares_s,
    info_s,
    infos_s,
    answer_s,
    part_s,
    joint_s,
    pair_s,
    first_a,
    first_b,
    turn_a,
    turn_b,
    second_a,
    second_b,
    level_s,
    levels_s,
    ld,
    kv_sem,
    z_recv,
    rows_send,
    x_recv,
    y_recv,
    da_recv,
    db_recv,
    f_recv,
    i_send,
    i_recv,
    q_send,
    q_recv,
    back_send,
    c_recv,
    s1a_recv,
    s1b_recv,
    s2a_recv,
    s2b_recv,
    zz_recv,
):
    kind = jnp.float32
    half_type = jnp.bfloat16
    n = infos_s.shape[0]
    chips = n // 2
    deep = x_s.shape[0]
    plane = chips // deep
    side = 2
    seqs, width = tokens_s.shape
    block, wide = rows_s.shape[1:]
    cut = wide // 2
    fold = wide - width
    folds = width // fold
    spare = seqs - block
    members = 2 * plane
    bulk = members * block
    tail = members * spare
    length, pair = keys_s.shape[1:]
    group = HEADS // KV_HEADS
    tiles = HEADS * HEAD_DIM // pair
    me = lax.axis_index("ep")
    core = lax.rem(me, 2)
    chip = me // 2
    other = chip * 2 + 1 - core
    level = chip // plane
    spot = lax.rem(chip, plane)
    row = spot // side
    col = lax.rem(spot, side)

    barrier = pltpu.get_barrier_semaphore()

    @pl.loop(1, n)
    def _(k):
        pl.semaphore_signal(
            barrier,
            inc=1,
            device_id=(lax.rem(me + k, n),),
            device_id_type=pl.DeviceIdType.MESH,
        )

    heads_wide = HEADS * HEAD_DIM
    loads = [
        (tokens_h, tokens_s),
        (gain_h, gain_s),
        (w_query_h, w_qkv_s.at[:, 0:heads_wide]),
        (w_key_h, w_qkv_s.at[:, heads_wide : heads_wide + pair]),
        (w_value_h, w_qkv_s.at[:, heads_wide + pair : heads_wide + 2 * pair]),
        (w_forget_h, w_forget_s),
        (bias_h, bias_s),
        (lengths_h, lengths_s),
        (logcum_h, logcum_s),
        (ids_h, ids_s),
        (weights_h, weights_s),
    ]
    later = [
        (w_out_h, w_out_s),
        (gain_next_h, gain_next_s),
        (d_gate_h, d_in_s.at[:, 0:pair]),
        (d_up_h, d_in_s.at[:, pair : 2 * pair]),
        (d_gain_h, d_gain_s),
        (branch_h, branch_s),
        (e_gate_h.at[0], e_gate_s),
        (e_up_h.at[0], e_up_s),
        (e_down_h.at[0], e_down_s),
        (d_down_h, d_down_s),
    ]
    copies = [
        pltpu.make_async_copy(source, target, ld.at[at])
        for at, (source, target) in enumerate(loads + later)
    ]
    batch = seqs // kv_sem.shape[1]
    groups = kv_sem.shape[1]

    def cached(at):
        part = pl.ds(at * batch, batch)
        return (
            pltpu.make_async_copy(keys_h.at[part], keys_s.at[part], kv_sem.at[0, at]),
            pltpu.make_async_copy(values_h.at[part], values_s.at[part], kv_sem.at[1, at]),
        )

    for copy in copies[: len(loads)]:
        copy.start()

    @pl.loop(0, groups)
    def _(at):
        for copy in cached(at):
            copy.start()

    for copy in copies[len(loads) :]:
        copy.start()

    for at in (1, 2):
        copies[len(loads) - at].wait()

    experts = lax.broadcasted_iota(jnp.int32, (n, seqs), 0)
    matched = jnp.zeros((n, seqs), kind)
    for at in range(TOPK):
        chosen = ids_s[at : at + 1, :] == experts
        matched = matched + jnp.where(chosen, weights_s[at : at + 1, :], 0.0)
    token = lax.broadcasted_iota(jnp.int32, (seqs, 2 * bulk), 0)
    spread = lax.broadcasted_iota(jnp.int32, (seqs, 2 * bulk), 1)
    member = core * plane + spot
    exact = lax.Precision.HIGHEST
    in_block = (token < block) & (spread == member * block + token)
    in_tail = (token >= block) & (spread == bulk + (token - block) * members + member)
    spread = jnp.where(in_block | in_tail, 1.0, 0.0)
    spread = jnp.dot(matched, spread, preferred_element_type=kind, precision=exact)
    for at in range(n):
        info_s[at] = spread[at : at + 1, :]
    infos_s[pl.ds(me, 1)] = info_s[pl.ds(me, 1)]
    square_s[...] = jnp.zeros_like(square_s)

    for at in range(9):
        copies[at].wait()

    normed = normalize(tokens_s[...].astype(kind), gain_s[...]).astype(half_type)
    product = jnp.dot(normed, w_qkv_s[...], preferred_element_type=kind)
    product = product.astype(half_type).astype(kind)
    key_s[...] = product[:, heads_wide : heads_wide + pair]
    value_s[...] = product[:, heads_wide + pair : heads_wide + 2 * pair]
    lane = lax.broadcasted_iota(jnp.int32, (seqs, pair), 1)
    for head in range(HEADS):
        piece = product[:, head // 2 * pair : (head // 2 + 1) * pair]
        if head % 2 != head // group:
            piece = pltpu.roll(piece, HEAD_DIM, 1)
        piece = jnp.where(lane // HEAD_DIM == head // group, piece, 0.0)
        query_s[pl.ds(head, seqs, stride=HEADS), :] = piece
    forget = lax.dot_general(
        w_forget_s[...], normed, (((1,), (1,)), ((), ())), preferred_element_type=kind
    )
    eye = lax.broadcasted_iota(jnp.int32, (HEADS, HEADS), 0)
    eye = eye == lax.broadcasted_iota(jnp.int32, (HEADS, HEADS), 1)
    forget = forget + to_column(bias_s[...], eye)
    forget_s[...] = jnp.minimum(forget, 0.0) - jnp.log1p(jnp.exp(-jnp.abs(forget)))

    seq_lane = lax.broadcasted_iota(jnp.int32, forget_s.shape, 1)
    position = lax.broadcasted_iota(jnp.int32, (HEADS, length), 1)
    unit = HEAD_DIM ** (-0.5)

    def attend(at):
        for copy in cached(at):
            copy.wait()
        scores_all = []
        own_all = []
        for item in range(batch):
            seq = at * batch + item
            query = query_s[pl.ds(pl.multiple_of(seq * HEADS, HEADS), HEADS), :]
            own = jnp.sum(query * key_s[pl.ds(seq, 1), :], axis=1, keepdims=True) * unit
            forget = jnp.sum(jnp.where(seq_lane == seq, forget_s[...], 0.0), axis=1, keepdims=True)
            cum = logcum_s[seq]
            live = lengths_s[seq]
            last = jnp.sum(jnp.where(position == live - 1, cum, 0.0), axis=1, keepdims=True)
            scores = lax.dot_general(
                query.astype(half_type),
                keys_s[seq],
                (((1,), (1,)), ((), ())),
                preferred_element_type=kind,
            )
            scores = scores * unit + ((last + forget) - cum)
            scores_all.append(jnp.where(position < live, scores, -jnp.inf))
            own_all.append(own)
        scores = jnp.concatenate(scores_all, axis=0)
        own = jnp.concatenate(own_all, axis=0)
        top = jnp.maximum(jnp.max(scores, axis=1, keepdims=True), own)
        expo = jnp.exp(scores - top)
        own_expo = jnp.exp(own - top)
        total = jnp.sum(expo, axis=1, keepdims=True) + own_expo
        share = (expo / total).astype(half_type)
        own_share = (own_expo / total).astype(half_type).astype(kind)
        for item in range(batch):
            seq = at * batch + item
            part = slice(item * HEADS, (item + 1) * HEADS)
            result = jnp.dot(share[part], values_s[seq], preferred_element_type=kind)
            result = result + own_share[part] * value_s[pl.ds(seq, 1), :]
            heads_s[pl.ds(pl.multiple_of(seq * HEADS, HEADS), HEADS), :] = result

    def inform(k):
        to = lax.rem(me + k, n)
        return reach(info_s.at[to], infos_s.at[me], i_send.at[0], i_recv.at[0], to)

    def informed():
        every = infos_s.at[pl.ds(0, n - 1)]
        return reach(every, every, i_send.at[0], i_recv.at[0], other)

    pl.loop(0, groups // 2)(attend)
    pl.semaphore_wait(barrier, n - 1)

    @pl.loop(1, n)
    def _(k):
        inform(k).start()

    pl.loop(groups // 2, groups)(attend)

    for at in range(len(loads), len(loads) + 6):
        copies[at].wait()

    found = [heads_s[pl.ds(head, seqs, stride=HEADS), :] for head in range(HEADS)]
    pieces = []
    for tile in range(tiles):
        left, right = found[2 * tile], found[2 * tile + 1]
        if 2 * tile // group:
            left = pltpu.roll(left, HEAD_DIM, 1)
        else:
            right = pltpu.roll(right, HEAD_DIM, 1)
        pieces.append(jnp.where(lane < HEAD_DIM, left, right))
    attended = jnp.concatenate(pieces, axis=1).astype(half_type)
    mixed = tokens_s[...].astype(kind) + jnp.dot(
        attended, w_out_s[...], preferred_element_type=kind
    )
    mixed = mixed.astype(half_type).astype(kind)
    mixed_s[...] = mixed
    routed = normalize(mixed, gain_next_s[...])

    def slot(at, which, place):
        return (at * 2 + which) * plane + place

    home = slot(level, core, spot)
    for part in range(folds):
        fold_s[pl.ds(part * spare, spare), :] = routed[block:, part * fold : (part + 1) * fold]
    rows_s[home, :, 0:width] = routed[:block].astype(half_type)
    rows_s[home, :, width:wide] = fold_s[...].astype(half_type)

    def device(z, y, x, which):
        return ((z * side + y) * side + x) * 2 + which

    spot_x = row * side + 1 - col
    spot_y = (1 - row) * side + col
    spot_d = (1 - row) * side + 1 - col
    near_x = device(level, row, 1 - col, core)
    near_y = device(level, 1 - row, col, core)

    def part_of(at, place, piece):
        return rows_s.at[slot(at, core, place), :, piece * cut : (piece + 1) * cut]

    def along(at, to, piece):
        here = part_of(at, spot, piece)
        to = device(to, row, col, core)
        return reach(here, here, rows_send.at[0], z_recv.at[piece, at], to)

    def beside(at, place, piece):
        here = part_of(at, place, piece)
        return reach(here, here, rows_send.at[0], x_recv.at[piece, at], near_x)

    def above(at, place, piece):
        here = part_of(at, place, piece)
        return reach(here, here, rows_send.at[0], y_recv.at[piece, at], near_y)

    def relay_a(at, place):
        here = rows_s.at[slot(at, core, place), :, 0:cut]
        return reach(here, here, rows_send.at[0], da_recv.at[at], near_y)

    def relay_b(at, place):
        here = rows_s.at[slot(at, core, place), :, cut:wide]
        return reach(here, here, rows_send.at[0], db_recv.at[at], near_x)

    def across(at, which, place):
        here = rows_s.at[slot(at, which, place)]
        return reach(here, here, rows_send.at[0], f_recv.at[at], other)

    def crossed(at):
        here = rows_s.at[pl.ds(slot(at, 1 - core, 0), plane)]
        return reach(here, here, rows_send.at[0], f_recv.at[at], other)

    balance = jnp.minimum(level, deep - 1 - level)
    lean = jnp.where(2 * level < deep - 1, 1, -1)

    def ordered(j):
        paired = jnp.where(lax.rem(j, 2) == 1, -1, 1) * ((j + 1) // 2)
        single = lean * (j - balance)
        return level + jnp.where(j <= 2 * balance, paired, single)

    rank = jnp.where(level == 0, deep - 2, jnp.where(level == deep - 1, level, level - 1))

    def returned(j):
        k = j + jnp.where(j >= rank, 1, 0)
        k = jnp.where(k < deep - 2, k + 1, jnp.where(k == deep - 2, 0, deep - 1))
        return jnp.where(j == deep - 1, level, k)

    def share(k, at):
        return reach(
            square_s.at[at],
            squares_s.at[at, k],
            q_send.at[0],
            q_recv.at[at],
            lax.rem(me + k, n),
        )

    def shared(at):
        every = squares_s.at[at, pl.ds(1, n - 1)]
        return reach(every, every, q_send.at[0], q_recv.at[at], other)

    def sent(blocks, sem):
        every = rows_s.at[pl.ds(0, blocks)]
        return reach(every, every, sem, sem, other)

    def spread_piece(at, piece):
        if piece:
            above(at, spot, piece).start()
            beside(at, spot, piece).start()
        else:
            beside(at, spot, piece).start()
            above(at, spot, piece).start()

    for piece in range(2):
        spread_piece(level, piece)

    @pl.loop(1, deep)
    def _(j):
        for piece in range(2):
            along(level, ordered(j), piece).start()

    across(level, core, spot).start()

    for at in range(len(loads) + 6, len(loads) + len(later)):
        copies[at].wait()

    ones = jnp.ones((8, pair), kind)
    same_bulk = lax.broadcasted_iota(jnp.int32, (bulk, bulk), 0)
    same_bulk = same_bulk == lax.broadcasted_iota(jnp.int32, (bulk, bulk), 1)
    tail_at = lax.broadcasted_iota(jnp.int32, (tail, bulk), 1)
    tail_of = lax.broadcasted_iota(jnp.int32, (tail, bulk), 0)

    def dense_units(at):
        crossed(at).wait_recv()

        part = pl.ds(at * members, members)
        x_s[at, 0:bulk, :] = rows_s[part, :, 0:width].reshape(bulk, width)
        folded = rows_s[part, :, width:wide].astype(kind).reshape(bulk, fold)
        for tile in range(fold // pair):
            spread_s[tile] = folded[:, tile * pair : (tile + 1) * pair]
        for piece in range(folds):
            for tile in range(fold // pair):
                lanes = slice(piece * fold + tile * pair, piece * fold + (tile + 1) * pair)
                taken = [
                    spread_s[tile, pl.ds(piece * spare + extra, members, stride=block), :]
                    for extra in range(spare)
                ]
                x_s[at, bulk : bulk + tail, lanes] = jnp.concatenate(taken, axis=0).astype(
                    half_type
                )
        values = x_s[at]
        inner = jnp.sum(values.astype(kind) * branch_s[...], axis=1, keepdims=True)
        branch_col_s[at] = jnp.broadcast_to(jax.nn.sigmoid(inner), (bulk + tail, pair))
        both = jnp.dot(values, d_in_s[...], preferred_element_type=kind)
        gate, up = both[:, 0:pair], both[:, pair : 2 * pair]
        units = (gate * jax.nn.sigmoid(gate) * up).astype(half_type).astype(kind)
        hidden_s[at] = (units * d_gain_s[pl.ds(me, 1), :]).astype(half_type)
        squares = lax.dot_general(
            ones,
            units * units,
            (((1,), (1,)), ((), ())),
            preferred_element_type=kind,
            precision=exact,
        )
        square_s[at, :, 0:bulk] = squares[0:1, 0:bulk]
        square_s[at, :, bulk : bulk + tail] = squares[0:1, bulk : bulk + tail]
        squares_s[at, 0] = square_s[at]

        @pl.loop(1, n)
        def _(k):
            share(k, at).start()

    def run_expert(at):
        values = x_s[at]
        gate = jnp.minimum(jnp.dot(values, e_gate_s[...], preferred_element_type=kind), LIMIT)
        up = jnp.clip(jnp.dot(values, e_up_s[...], preferred_element_type=kind), -LIMIT, LIMIT)
        act = ((up + 1.0) * gate * jax.nn.sigmoid(gate * ALPHA)).astype(half_type)
        answer_s[at] = jnp.dot(act, e_down_s[...], preferred_element_type=kind).astype(half_type)

    def columns(line):
        main = to_column(line[:, 0:bulk], same_bulk)
        ends = jnp.where(tail_at == tail_of, line[:, bulk : 2 * bulk], 0.0)
        return main, jnp.sum(ends, axis=1, keepdims=True)

    def cross(at):
        return reach(
            part_s.at[at, pl.ds((1 - core) * plane, plane)],
            joint_s.at[at],
            back_send.at[0],
            c_recv.at[at],
            other,
        )

    def first(at, k):
        place_a = lax.rem(row + 1 + k, side)
        place_b = lax.rem(col + 1 + k, side)
        return (
            reach(
                pair_s.at[at, place_a * side + 1 - col, :, 0:cut],
                first_a.at[at, place_a],
                back_send.at[0],
                s1a_recv.at[at, lax.rem(place_a + row, side)],
                near_x,
            ),
            reach(
                pair_s.at[at, (1 - row) * side + place_b, :, cut:wide],
                first_b.at[at, place_b],
                back_send.at[0],
                s1b_recv.at[at, lax.rem(place_b + col, side)],
                near_y,
            ),
        )

    def second(at):
        return (
            reach(turn_a.at[at], second_a.at[at], back_send.at[0], s2a_recv.at[at], near_y),
            reach(turn_b.at[at], second_b.at[at], back_send.at[0], s2b_recv.at[at], near_x),
        )

    def home_to(at):
        return reach(
            level_s.at[at],
            levels_s.at[level],
            back_send.at[0],
            zz_recv.at[level],
            device(at, row, col, core),
        )

    def home_from(at):
        return reach(
            level_s.at[at],
            levels_s.at[at],
            back_send.at[0],
            zz_recv.at[at],
            device(at, row, col, core),
        )

    def combine(at):
        shared(at).wait_recv()
        dense = jnp.dot(hidden_s[at], d_down_s[...], preferred_element_type=kind)
        coef = jnp.sum(infos_s[pl.ds(at * members, members)], axis=0)
        scale = lax.rsqrt(jnp.sum(squares_s[at], axis=0) / units_total + EPS)
        weight, weight_end = columns(coef)
        scale, scale_end = columns(scale)
        twice = branch_col_s[at, :, 0:1]
        main = weight * answer_s[at, 0:bulk, :].astype(kind)
        main = main + (scale * twice[0:bulk]) * dense[0:bulk]
        ends = weight_end * answer_s[at, bulk : bulk + tail, :].astype(kind)
        ends = ends + (scale_end * twice[bulk:]) * dense[bulk:]
        part_s[at, :, :, 0:width] = main.astype(half_type).reshape(members, block, width)
        for piece in range(folds):
            for tile in range(fold // pair):
                first_lane = piece * fold + tile * pair
                for extra in range(spare):
                    spread_s[tile, pl.ds(piece * spare + extra, members, stride=block), :] = (
                        ends[
                            extra * members : (extra + 1) * members,
                            first_lane : first_lane + pair,
                        ]
                    )
        for tile in range(fold // pair):
            part_s[at, :, :, width + tile * pair : width + (tile + 1) * pair] = (
                spread_s[tile].astype(half_type).reshape(members, block, pair)
            )
        cross(at).start()

    def join(at):
        cross(at).wait_recv()
        mine = part_s[at, pl.ds(core * plane, plane)].astype(kind)
        pair_s[at] = (mine + joint_s[at].astype(kind)).astype(half_type)
        for k in range(side):
            for copy in first(at, k):
                copy.start()

    def turn(at):
        for copy in first(at, 0):
            copy.wait_recv()
        turned = pair_s[at, spot_y, :, 0:cut].astype(kind) + first_a[at, 1 - row].astype(kind)
        turn_a[at] = turned.astype(half_type)
        turned = pair_s[at, spot_x, :, cut:wide].astype(kind) + first_b[at, 1 - col].astype(kind)
        turn_b[at] = turned.astype(half_type)
        for copy in second(at):
            copy.start()

    def settle(at):
        for copy in first(at, 1):
            copy.wait_recv()
        for copy in second(at):
            copy.wait_recv()
        total = pair_s[at, spot, :, 0:cut].astype(kind) + first_a[at, row].astype(kind)
        total = total + second_a[at].astype(kind)
        level_s[at, :, 0:cut] = total.astype(half_type)
        total = pair_s[at, spot, :, cut:wide].astype(kind) + first_b[at, col].astype(kind)
        total = total + second_b[at].astype(kind)
        level_s[at, :, cut:wide] = total.astype(half_type)

        @pl.when(at != level)
        def _():
            home_to(at).start()

    def native(at):
        for piece in range(2):
            along(at, 0, piece).wait_recv()
            spread_piece(at, piece)
        across(at, core, spot).start()

    def relay(at):
        beside(at, spot_x, 0).wait_recv()
        relay_a(at, spot_x).start()
        above(at, spot_y, 1).wait_recv()
        relay_b(at, spot_y).start()
        beside(at, spot_x, 1).wait_recv()
        across(at, core, spot_x).start()
        above(at, spot_y, 0).wait_recv()
        across(at, core, spot_y).start()

    def corner(at):
        relay_a(at, spot_d).wait_recv()
        relay_b(at, spot_d).wait_recv()
        across(at, core, spot_d).start()

    def at_step(step, start, stop, act, lag, order):
        @pl.when((step >= start) & (step < stop))
        def _():
            act(order(step - lag))

    relay(ordered(0))
    native(ordered(1))
    corner(ordered(0))
    native(ordered(2))
    relay(ordered(1))
    native(ordered(3))
    dense_units(ordered(0))
    relay(ordered(2))
    corner(ordered(1))
    run_expert(ordered(0))
    relay(ordered(3))
    corner(ordered(2))
    dense_units(ordered(1))
    dense_units(ordered(2))
    corner(ordered(3))
    run_expert(ordered(1))
    dense_units(ordered(3))
    run_expert(ordered(2))
    run_expert(ordered(3))

    informed().wait_recv()

    @pl.loop(0, deep + 3)
    def _(step):
        at_step(step, 0, deep, combine, 0, returned)
        at_step(step, 1, deep + 1, join, 1, returned)
        at_step(step, 2, deep + 2, turn, 2, returned)
        at_step(step, 3, deep + 3, settle, 3, returned)

    total = level_s[level].astype(kind)
    for j in range(deep - 1):
        at = returned(j)
        home_from(at).wait_recv()
        total = total + levels_s[at].astype(kind)
    out[0:block, :] = (mixed_s[0:block, :] + total[:, 0:width]).astype(half_type)
    fold_s[...] = total[:, width:wide]
    for part in range(folds):
        lanes = slice(part * fold, (part + 1) * fold)
        ends = mixed_s[block:seqs, lanes] + fold_s[pl.ds(part * spare, spare), :]
        out[block:seqs, lanes] = ends.astype(half_type)

    sent(chips + 4 * deep - 1, rows_send.at[0]).wait_send()
    sent(chips + 4 * deep - 1, back_send.at[0]).wait_send()
    informed().wait_send()
    every = squares_s.at[:, pl.ds(1, n - 1)]
    reach(every, every, q_send.at[0], q_recv.at[0], other).wait_send()


def fast(n, deep, arrays, units_total):
    (tokens, keys, logcum, e_gate, e_down, d_gate, d_gain) = (
        arrays[0],
        arrays[8],
        arrays[10],
        arrays[15],
        arrays[17],
        arrays[18],
        arrays[21],
    )
    seqs, width = tokens.shape
    length, pair = keys.shape[1:]
    hidden = e_gate.shape[2]
    local = d_gate.shape[1]
    chips = n // 2
    plane = chips // deep
    block = seqs // 16 * 16
    spare = seqs - block
    wide = width + spare * width // block
    fold = wide - width
    cut = wide // 2
    members = 2 * plane
    bulk = members * block
    tail = members * spare
    heads_wide = HEADS * HEAD_DIM
    half_type = jnp.bfloat16
    kind = jnp.float32
    dma = pltpu.SemaphoreType.DMA
    groups = 3
    vmem = pltpu.VMEM
    scratch = [
        vmem((seqs, width), half_type),
        vmem((1, width), kind),
        vmem((width, heads_wide + 2 * pair), half_type),
        vmem((HEADS, width), half_type),
        vmem((1, HEADS), kind),
        vmem((heads_wide, width), half_type),
        vmem((seqs, length, pair), half_type),
        vmem((seqs, length, pair), half_type),
        vmem((seqs, HEADS, length), kind),
        pltpu.SMEM((seqs,), jnp.int32),
        vmem((1, width), kind),
        vmem((TOPK, seqs), jnp.int32),
        vmem((TOPK, seqs), kind),
        vmem((width, hidden), half_type),
        vmem((width, hidden), half_type),
        vmem((hidden, width), half_type),
        vmem((width, 2 * local), half_type),
        vmem((local, width), half_type),
        vmem(d_gain.shape, kind),
        vmem((1, width), kind),
        vmem((seqs * HEADS, pair), kind),
        vmem((seqs, pair), kind),
        vmem((seqs, pair), kind),
        vmem((HEADS, seqs), kind),
        vmem((seqs * HEADS, pair), kind),
        vmem((seqs, width), kind),
        vmem((block, fold), kind),
        vmem((n, block, wide), half_type),
        vmem((deep, bulk + tail, width), half_type),
        vmem((fold // pair, bulk, pair), kind),
        vmem((deep, bulk + tail, local), half_type),
        vmem((deep, bulk + tail, pair), kind),
        vmem((deep, 1, 2 * bulk), kind),
        vmem((deep, n, 1, 2 * bulk), kind),
        vmem((n, 1, 2 * bulk), kind),
        vmem((n, 1, 2 * bulk), kind),
        vmem((deep, bulk + tail, width), half_type),
        vmem((deep, members, block, wide), half_type),
        vmem((deep, plane, block, wide), half_type),
        vmem((deep, plane, block, wide), half_type),
        vmem((deep, 2, block, cut), half_type),
        vmem((deep, 2, block, cut), half_type),
        vmem((deep, block, cut), half_type),
        vmem((deep, block, cut), half_type),
        vmem((deep, block, cut), half_type),
        vmem((deep, block, cut), half_type),
        vmem((deep, block, wide), half_type),
        vmem((deep, block, wide), half_type),
        dma((21,)),
        dma((2, groups)),
        dma((2, deep)),
        dma((1,)),
        dma((2, deep)),
        dma((2, deep)),
        dma((deep,)),
        dma((deep,)),
        dma((deep,)),
        dma((1,)),
        dma((1,)),
        dma((1,)),
        dma((deep,)),
        dma((1,)),
        dma((deep,)),
        dma((deep, 2)),
        dma((deep, 2)),
        dma((deep,)),
        dma((deep,)),
        dma((deep,)),
    ]
    return pl.pallas_call(
        functools.partial(fast_body, units_total),
        out_shape=jax.ShapeDtypeStruct(tokens.shape, half_type),
        in_specs=[pl.BlockSpec(memory_space=pl.ANY)] * len(arrays),
        out_specs=pl.BlockSpec(memory_space=pltpu.VMEM),
        scratch_shapes=scratch,
        compiler_params=pltpu.CompilerParams(
            collective_id=0, has_side_effects=True, vmem_limit_bytes=62 * 1024 * 1024
        ),
        name="layer",
    )(*arrays)


def shards(
    tokens,
    attn_norm_gain,
    w_query,
    w_key,
    w_value,
    w_forget,
    forget_bias,
    w_attn_out,
    cache_keys,
    cache_values,
    cache_logcum,
    cache_lengths,
    expert_norm_gain,
    expert_ids,
    expert_weights,
    w_expert_gate,
    w_expert_up,
    w_expert_down,
    w_dense_gate,
    w_dense_up,
    w_dense_down,
    dense_norm_gain,
    branch_gate,
):
    n = lax.axis_size("ep")
    deep = 4
    seqs, width = tokens.shape
    local = w_dense_gate.shape[1]
    spare = seqs % 16
    fits = n == 8 * deep and local == cache_keys.shape[2] and 0 < spare and spare * width % 2048 == 0
    if fits and seqs // 16 == 1:
        return fast(
            n,
            deep,
            (
                tokens,
                attn_norm_gain[None, :],
                w_query,
                w_key,
                w_value,
                w_forget.T,
                forget_bias[None, :],
                w_attn_out,
                cache_keys,
                cache_values,
                cache_logcum,
                cache_lengths,
                expert_norm_gain[None, :],
                expert_ids.T,
                expert_weights.T,
                w_expert_gate,
                w_expert_up,
                w_expert_down,
                w_dense_gate,
                w_dense_up,
                w_dense_down,
                dense_norm_gain.reshape(n, local),
                branch_gate[None, :],
            ),
            dense_norm_gain.shape[0],
        )
    mixed, routed_in = front(
        tokens,
        attn_norm_gain,
        w_query,
        w_key,
        w_value,
        w_forget,
        forget_bias,
        w_attn_out,
        cache_keys,
        cache_values,
        cache_logcum,
        cache_lengths,
        expert_norm_gain,
    )
    n = lax.axis_size("ep")
    me = lax.axis_index("ep")
    seqs = tokens.shape[0]
    extra = jnp.concatenate([expert_ids.astype(jnp.bfloat16), *split3(expert_weights)], axis=1)
    packed = jnp.concatenate([routed_in, jnp.pad(extra, ((0, 0), (0, 128 - 4 * TOPK)))], axis=1)
    packed = jnp.pad(packed, ((0, -seqs % 8), (0, 0)))
    local = w_dense_gate.shape[1]
    gain = lax.dynamic_slice_in_dim(dense_norm_gain, me * local, local, 0)
    return rest(
        n,
        packed,
        mixed,
        w_expert_gate[0],
        w_expert_up[0],
        w_expert_down[0],
        w_dense_gate,
        w_dense_up,
        w_dense_down,
        gain[None, :],
        branch_gate[None, :],
        dense_norm_gain.shape[0],
    )


def solution(mesh):
    in_specs = (
        P("ep", None),
        P(),
        P(),
        P(),
        P(),
        P(),
        P(),
        P(),
        P("ep", None, None),
        P("ep", None, None),
        P("ep", None, None),
        P("ep"),
        P(),
        P("ep", None),
        P("ep", None),
        P("ep", None, None),
        P("ep", None, None),
        P("ep", None, None),
        P(None, "ep"),
        P(None, "ep"),
        P("ep", None),
        P(),
        P(),
    )
    out_specs = P("ep", None)
    return jax.shard_map(shards, mesh=mesh, in_specs=in_specs, out_specs=out_specs, check_vma=False)
```

```python
import functools

import jax
import jax.numpy as jnp
from jax import lax
from jax.experimental import pallas as pl
from jax.experimental.pallas import tpu as pltpu
from jax.sharding import PartitionSpec as P

HEADS = 8
KV_HEADS = 2
HEAD_DIM = 64
TOPK = 6


EPS = 1e-06
LIMIT = 7.0
ALPHA = 1.702


def normalize(values, gain):
    return values * lax.rsqrt(jnp.mean(values * values, axis=-1, keepdims=True) + EPS) * gain


def stored(values):
    return lax.optimization_barrier(values.astype(jnp.bfloat16))


def front_body(
    lengths,
    tokens,
    gain_ref,
    w_query,
    w_key,
    w_value,
    w_forget,
    bias,
    w_out,
    gain_next,
    keys,
    values,
    logcum,
    mixed_ref,
    routed_ref,
    query_s,
    key_s,
    value_s,
    forget_s,
    attended_s,
):
    step = pl.program_id(0)
    batch, length, pair = keys.shape
    rows = jnp.float32
    group = HEADS // KV_HEADS
    tiles = HEADS * HEAD_DIM // pair

    @pl.when(step == 0)
    def _():
        normed = normalize(tokens[...].astype(rows), gain_ref[...]).astype(jnp.bfloat16)
        for weight, kept in ((w_key, key_s), (w_value, value_s)):
            product = jnp.dot(normed, weight[...], preferred_element_type=rows)
            kept[...] = product.astype(jnp.bfloat16).astype(rows)
        product = jnp.dot(normed, w_query[...], preferred_element_type=rows)
        product = product.astype(jnp.bfloat16).astype(rows)
        for tile in range(tiles):
            query_s[tile] = product[:, tile * pair : (tile + 1) * pair]
        forget = lax.dot_general(
            w_forget[...], normed, (((1,), (1,)), ((), ())), preferred_element_type=rows
        )
        forget = forget + bias[...]
        forget_s[...] = jnp.minimum(forget, 0.0) - jnp.log1p(jnp.exp(-jnp.abs(forget)))

    lane = lax.broadcasted_iota(jnp.int32, (HEADS, pair), 1)
    head = lax.broadcasted_iota(jnp.int32, (HEADS, pair), 0)
    odd = lane // HEAD_DIM
    place = head // group
    seq_lane = lax.broadcasted_iota(jnp.int32, forget_s.shape, 1)
    position = lax.broadcasted_iota(jnp.int32, (HEADS, length), 1)
    scale = HEAD_DIM ** (-0.5)
    for item in range(batch):
        seq = step * batch + item
        stay = jnp.zeros((HEADS, pair), rows)
        move = jnp.zeros((HEADS, pair), rows)
        for tile in range(tiles):
            piece = jnp.broadcast_to(
                query_s[tile, pl.ds(seq, 1), :], (HEADS, pair)
            )
            own_lanes = head == 2 * tile + odd
            stay = jnp.where(own_lanes & (odd == place), piece, stay)
            move = jnp.where(own_lanes & (odd != place), piece, move)
        query = stay + pltpu.roll(move, HEAD_DIM, 1)
        own = jnp.sum(query * key_s[pl.ds(seq, 1), :], axis=1, keepdims=True) * scale
        forget = jnp.sum(jnp.where(seq_lane == seq, forget_s[...], 0.0), axis=1, keepdims=True)
        cum = logcum[item]
        live_count = lengths[seq]
        last = jnp.sum(jnp.where(position == live_count - 1, cum, 0.0), axis=1, keepdims=True)
        scores = lax.dot_general(
            query.astype(jnp.bfloat16),
            keys[item],
            (((1,), (1,)), ((), ())),
            preferred_element_type=rows,
        )
        scores = scores * scale + ((last + forget) - cum)
        scores = jnp.where(position < live_count, scores, -jnp.inf)
        top = jnp.maximum(jnp.max(scores, axis=1, keepdims=True), own)
        expo = jnp.exp(scores - top)
        own_expo = jnp.exp(own - top)
        total = jnp.sum(expo, axis=1, keepdims=True) + own_expo
        weights = (expo / total).astype(jnp.bfloat16)
        own_weight = (own_expo / total).astype(jnp.bfloat16).astype(rows)
        out = jnp.dot(weights, values[item], preferred_element_type=rows)
        out = out + own_weight * value_s[pl.ds(seq, 1), :]
        turned = pltpu.roll(out, HEAD_DIM, 1)
        for tile in range(tiles):
            own_lanes = head == 2 * tile + odd
            part = jnp.where(own_lanes, jnp.where(odd == place, out, turned), 0.0)
            attended_s[tile, pl.ds(seq, 1), :] = jnp.sum(part, axis=0, keepdims=True)

    @pl.when(step == pl.num_programs(0) - 1)
    def _():
        attended = jnp.concatenate([attended_s[tile] for tile in range(tiles)], axis=1)
        attended = attended.astype(jnp.bfloat16)
        mixed = tokens[...].astype(rows) + jnp.dot(
            attended, w_out[...], preferred_element_type=rows
        )
        mixed = mixed.astype(jnp.bfloat16)
        mixed_ref[...] = mixed
        routed_ref[...] = normalize(mixed.astype(rows), gain_next[...]).astype(jnp.bfloat16)


def front(
    tokens, gain, w_query, w_key, w_value, w_forget, bias, w_out, keys, values, logcum, lengths, gain_next
):
    seqs, width = tokens.shape
    batch = max(size for size in (1, 2, 3) if seqs % size == 0)
    pair = keys.shape[2]

    def whole(*shape):
        return pl.BlockSpec(shape, lambda i, *_: (0,) * len(shape))

    def each(*shape):
        return pl.BlockSpec((batch, *shape), lambda i, *_: (i, 0, 0))

    small = (
        tokens,
        gain[None, :],
        w_query,
        w_key,
        w_value,
        w_forget.T,
        bias[:, None],
        w_out,
        gain_next[None, :],
    )
    kept = jax.ShapeDtypeStruct((seqs, width), jnp.bfloat16)
    return pl.pallas_call(
        front_body,
        out_shape=(kept, kept),
        grid_spec=pltpu.PrefetchScalarGridSpec(
            num_scalar_prefetch=1,
            grid=(seqs // batch,),
            in_specs=[whole(*array.shape) for array in small]
            + [each(*keys.shape[1:]), each(*values.shape[1:]), each(*logcum.shape[1:])],
            out_specs=[whole(seqs, width)] * 2,
            scratch_shapes=[
                pltpu.VMEM((HEADS * HEAD_DIM // pair, seqs, pair), jnp.float32),
                pltpu.VMEM((seqs, pair), jnp.float32),
                pltpu.VMEM((seqs, pair), jnp.float32),
                pltpu.VMEM((HEADS, seqs), jnp.float32),
                pltpu.VMEM((HEADS * HEAD_DIM // pair, seqs, pair), jnp.float32),
            ],
        ),
        compiler_params=pltpu.CompilerParams(
            dimension_semantics=("arbitrary",), vmem_limit_bytes=40 * 1024 * 1024
        ),
        cost_estimate=pl.CostEstimate(
            flops=10**9, bytes_accessed=16 * 10**6, transcendentals=2 * 10**5
        ),
        name="front",
    )(lengths, *small, keys, values, logcum)


def split3(values):
    parts = []
    for _ in range(3):
        part = stored(values)
        parts.append(part)
        values = values - part.astype(jnp.float32)
    return parts


def expert_unit(rows, gate_w, up_w, down_w):
    gate = jnp.minimum(jnp.dot(rows, gate_w, preferred_element_type=jnp.float32), LIMIT)
    up = jnp.clip(jnp.dot(rows, up_w, preferred_element_type=jnp.float32), -LIMIT, LIMIT)
    act = ((up + 1.0) * gate * jax.nn.sigmoid(gate * ALPHA)).astype(jnp.bfloat16)
    return jnp.dot(act, down_w, preferred_element_type=jnp.float32).astype(jnp.bfloat16)


def reach(source, target, sent, landed, device):
    return pltpu.make_async_remote_copy(
        src_ref=source,
        dst_ref=target,
        send_sem=sent,
        recv_sem=landed,
        device_id=(device,),
        device_id_type=pl.DeviceIdType.MESH,
    )


def to_row(column, same):
    return jnp.sum(jnp.where(same, column, 0.0), axis=0, keepdims=True)


def to_column(row, same):
    return jnp.sum(jnp.where(same, row, 0.0), axis=1, keepdims=True)


def rest_body(
    units_total,
    plane,
    packed,
    mixed,
    w_gate,
    w_up,
    w_down,
    d_gate,
    d_up,
    d_down,
    gain,
    branch,
    out,
    rows_s,
    units_s,
    answer_s,
    coef_s,
    square_s,
    squares_s,
    theirs_s,
    joint_s,
    final_s,
    own_sem,
    ag_send,
    ag_recv,
    fw_send,
    fw_recv,
    sq_send,
    sq_recv,
    d2d_send,
    d2d_recv,
    rs_send,
    rs_recv,
):
    kind = jnp.float32
    n = squares_s.shape[0]
    chips = n // 2
    pad = packed.shape[0]
    width = out.shape[1]
    chunk = units_s.shape[1] // pad
    halves = chips // chunk
    size = chunk * pad
    me = lax.axis_index("ep")
    core = lax.rem(me, 2)
    chip = me // 2
    other = chip * 2 + 1 - core
    mine = core * chips
    peer = (1 - core) * chips

    barrier = pltpu.get_barrier_semaphore()

    @pl.loop(1, n)
    def _(k):
        pl.semaphore_signal(
            barrier,
            inc=1,
            device_id=(lax.rem(me + k, n),),
            device_id_type=pl.DeviceIdType.MESH,
        )

    pl.semaphore_wait(barrier, n - 1)

    deep = chips // plane
    level = chip // plane
    spot = lax.rem(chip, plane)

    def before(dz, dp):
        return lax.rem(level - dz + deep, deep) * plane + lax.rem(spot - dp + plane, plane)

    def along(dz):
        to = lax.rem(level + dz, deep) * plane + spot
        k = dz * plane
        return reach(packed, rows_s.at[mine + chip], ag_send.at[k], ag_recv.at[k], to * 2 + core)

    def across(dz, dp):
        to = level * plane + lax.rem(spot + dp, plane)
        k = dz * plane + dp
        slot = rows_s.at[mine + before(dz, 0)]
        return reach(slot, slot, ag_send.at[k], ag_recv.at[k], to * 2 + core)

    def landed(dz, dp):
        slot = rows_s.at[mine + before(dz, dp)]
        k = dz * plane + dp
        return reach(slot, slot, ag_send.at[k], ag_recv.at[k], before(0, dp) * 2 + core)

    def forward(dz, dp):
        slot = rows_s.at[mine + before(dz, dp)]
        k = dz * plane + dp
        return reach(slot, slot, fw_send.at[k], fw_recv.at[k], other)

    def forwarded(dz, dp):
        slot = rows_s.at[peer + before(dz, dp)]
        k = dz * plane + dp
        return reach(slot, slot, fw_send.at[k], fw_recv.at[k], other)

    keep = pltpu.make_async_copy(packed, rows_s.at[mine + chip], own_sem)
    keep.start()

    @pl.loop(1, deep)
    def _(dz):
        along(dz).start()

    keep.wait()

    @pl.loop(1, plane)
    def _(dp):
        across(0, dp).start()

    forward(0, 0).start()

    @pl.loop(1, deep)
    def _(dz):
        landed(dz, 0).wait_recv()

        @pl.loop(1, plane)
        def _(dp):
            across(dz, dp).start()

        forward(dz, 0).start()

    @pl.loop(0, deep)
    def _(dz):
        @pl.loop(1, plane)
        def _(dp):
            landed(dz, dp).wait_recv()
            forward(dz, dp).start()

    @pl.loop(0, deep)
    def _(dz):
        @pl.loop(0, plane)
        def _(dp):
            forwarded(dz, dp).wait_recv()

    first = lax.broadcasted_iota(jnp.int32, (size, size), 0)
    second = lax.broadcasted_iota(jnp.int32, (size, size), 1)
    same = first == second

    def load(at):
        block = rows_s[pl.ds(at * chunk, chunk)]
        return block.astype(kind).reshape(size, block.shape[2])

    @pl.loop(0, 2 * halves)
    def _(at):
        wide = load(at)
        block = wide[:, :width].astype(jnp.bfloat16)
        gate = jnp.dot(block, d_gate[...], preferred_element_type=kind)
        up = jnp.dot(block, d_up[...], preferred_element_type=kind)
        units = (gate * jax.nn.sigmoid(gate) * up).astype(jnp.bfloat16).astype(kind)
        units_s[at] = units
        square_s[at] = to_row(jnp.sum(units * units, axis=1, keepdims=True), same)
        side = wide[:, width:]
        lane = lax.broadcasted_iota(jnp.int32, side.shape, 1)
        picked = jnp.where((side == me.astype(kind)) & (lane < TOPK), 1.0, 0.0)
        weight = jnp.zeros((size, 1), kind)
        for part in (3, 2, 1):
            moved = pltpu.roll(side, side.shape[1] - part * TOPK, 1)
            weight = weight + jnp.sum(picked * moved, axis=1, keepdims=True)
        branch_scale = jax.nn.sigmoid(
            jnp.sum(wide[:, :width] * branch[...], axis=1, keepdims=True)
        )
        coef_s[at] = jnp.where(lane == 0, weight, branch_scale)

    def share(k):
        return reach(
            square_s, squares_s.at[k], sq_send.at[k], sq_recv.at[k], lax.rem(me + k, n)
        )

    @pl.loop(1, n)
    def _(k):
        share(k).start()

    @pl.loop(0, 2 * halves)
    def _(at):
        block = load(at)[:, :width].astype(jnp.bfloat16)
        answer_s[at] = expert_unit(block, w_gate[...], w_up[...], w_down[...])

    @pl.loop(1, n)
    def _(k):
        share(k).wait_recv()

    squares_s[0] = square_s[...]
    totals = jnp.sum(squares_s[...], axis=0)
    square_rows = lax.rsqrt(totals / units_total + EPS)
    squares_s[0] = square_rows

    def partial(at):
        scale = to_column(squares_s[0, at], same)
        hidden = (units_s[at] * scale * gain[...]).astype(jnp.bfloat16)
        dense = jnp.dot(hidden, d_down[...], preferred_element_type=kind)
        coef = coef_s[at]
        routed = coef[:, 0:1] * answer_s[at].astype(kind)
        return (routed + coef[:, 1:2] * dense).reshape(chunk, pad, width)

    def cross(half):
        part = pl.ds(half * chunk, chunk)
        return reach(theirs_s.at[part], joint_s.at[part], d2d_send.at[half], d2d_recv.at[half], other)

    def back(dz, dp):
        k = dz * plane + dp
        slot = joint_s.at[before(dz, dp)]
        return reach(slot, final_s.at[k], rs_send.at[k], rs_recv.at[k], before(0, dp) * 2 + core)

    def down(dz):
        k = dz * plane
        to = before(dz, 0)
        return reach(joint_s.at[to], final_s.at[k], rs_send.at[k], rs_recv.at[k], to * 2 + core)

    def collected(dz):
        total = joint_s[before(dz, 0)].astype(kind)
        for dp in range(1, plane):
            back(dz, dp).wait_recv()
            total = total + final_s[dz * plane + dp].astype(kind)
        return total

    @pl.loop(0, halves)
    def _(half):
        theirs_s[pl.ds(half * chunk, chunk)] = partial((1 - core) * halves + half).astype(
            jnp.bfloat16
        )
        cross(half).start()

    @pl.loop(0, halves)
    def _(half):
        part = pl.ds(half * chunk, chunk)
        own = partial(core * halves + half)
        cross(half).wait_recv()
        joint_s[part] = (own + joint_s[part].astype(kind)).astype(jnp.bfloat16)

    @pl.loop(1, deep + 1)
    def _(step):
        @pl.loop(1, plane)
        def _(dp):
            back(lax.rem(step, deep), dp).start()

    @pl.loop(1, deep)
    def _(dz):
        joint_s[before(dz, 0)] = collected(dz).astype(jnp.bfloat16)
        down(dz).start()

    total = collected(0)
    for dz in range(1, deep):
        down(dz).wait_recv()
        total = total + final_s[dz * plane].astype(kind)
    result = mixed[...].astype(kind) + total[: mixed.shape[0]]
    out[...] = result.astype(jnp.bfloat16)

    @pl.loop(1, deep)
    def _(dz):
        along(dz).wait_send()
        down(dz).wait_send()

    @pl.loop(0, deep)
    def _(dz):
        forward(dz, 0).wait_send()

        @pl.loop(1, plane)
        def _(dp):
            across(dz, dp).wait_send()
            back(dz, dp).wait_send()
            forward(dz, dp).wait_send()

    @pl.loop(1, n)
    def _(k):
        share(k).wait_send()

    @pl.loop(0, halves)
    def _(half):
        cross(half).wait_send()


def rest(n, packed, mixed, w_gate, w_up, w_down, d_gate, d_up, d_down, gain, branch, units_total):
    pad = packed.shape[0]
    width = mixed.shape[1]
    local = d_gate.shape[1]
    chips = n // 2
    chunk = max(size for size in (1, 2, 4, 8) if chips % size == 0)
    halves = chips // chunk
    plane = chips // 4 if chips % 4 == 0 else chips
    size = chunk * pad
    half_type = jnp.bfloat16
    vmem = pl.BlockSpec(memory_space=pltpu.VMEM)
    dma = pltpu.SemaphoreType.DMA
    return pl.pallas_call(
        functools.partial(rest_body, units_total, plane),
        out_shape=jax.ShapeDtypeStruct(mixed.shape, half_type),
        in_specs=[vmem] * 10,
        out_specs=vmem,
        scratch_shapes=[
            pltpu.VMEM((n, *packed.shape), half_type),
            pltpu.VMEM((2 * halves, size, local), jnp.float32),
            pltpu.VMEM((2 * halves, size, width), half_type),
            pltpu.VMEM((2 * halves, size, 128), jnp.float32),
            pltpu.VMEM((2 * halves, 1, size), jnp.float32),
            pltpu.VMEM((n, 2 * halves, 1, size), jnp.float32),
            pltpu.VMEM((chips, pad, width), half_type),
            pltpu.VMEM((chips, pad, width), half_type),
            pltpu.VMEM((chips, pad, width), half_type),
            dma,
            dma((chips,)),
            dma((chips,)),
            dma((chips,)),
            dma((chips,)),
            dma((n,)),
            dma((n,)),
            dma((halves,)),
            dma((halves,)),
            dma((chips,)),
            dma((chips,)),
        ],
        compiler_params=pltpu.CompilerParams(
            collective_id=0, has_side_effects=True, vmem_limit_bytes=62 * 1024 * 1024
        ),
        name="rest",
    )(packed, mixed, w_gate, w_up, w_down, d_gate, d_up, d_down, gain, branch)


def fast_body(
    units_total,
    tokens_h,
    gain_h,
    w_query_h,
    w_key_h,
    w_value_h,
    w_forget_h,
    bias_h,
    w_out_h,
    keys_h,
    values_h,
    logcum_h,
    lengths_h,
    gain_next_h,
    ids_h,
    weights_h,
    e_gate_h,
    e_up_h,
    e_down_h,
    d_gate_h,
    d_up_h,
    d_down_h,
    d_gain_h,
    branch_h,
    out,
    tokens_s,
    gain_s,
    w_qkv_s,
    w_forget_s,
    bias_s,
    w_out_s,
    keys_s,
    values_s,
    logcum_s,
    lengths_s,
    gain_next_s,
    ids_s,
    weights_s,
    e_in_s,
    e_down_s,
    d_in_s,
    d_down_s,
    d_gain_s,
    branch_s,
    query_s,
    key_s,
    value_s,
    forget_s,
    heads_s,
    mixed_s,
    fold_s,
    rows_s,
    x_s,
    spread_s,
    hidden_s,
    branch_col_s,
    square_s,
    squares_s,
    info_s,
    infos_s,
    answer_s,
    part_s,
    joint_s,
    pair_s,
    first_a,
    first_b,
    turn_a,
    turn_b,
    second_a,
    second_b,
    level_s,
    levels_s,
    ld,
    kv_sem,
    z_recv,
    rows_send,
    x_recv,
    y_recv,
    da_recv,
    db_recv,
    f_recv,
    i_send,
    i_recv,
    q_send,
    q_recv,
    back_send,
    c_recv,
    s1a_recv,
    s1b_recv,
    s2a_recv,
    s2b_recv,
    zz_recv,
):
    kind = jnp.float32
    half_type = jnp.bfloat16
    n = infos_s.shape[0]
    chips = n // 2
    deep = x_s.shape[0]
    plane = chips // deep
    side = 2
    seqs, width = tokens_s.shape
    block, wide = rows_s.shape[1:]
    cut = wide // 2
    fold = wide - width
    folds = width // fold
    spare = seqs - block
    members = 2 * plane
    bulk = members * block
    tail = members * spare
    length, pair = keys_s.shape[1:]
    group = HEADS // KV_HEADS
    tiles = HEADS * HEAD_DIM // pair
    me = lax.axis_index("ep")
    core = lax.rem(me, 2)
    chip = me // 2
    other = chip * 2 + 1 - core
    level = chip // plane
    spot = lax.rem(chip, plane)
    row = spot // side
    col = lax.rem(spot, side)

    barrier = pltpu.get_barrier_semaphore()

    @pl.loop(1, n)
    def _(k):
        pl.semaphore_signal(
            barrier,
            inc=1,
            device_id=(lax.rem(me + k, n),),
            device_id_type=pl.DeviceIdType.MESH,
        )

    heads_wide = HEADS * HEAD_DIM
    loads = [
        (tokens_h, tokens_s),
        (gain_h, gain_s),
        (w_query_h, w_qkv_s.at[:, 0:heads_wide]),
        (w_key_h, w_qkv_s.at[:, heads_wide : heads_wide + pair]),
        (w_value_h, w_qkv_s.at[:, heads_wide + pair : heads_wide + 2 * pair]),
        (w_forget_h, w_forget_s),
        (bias_h, bias_s),
        (lengths_h, lengths_s),
        (logcum_h, logcum_s),
        (ids_h, ids_s),
        (weights_h, weights_s),
    ]
    later = [
        (w_out_h, w_out_s),
        (gain_next_h, gain_next_s),
        (d_gate_h, d_in_s.at[:, 0:pair]),
        (d_up_h, d_in_s.at[:, pair : 2 * pair]),
        (d_gain_h, d_gain_s),
        (branch_h, branch_s),
        (e_gate_h.at[0], e_in_s.at[:, 0 : e_in_s.shape[1] // 2]),
        (e_up_h.at[0], e_in_s.at[:, e_in_s.shape[1] // 2 :]),
        (e_down_h.at[0], e_down_s),
        (d_down_h, d_down_s),
    ]
    copies = [
        pltpu.make_async_copy(source, target, ld.at[at])
        for at, (source, target) in enumerate(loads + later)
    ]
    batch = seqs // kv_sem.shape[1]
    groups = kv_sem.shape[1]

    def cached(at):
        part = pl.ds(at * batch, batch)
        return (
            pltpu.make_async_copy(keys_h.at[part], keys_s.at[part], kv_sem.at[0, at]),
            pltpu.make_async_copy(values_h.at[part], values_s.at[part], kv_sem.at[1, at]),
        )

    for copy in copies[: len(loads)]:
        copy.start()

    @pl.loop(0, groups)
    def _(at):
        for copy in cached(at):
            copy.start()

    for copy in copies[len(loads) :]:
        copy.start()

    for at in (1, 2):
        copies[len(loads) - at].wait()

    experts = lax.broadcasted_iota(jnp.int32, (n, seqs), 0)
    matched = jnp.zeros((n, seqs), kind)
    for at in range(TOPK):
        chosen = ids_s[at : at + 1, :] == experts
        matched = matched + jnp.where(chosen, weights_s[at : at + 1, :], 0.0)
    token = lax.broadcasted_iota(jnp.int32, (seqs, 2 * bulk), 0)
    spread = lax.broadcasted_iota(jnp.int32, (seqs, 2 * bulk), 1)
    member = core * plane + spot
    exact = lax.Precision.HIGHEST
    in_block = (token < block) & (spread == member * block + token)
    in_tail = (token >= block) & (spread == bulk + (token - block) * members + member)
    spread = jnp.where(in_block | in_tail, 1.0, 0.0)
    spread = jnp.dot(matched, spread, preferred_element_type=kind, precision=exact)
    for at in range(n):
        info_s[at] = spread[at : at + 1, :]
    infos_s[pl.ds(me, 1)] = info_s[pl.ds(me, 1)]
    square_s[...] = jnp.zeros_like(square_s)

    for at in range(9):
        copies[at].wait()

    normed = normalize(tokens_s[...].astype(kind), gain_s[...]).astype(half_type)
    product = jnp.dot(normed, w_qkv_s[...], preferred_element_type=kind)
    product = product.astype(half_type).astype(kind)
    key_s[...] = product[:, heads_wide : heads_wide + pair]
    value_s[...] = product[:, heads_wide + pair : heads_wide + 2 * pair]
    lane = lax.broadcasted_iota(jnp.int32, (seqs, pair), 1)
    for head in range(HEADS):
        piece = product[:, head // 2 * pair : (head // 2 + 1) * pair]
        if head % 2 != head // group:
            piece = pltpu.roll(piece, HEAD_DIM, 1)
        piece = jnp.where(lane // HEAD_DIM == head // group, piece, 0.0)
        query_s[pl.ds(head, seqs, stride=HEADS), :] = piece
    forget = lax.dot_general(
        w_forget_s[...], normed, (((1,), (1,)), ((), ())), preferred_element_type=kind
    )
    eye = lax.broadcasted_iota(jnp.int32, (HEADS, HEADS), 0)
    eye = eye == lax.broadcasted_iota(jnp.int32, (HEADS, HEADS), 1)
    forget = forget + to_column(bias_s[...], eye)
    forget_s[...] = jnp.minimum(forget, 0.0) - jnp.log1p(jnp.exp(-jnp.abs(forget)))

    seq_lane = lax.broadcasted_iota(jnp.int32, forget_s.shape, 1)
    position = lax.broadcasted_iota(jnp.int32, (HEADS, length), 1)
    unit = HEAD_DIM ** (-0.5)

    def attend(at):
        for copy in cached(at):
            copy.wait()
        scores_all = []
        own_all = []
        for item in range(batch):
            seq = at * batch + item
            query = query_s[pl.ds(pl.multiple_of(seq * HEADS, HEADS), HEADS), :]
            own = jnp.sum(query * key_s[pl.ds(seq, 1), :], axis=1, keepdims=True) * unit
            forget = jnp.sum(jnp.where(seq_lane == seq, forget_s[...], 0.0), axis=1, keepdims=True)
            cum = logcum_s[seq]
            live = lengths_s[seq]
            last = jnp.sum(jnp.where(position == live - 1, cum, 0.0), axis=1, keepdims=True)
            scores = lax.dot_general(
                query.astype(half_type),
                keys_s[seq],
                (((1,), (1,)), ((), ())),
                preferred_element_type=kind,
            )
            scores = scores * unit + ((last + forget) - cum)
            scores_all.append(jnp.where(position < live, scores, -jnp.inf))
            own_all.append(own)
        scores = jnp.concatenate(scores_all, axis=0)
        own = jnp.concatenate(own_all, axis=0)
        top = jnp.maximum(jnp.max(scores, axis=1, keepdims=True), own)
        expo = jnp.exp(scores - top)
        own_expo = jnp.exp(own - top)
        total = jnp.sum(expo, axis=1, keepdims=True) + own_expo
        share = (expo / total).astype(half_type)
        own_share = (own_expo / total).astype(half_type).astype(kind)
        for item in range(batch):
            seq = at * batch + item
            part = slice(item * HEADS, (item + 1) * HEADS)
            if item % 2 == 0:
                paired = jnp.dot(
                    share[item * HEADS : (item + 2) * HEADS],
                    jnp.concatenate([values_s[seq], values_s[seq + 1]], axis=1),
                    preferred_element_type=kind,
                )
            odd = item % 2
            result = paired[odd * HEADS : (odd + 1) * HEADS, odd * pair : (odd + 1) * pair]
            result = result + own_share[part] * value_s[pl.ds(seq, 1), :]
            heads_s[pl.ds(pl.multiple_of(seq * HEADS, HEADS), HEADS), :] = result

    def inform(k):
        to = lax.rem(me + k, n)
        return reach(info_s.at[to], infos_s.at[me], i_send.at[0], i_recv.at[0], to)

    def informed():
        every = infos_s.at[pl.ds(0, n - 1)]
        return reach(every, every, i_send.at[0], i_recv.at[0], other)

    pl.loop(0, groups // 2)(attend)
    pl.semaphore_wait(barrier, n - 1)

    @pl.loop(1, n)
    def _(k):
        inform(k).start()

    pl.loop(groups // 2, groups)(attend)

    for at in range(len(loads), len(loads) + 6):
        copies[at].wait()

    found = [heads_s[pl.ds(head, seqs, stride=HEADS), :] for head in range(HEADS)]
    pieces = []
    for tile in range(tiles):
        left, right = found[2 * tile], found[2 * tile + 1]
        if 2 * tile // group:
            left = pltpu.roll(left, HEAD_DIM, 1)
        else:
            right = pltpu.roll(right, HEAD_DIM, 1)
        pieces.append(jnp.where(lane < HEAD_DIM, left, right))
    attended = jnp.concatenate(pieces, axis=1).astype(half_type)
    mixed = tokens_s[...].astype(kind) + jnp.dot(
        attended, w_out_s[...], preferred_element_type=kind
    )
    mixed = mixed.astype(half_type).astype(kind)
    mixed_s[...] = mixed
    routed = normalize(mixed, gain_next_s[...])

    def slot(at, which, place):
        return (at * 2 + which) * plane + place

    home = slot(level, core, spot)
    for part in range(folds):
        fold_s[pl.ds(part * spare, spare), :] = routed[block:, part * fold : (part + 1) * fold]
    rows_s[home, :, 0:width] = routed[:block].astype(half_type)
    rows_s[home, :, width:wide] = fold_s[...].astype(half_type)

    def device(z, y, x, which):
        return ((z * side + y) * side + x) * 2 + which

    spot_x = row * side + 1 - col
    spot_y = (1 - row) * side + col
    spot_d = (1 - row) * side + 1 - col
    near_x = device(level, row, 1 - col, core)
    near_y = device(level, 1 - row, col, core)

    def part_of(at, place, piece):
        return rows_s.at[slot(at, core, place), :, piece * cut : (piece + 1) * cut]

    def along(at, to, piece):
        here = part_of(at, spot, piece)
        to = device(to, row, col, core)
        return reach(here, here, rows_send.at[0], z_recv.at[piece, at], to)

    def beside(at, place, piece):
        here = part_of(at, place, piece)
        return reach(here, here, rows_send.at[0], x_recv.at[piece, at], near_x)

    def above(at, place, piece):
        here = part_of(at, place, piece)
        return reach(here, here, rows_send.at[0], y_recv.at[piece, at], near_y)

    def relay_a(at, place):
        here = rows_s.at[slot(at, core, place), :, 0:cut]
        return reach(here, here, rows_send.at[0], da_recv.at[at], near_y)

    def relay_b(at, place):
        here = rows_s.at[slot(at, core, place), :, cut:wide]
        return reach(here, here, rows_send.at[0], db_recv.at[at], near_x)

    def across(at, which, place):
        here = rows_s.at[slot(at, which, place)]
        return reach(here, here, rows_send.at[0], f_recv.at[at], other)

    def crossed(at):
        here = rows_s.at[pl.ds(slot(at, 1 - core, 0), plane)]
        return reach(here, here, rows_send.at[0], f_recv.at[at], other)

    def paired(j):
        high = lax.rem(level // 2 + j // 2, 2)
        return high * 2 + lax.rem(level + j, 2)

    def ordered(j):
        return paired(j)

    def returned(j):
        return paired(deep - 1 - j)

    def share(k, at):
        return reach(
            square_s.at[at],
            squares_s.at[at, k],
            q_send.at[0],
            q_recv.at[at],
            lax.rem(me + k, n),
        )

    def shared(at):
        every = squares_s.at[at, pl.ds(1, n - 1)]
        return reach(every, every, q_send.at[0], q_recv.at[at], other)

    def sent(blocks, sem):
        every = rows_s.at[pl.ds(0, blocks)]
        return reach(every, every, sem, sem, other)

    def spread_piece(at, piece):
        if piece:
            above(at, spot, piece).start()
            beside(at, spot, piece).start()
        else:
            beside(at, spot, piece).start()
            above(at, spot, piece).start()

    for piece in range(2):
        spread_piece(level, piece)

    @pl.loop(1, deep)
    def _(j):
        for piece in range(2):
            along(level, ordered(j), piece).start()

    across(level, core, spot).start()

    for at in range(len(loads) + 6, len(loads) + len(later)):
        copies[at].wait()

    ones = jnp.ones((8, pair), kind)
    same_bulk = lax.broadcasted_iota(jnp.int32, (bulk, bulk), 0)
    same_bulk = same_bulk == lax.broadcasted_iota(jnp.int32, (bulk, bulk), 1)
    tail_at = lax.broadcasted_iota(jnp.int32, (tail, bulk), 1)
    tail_of = lax.broadcasted_iota(jnp.int32, (tail, bulk), 0)

    def dense_units(at):
        crossed(at).wait_recv()

        part = pl.ds(at * members, members)
        x_s[at, 0:bulk, :] = rows_s[part, :, 0:width].reshape(bulk, width)
        folded = rows_s[part, :, width:wide].astype(kind).reshape(bulk, fold)
        for tile in range(fold // pair):
            spread_s[tile] = folded[:, tile * pair : (tile + 1) * pair]
        for piece in range(folds):
            for tile in range(fold // pair):
                lanes = slice(piece * fold + tile * pair, piece * fold + (tile + 1) * pair)
                taken = [
                    spread_s[tile, pl.ds(piece * spare + extra, members, stride=block), :]
                    for extra in range(spare)
                ]
                x_s[at, bulk : bulk + tail, lanes] = jnp.concatenate(taken, axis=0).astype(
                    half_type
                )
        values = x_s[at]
        inner = jnp.sum(values.astype(kind) * branch_s[...], axis=1, keepdims=True)
        branch_col_s[at] = jnp.broadcast_to(jax.nn.sigmoid(inner), (bulk + tail, pair))
        both = jnp.dot(values, d_in_s[...], preferred_element_type=kind)
        gate, up = both[:, 0:pair], both[:, pair : 2 * pair]
        units = (gate * jax.nn.sigmoid(gate) * up).astype(half_type).astype(kind)
        hidden_s[at] = (units * d_gain_s[pl.ds(me, 1), :]).astype(half_type)
        squares = jnp.sum(units * units, axis=1, keepdims=True)
        square_s[at, :, 0:bulk] = to_row(squares[0:bulk], same_bulk)
        ends = jnp.where(tail_at == tail_of, squares[bulk:], 0.0)
        square_s[at, :, bulk : 2 * bulk] = jnp.sum(ends, axis=0, keepdims=True)
        squares_s[at, 0] = square_s[at]

        for k in range(1, n):
            share(k, at).start()

    def run_expert(at):
        values = x_s[at]
        both = jnp.dot(values, e_in_s[...], preferred_element_type=kind)
        ff = e_in_s.shape[1] // 2
        gate = jnp.minimum(both[:, 0:ff], LIMIT)
        up = jnp.clip(both[:, ff : 2 * ff], -LIMIT, LIMIT)
        act = ((up + 1.0) * gate * jax.nn.sigmoid(gate * ALPHA)).astype(half_type)
        answer_s[at] = jnp.dot(act, e_down_s[...], preferred_element_type=kind).astype(half_type)

    def columns(line):
        main = to_column(line[:, 0:bulk], same_bulk)
        ends = jnp.where(tail_at == tail_of, line[:, bulk : 2 * bulk], 0.0)
        return main, jnp.sum(ends, axis=1, keepdims=True)

    def cross(at):
        return reach(
            part_s.at[at, pl.ds((1 - core) * plane, plane)],
            joint_s.at[at],
            back_send.at[0],
            c_recv.at[at],
            other,
        )

    def first(at, k):
        place_a = lax.rem(row + 1 + k, side)
        place_b = lax.rem(col + 1 + k, side)
        return (
            reach(
                pair_s.at[at, place_a * side + 1 - col, :, 0:cut],
                first_a.at[at, place_a],
                back_send.at[0],
                s1a_recv.at[at, lax.rem(place_a + row, side)],
                near_x,
            ),
            reach(
                pair_s.at[at, (1 - row) * side + place_b, :, cut:wide],
                first_b.at[at, place_b],
                back_send.at[0],
                s1b_recv.at[at, lax.rem(place_b + col, side)],
                near_y,
            ),
        )

    def second(at):
        return (
            reach(turn_a.at[at], second_a.at[at], back_send.at[0], s2a_recv.at[at], near_y),
            reach(turn_b.at[at], second_b.at[at], back_send.at[0], s2b_recv.at[at], near_x),
        )

    def home_to(at):
        return reach(
            level_s.at[at],
            levels_s.at[level],
            back_send.at[0],
            zz_recv.at[level],
            device(at, row, col, core),
        )

    def home_from(at):
        return reach(
            level_s.at[at],
            levels_s.at[at],
            back_send.at[0],
            zz_recv.at[at],
            device(at, row, col, core),
        )

    def combine(at):
        shared(at).wait_recv()
        dense = jnp.dot(hidden_s[at], d_down_s[...], preferred_element_type=kind)
        coef = jnp.sum(infos_s[pl.ds(at * members, members)], axis=0)
        scale = lax.rsqrt(jnp.sum(squares_s[at], axis=0) / units_total + EPS)
        weight, weight_end = columns(coef)
        scale, scale_end = columns(scale)
        twice = branch_col_s[at, :, 0:1]
        main = weight * answer_s[at, 0:bulk, :].astype(kind)
        main = main + (scale * twice[0:bulk]) * dense[0:bulk]
        ends = weight_end * answer_s[at, bulk : bulk + tail, :].astype(kind)
        ends = ends + (scale_end * twice[bulk:]) * dense[bulk:]
        part_s[at, :, :, 0:width] = main.astype(half_type).reshape(members, block, width)
        for piece in range(folds):
            for tile in range(fold // pair):
                first_lane = piece * fold + tile * pair
                for extra in range(spare):
                    spread_s[tile, pl.ds(piece * spare + extra, members, stride=block), :] = (
                        ends[
                            extra * members : (extra + 1) * members,
                            first_lane : first_lane + pair,
                        ]
                    )
        for tile in range(fold // pair):
            part_s[at, :, :, width + tile * pair : width + (tile + 1) * pair] = (
                spread_s[tile].astype(half_type).reshape(members, block, pair)
            )
        cross(at).start()

    def join(at):
        cross(at).wait_recv()
        mine = part_s[at, pl.ds(core * plane, plane)].astype(kind)
        pair_s[at] = (mine + joint_s[at].astype(kind)).astype(half_type)
        for k in range(side):
            for copy in first(at, k):
                copy.start()

    def turn(at):
        for copy in first(at, 0):
            copy.wait_recv()
        turned = pair_s[at, spot_y, :, 0:cut].astype(kind) + first_a[at, 1 - row].astype(kind)
        turn_a[at] = turned.astype(half_type)
        turned = pair_s[at, spot_x, :, cut:wide].astype(kind) + first_b[at, 1 - col].astype(kind)
        turn_b[at] = turned.astype(half_type)
        for copy in second(at):
            copy.start()

    def settle(at):
        for copy in first(at, 1):
            copy.wait_recv()
        for copy in second(at):
            copy.wait_recv()
        total = pair_s[at, spot, :, 0:cut].astype(kind) + first_a[at, row].astype(kind)
        total = total + second_a[at].astype(kind)
        level_s[at, :, 0:cut] = total.astype(half_type)
        total = pair_s[at, spot, :, cut:wide].astype(kind) + first_b[at, col].astype(kind)
        total = total + second_b[at].astype(kind)
        level_s[at, :, cut:wide] = total.astype(half_type)

        @pl.when(at != level)
        def _():
            home_to(at).start()

    def native(at):
        for piece in range(2):
            along(at, 0, piece).wait_recv()
            spread_piece(at, piece)
        across(at, core, spot).start()

    def relay(at):
        beside(at, spot_x, 0).wait_recv()
        relay_a(at, spot_x).start()
        above(at, spot_y, 1).wait_recv()
        relay_b(at, spot_y).start()
        beside(at, spot_x, 1).wait_recv()
        across(at, core, spot_x).start()
        above(at, spot_y, 0).wait_recv()
        across(at, core, spot_y).start()

    def corner(at):
        relay_a(at, spot_d).wait_recv()
        relay_b(at, spot_d).wait_recv()
        across(at, core, spot_d).start()

    def at_step(step, start, stop, act, lag, order):
        @pl.when((step >= start) & (step < stop))
        def _():
            act(order(step - lag))

    relay(ordered(0))
    native(ordered(1))
    corner(ordered(0))
    native(ordered(2))
    relay(ordered(1))
    native(ordered(3))
    dense_units(ordered(0))
    relay(ordered(2))
    corner(ordered(1))
    run_expert(ordered(0))
    relay(ordered(3))
    corner(ordered(2))
    dense_units(ordered(1))
    run_expert(ordered(1))
    corner(ordered(3))
    dense_units(ordered(2))
    dense_units(ordered(3))
    run_expert(ordered(2))
    run_expert(ordered(3))

    informed().wait_recv()

    @pl.loop(0, deep + 3)
    def _(step):
        at_step(step, 0, deep, combine, 0, returned)
        at_step(step, 1, deep + 1, join, 1, returned)
        at_step(step, 2, deep + 2, turn, 2, returned)
        at_step(step, 3, deep + 3, settle, 3, returned)

    total = level_s[level].astype(kind)
    for j in range(deep - 1):
        at = returned(j)
        home_from(at).wait_recv()
        total = total + levels_s[at].astype(kind)
    out[0:block, :] = (mixed_s[0:block, :] + total[:, 0:width]).astype(half_type)
    fold_s[...] = total[:, width:wide]
    for part in range(folds):
        lanes = slice(part * fold, (part + 1) * fold)
        ends = mixed_s[block:seqs, lanes] + fold_s[pl.ds(part * spare, spare), :]
        out[block:seqs, lanes] = ends.astype(half_type)

    sent(chips + 4 * deep - 1, rows_send.at[0]).wait_send()
    sent(chips + 4 * deep - 1, back_send.at[0]).wait_send()
    informed().wait_send()
    every = squares_s.at[:, pl.ds(1, n - 1)]
    reach(every, every, q_send.at[0], q_recv.at[0], other).wait_send()


def fast(n, deep, arrays, units_total):
    (tokens, keys, logcum, e_gate, e_down, d_gate, d_gain) = (
        arrays[0],
        arrays[8],
        arrays[10],
        arrays[15],
        arrays[17],
        arrays[18],
        arrays[21],
    )
    seqs, width = tokens.shape
    length, pair = keys.shape[1:]
    hidden = e_gate.shape[2]
    local = d_gate.shape[1]
    chips = n // 2
    plane = chips // deep
    block = seqs // 16 * 16
    spare = seqs - block
    wide = width + spare * width // block
    fold = wide - width
    cut = wide // 2
    members = 2 * plane
    bulk = members * block
    tail = members * spare
    heads_wide = HEADS * HEAD_DIM
    half_type = jnp.bfloat16
    kind = jnp.float32
    dma = pltpu.SemaphoreType.DMA
    groups = 3
    vmem = pltpu.VMEM
    scratch = [
        vmem((seqs, width), half_type),
        vmem((1, width), kind),
        vmem((width, heads_wide + 2 * pair), half_type),
        vmem((HEADS, width), half_type),
        vmem((1, HEADS), kind),
        vmem((heads_wide, width), half_type),
        vmem((seqs, length, pair), half_type),
        vmem((seqs, length, pair), half_type),
        vmem((seqs, HEADS, length), kind),
        pltpu.SMEM((seqs,), jnp.int32),
        vmem((1, width), kind),
        vmem((TOPK, seqs), jnp.int32),
        vmem((TOPK, seqs), kind),
        vmem((width, 2 * hidden), half_type),
        vmem((hidden, width), half_type),
        vmem((width, 2 * local), half_type),
        vmem((local, width), half_type),
        vmem(d_gain.shape, kind),
        vmem((1, width), kind),
        vmem((seqs * HEADS, pair), kind),
        vmem((seqs, pair), kind),
        vmem((seqs, pair), kind),
        vmem((HEADS, seqs), kind),
        vmem((seqs * HEADS, pair), kind),
        vmem((seqs, width), kind),
        vmem((block, fold), kind),
        vmem((n, block, wide), half_type),
        vmem((deep, bulk + tail, width), half_type),
        vmem((fold // pair, bulk, pair), kind),
        vmem((deep, bulk + tail, local), half_type),
        vmem((deep, bulk + tail, pair), kind),
        vmem((deep, 1, 2 * bulk), kind),
        vmem((deep, n, 1, 2 * bulk), kind),
        vmem((n, 1, 2 * bulk), kind),
        vmem((n, 1, 2 * bulk), kind),
        vmem((deep, bulk + tail, width), half_type),
        vmem((deep, members, block, wide), half_type),
        vmem((deep, plane, block, wide), half_type),
        vmem((deep, plane, block, wide), half_type),
        vmem((deep, 2, block, cut), half_type),
        vmem((deep, 2, block, cut), half_type),
        vmem((deep, block, cut), half_type),
        vmem((deep, block, cut), half_type),
        vmem((deep, block, cut), half_type),
        vmem((deep, block, cut), half_type),
        vmem((deep, block, wide), half_type),
        vmem((deep, block, wide), half_type),
        dma((21,)),
        dma((2, groups)),
        dma((2, deep)),
        dma((1,)),
        dma((2, deep)),
        dma((2, deep)),
        dma((deep,)),
        dma((deep,)),
        dma((deep,)),
        dma((1,)),
        dma((1,)),
        dma((1,)),
        dma((deep,)),
        dma((1,)),
        dma((deep,)),
        dma((deep, 2)),
        dma((deep, 2)),
        dma((deep,)),
        dma((deep,)),
        dma((deep,)),
    ]
    return pl.pallas_call(
        functools.partial(fast_body, units_total),
        out_shape=jax.ShapeDtypeStruct(tokens.shape, half_type),
        in_specs=[pl.BlockSpec(memory_space=pl.ANY)] * len(arrays),
        out_specs=pl.BlockSpec(memory_space=pltpu.VMEM),
        scratch_shapes=scratch,
        compiler_params=pltpu.CompilerParams(
            collective_id=0, has_side_effects=True, vmem_limit_bytes=62 * 1024 * 1024
        ),
        name="layer",
    )(*arrays)


def shards(
    tokens,
    attn_norm_gain,
    w_query,
    w_key,
    w_value,
    w_forget,
    forget_bias,
    w_attn_out,
    cache_keys,
    cache_values,
    cache_logcum,
    cache_lengths,
    expert_norm_gain,
    expert_ids,
    expert_weights,
    w_expert_gate,
    w_expert_up,
    w_expert_down,
    w_dense_gate,
    w_dense_up,
    w_dense_down,
    dense_norm_gain,
    branch_gate,
):
    n = lax.axis_size("ep")
    deep = 4
    seqs, width = tokens.shape
    local = w_dense_gate.shape[1]
    spare = seqs % 16
    fits = n == 8 * deep and local == cache_keys.shape[2] and 0 < spare and spare * width % 2048 == 0
    if fits and seqs // 16 == 1:
        return fast(
            n,
            deep,
            (
                tokens,
                attn_norm_gain[None, :],
                w_query,
                w_key,
                w_value,
                w_forget.T,
                forget_bias[None, :],
                w_attn_out,
                cache_keys,
                cache_values,
                cache_logcum,
                cache_lengths,
                expert_norm_gain[None, :],
                expert_ids.T,
                expert_weights.T,
                w_expert_gate,
                w_expert_up,
                w_expert_down,
                w_dense_gate,
                w_dense_up,
                w_dense_down,
                dense_norm_gain.reshape(n, local),
                branch_gate[None, :],
            ),
            dense_norm_gain.shape[0],
        )
    mixed, routed_in = front(
        tokens,
        attn_norm_gain,
        w_query,
        w_key,
        w_value,
        w_forget,
        forget_bias,
        w_attn_out,
        cache_keys,
        cache_values,
        cache_logcum,
        cache_lengths,
        expert_norm_gain,
    )
    n = lax.axis_size("ep")
    me = lax.axis_index("ep")
    seqs = tokens.shape[0]
    extra = jnp.concatenate([expert_ids.astype(jnp.bfloat16), *split3(expert_weights)], axis=1)
    packed = jnp.concatenate([routed_in, jnp.pad(extra, ((0, 0), (0, 128 - 4 * TOPK)))], axis=1)
    packed = jnp.pad(packed, ((0, -seqs % 8), (0, 0)))
    local = w_dense_gate.shape[1]
    gain = lax.dynamic_slice_in_dim(dense_norm_gain, me * local, local, 0)
    return rest(
        n,
        packed,
        mixed,
        w_expert_gate[0],
        w_expert_up[0],
        w_expert_down[0],
        w_dense_gate,
        w_dense_up,
        w_dense_down,
        gain[None, :],
        branch_gate[None, :],
        dense_norm_gain.shape[0],
    )


def solution(mesh):
    in_specs = (
        P("ep", None),
        P(),
        P(),
        P(),
        P(),
        P(),
        P(),
        P(),
        P("ep", None, None),
        P("ep", None, None),
        P("ep", None, None),
        P("ep"),
        P(),
        P("ep", None),
        P("ep", None),
        P("ep", None, None),
        P("ep", None, None),
        P("ep", None, None),
        P(None, "ep"),
        P(None, "ep"),
        P("ep", None),
        P(),
        P(),
    )
    out_specs = P("ep", None)
    return jax.shard_map(shards, mesh=mesh, in_specs=in_specs, out_specs=out_specs, check_vma=False)
```
